128 devices in a mesh: kv: 16 (over z, y), tp: 8 (over x, core).
Axes of the slice: x: 4, y: 4, z: 4, core: 2. Of those that a mesh axis runs over, the one named last changes fastest.
Arguments:
- residual_entries: bfloat16 [1024, 4096], P(None, ('kv', 'tp')), may hold values from -6 to 6
- fresh_extents: int32 [128], replicated, may hold values from 1 to 8, 512 in all
- memory_matrix: float32 [128, 16, 128, 128], P('kv', 'tp'), may hold values from -3 to 3
- initial_rescale_vector: float32 [4096], P('kv'), may hold values from 0.1 to 1.9
- probe_matrix: bfloat16 [4096, 2048], P('kv', 'tp'), may hold values from -0.09375 to 0.09375
- retain_matrix: bfloat16 [4096, 2048], P('kv', 'tp'), may hold values from -0.09375 to 0.09375
- content_matrix: bfloat16 [4096, 2048], P('kv', 'tp'), may hold values from -0.09375 to 0.09375
- result_switch_matrix: bfloat16 [4096, 2048], P('kv', 'tp'), may hold values from -0.09375 to 0.09375
- retain_lower_limit: float32 [2048], P('tp'), may hold values from 0 to 0.9
- extra_shrink_log: float32 [1024, 16], P('kv', 'tp'), may hold values from -0.7 to 0
- lane_result_rescale: float32 [128], replicated, may hold values from 0.1 to 1.9
- result_matrix: bfloat16 [2048, 4096], P('tp', 'kv'), may hold values from -0.125 to 0.125
- later_rescale_vector: float32 [4096], P(('kv', 'tp')), may hold values from 0.1 to 1.9
- mixer_switch_matrix: bfloat16 [4096, 11008], P(None, ('kv', 'tp')), may hold values from -0.09375 to 0.09375
- widening_matrix: bfloat16 [4096, 11008], P(None, ('kv', 'tp')), may hold values from -0.09375 to 0.09375
- narrowing_matrix: bfloat16 [11008, 4096], P(('kv', 'tp')), may hold values from -0.21875 to 0.21875
Outputs:
- mixed: bfloat16 [1024, 4096], P(None, ('kv', 'tp'))
- new_state: float32 [128, 16, 128, 128], P('kv', 'tp')
The draws below stay inside these ranges and needn't reach their ends.
Inputs may be any that keep to these rules, and one draw needn't show every extreme that they name: `fresh_extents`: the lengths sum to exactly 512.
All inputs are finite; a program needn't handle non-finite values.
Results may differ from the reference program's by a relative error of at most 0.022.
Values may be sent and summed in bfloat16 or wider, within the bound.
A program may use at most 64 MiB of HBM per device.

```python
import math
import jax
import jax.numpy as jnp
import numpy as np
from jax import lax

D = 4096
MIXER_LANES = 16
HEAD = 128
FF = 11008
FRESH_PLACES = 8
STRING_TOTAL = 128
PLACE_TOTAL = 1024
WIDTH = 2048
N_TP = 8


def with_spikes(result, rng, source, target, parts, factor):
    owner, partner = [(jnp.arange(result.shape[dim]) // (result.shape[dim] // parts)).reshape([-1 if axis == dim else 1 for axis in range(result.ndim)]) for dim in (source, target)]
    chosen = jax.random.permutation(rng, parts)[partner]
    strong = (owner == chosen) | (owner == (partner + parts // 2) % parts)
    return jnp.where(strong, factor * result, result)


def level_of(stream_key, extent, cuts, low, high):
    def one(dim, blocks):
        heights = jax.random.uniform(jax.random.fold_in(jax.random.fold_in(stream_key, 6), dim), (blocks,), jnp.float32, low / len(cuts), high / len(cuts))
        return jnp.repeat(jnp.exp(heights), extent[dim] // blocks).reshape((-1,) + (1,) * (len(extent) - dim - 1))

    level = one(*cuts[0])
    for cut in cuts[1:]:
        level = level * one(*cut)
    return level


def profile(count, total, limit, skew):
    portions = [(1 << 20) // math.isqrt(standing ** skew) + 1 for standing in range(2, count + 1)]
    spare, counts = total - limit - (count - 1), [1] * (count - 1)
    while spare > 0:
        candidates = [i for i in range(count - 1) if counts[i] < limit]
        whole, budget = sum([portions[i] for i in candidates]), spare
        for i in candidates:
            extra = min(limit - counts[i], max(1, budget * portions[i] // whole), spare)
            counts[i] = counts[i] + extra
            spare = spare - extra
    return np.array([limit] + counts)


def uneven(stream_key, number_of, total, most, slope):
    if number_of == 2:
        one = jax.random.randint(stream_key, (), max(1, total - most), min(most, total - 1) + 1)
        return jnp.stack([one, total - one])
    lengths = jnp.asarray(profile(number_of, total, most, slope), jnp.int32)
    twos = (number_of - 1) // 2
    giver, sink = lengths[1:1 + 2 * twos:2], lengths[2:2 + 2 * twos:2]
    slack = jnp.minimum(giver - 1, most - sink)
    shifted = jax.random.randint(jax.random.fold_in(stream_key, 1), (twos,), 0, 1 << 20) % (slack + 1)
    lengths = lengths.at[1:1 + 2 * twos:2].set(giver - shifted).at[2:2 + 2 * twos:2].set(sink + shifted)
    return lengths[jax.random.permutation(jax.random.fold_in(stream_key, 2), number_of)]


def normal_values(key, extent, width, limit, cuts=(), kind=jnp.bfloat16):
    level = level_of(key, extent, cuts, -0.22, 0.18) if cuts else 1.0
    array = jax.random.normal(key, extent, jnp.float32) * width * level
    return jnp.minimum(jnp.maximum(array, -limit), limit).astype(kind)


def bell_draw_with(key, shape, deviation, reach, split, heavy, kind=jnp.bfloat16):
    array = deviation * jax.random.normal(key, shape, jnp.float32)
    if split:
        array = array * level_of(key, shape, split, -0.22, 0.18)
    return jnp.clip(with_spikes(array, jax.random.fold_in(key, 3), *heavy), -reach, reach).astype(kind)


def setup_inputs(seed: int = 0) -> dict:
    key_of = jax.random.split(jax.random.key(seed), 17)
    return {
        "residual_entries": normal_values(key_of[0], (PLACE_TOTAL, D), 1.0, 6.0, ((1, 128),)),
        "fresh_extents": uneven(key_of[1], STRING_TOTAL, STRING_TOTAL * FRESH_PLACES // 2, FRESH_PLACES, 2).astype(jnp.int32),
        "memory_matrix": normal_values(key_of[2], (STRING_TOTAL, MIXER_LANES, HEAD, HEAD), 0.3, 3.0, ((0, 16), (1, 8)), jnp.float32),
        "initial_rescale_vector": jnp.clip(1.0 + 0.18 * jax.random.normal(key_of[3], (D,), jnp.float32), 0.1, 1.9),
        "probe_matrix": normal_values(key_of[4], (D, WIDTH), D ** -0.5, 0.09375, ((0, 16), (1, 8))),
        "retain_matrix": normal_values(key_of[5], (D, WIDTH), D ** -0.5, 0.09375, ((0, 16), (1, 8))),
        "content_matrix": normal_values(key_of[6], (D, WIDTH), D ** -0.5, 0.09375, ((0, 16), (1, 8))),
        "result_switch_matrix": normal_values(key_of[7], (D, WIDTH), D ** -0.5, 0.09375, ((0, 16), (1, 8))),
        "retain_lower_limit": jnp.clip(0.9 * jax.random.uniform(key_of[8], (WIDTH,), jnp.float32) ** level_of(key_of[8], (WIDTH,), ((0, 8),), -0.2, 0.2), 0.0, 0.9),
        "extra_shrink_log": jnp.clip(-0.7 + 0.7 * jax.random.uniform(key_of[9], (PLACE_TOTAL, MIXER_LANES), jnp.float32) ** level_of(key_of[9], (PLACE_TOTAL, MIXER_LANES), ((0, 16), (1, 8)), -0.2, 0.2), -0.7, 0.0),
        "lane_result_rescale": jnp.clip(1.0 + 0.18 * jax.random.normal(key_of[10], (HEAD,), jnp.float32), 0.1, 1.9),
        "result_matrix": normal_values(key_of[11], (WIDTH, D), WIDTH ** -0.5, 0.125, ((0, 8), (1, 16))),
        "later_rescale_vector": jnp.clip(1.0 + 0.18 * jax.random.normal(key_of[12], (D,), jnp.float32), 0.1, 1.9),
        "mixer_switch_matrix": normal_values(key_of[13], (D, FF), D ** -0.5, 0.09375, ((1, 128),)),
        "widening_matrix": normal_values(key_of[14], (D, FF), D ** -0.5, 0.09375, ((1, 128),)),
        "narrowing_matrix": bell_draw_with(key_of[15], (FF, D), FF ** -0.5, 0.21875, ((0, 128),), (0, 1, 128, 5.5)),
    }


epsilon = 1e-06

def reference(residual_entries, fresh_extents, memory_matrix, initial_rescale_vector, probe_matrix, retain_matrix, content_matrix, result_switch_matrix, retain_lower_limit, extra_shrink_log, lane_result_rescale, result_matrix, later_rescale_vector, mixer_switch_matrix, widening_matrix, narrowing_matrix):
    tokens_wide = residual_entries.astype(jnp.float32)
    first_scale = lax.rsqrt(lax.optimization_barrier(jnp.mean(tokens_wide * tokens_wide, axis=1)) + epsilon)
    scaled = (tokens_wide * initial_rescale_vector).astype(jnp.bfloat16)

    def project(weight):
        return jnp.dot(scaled, weight, preferred_element_type=jnp.float32) * first_scale[:, None]
    shape_four = (STRING_TOTAL, FRESH_PLACES, MIXER_LANES, HEAD)
    z_query = project(probe_matrix)
    z_forget = project(retain_matrix).reshape(shape_four)
    z_input = project(content_matrix).reshape(shape_four)
    z_outgate = project(result_switch_matrix)
    living = jnp.arange(FRESH_PLACES, dtype=jnp.int32)[None, :] < fresh_extents[:, None]
    query = jax.nn.silu(z_query).reshape(shape_four)
    bounds = retain_lower_limit.reshape(MIXER_LANES, HEAD)
    retain_factor = bounds + (1.0 - bounds) * jax.nn.sigmoid(z_forget)
    shrink_exponent = jnp.log(retain_factor) + extra_shrink_log.reshape(STRING_TOTAL, FRESH_PLACES, MIXER_LANES, 1)
    decays = jnp.where(living[:, :, None, None], jnp.exp(shrink_exponent), 1.0)
    key_gate = jnp.where(living[:, :, None, None], 1.0 - retain_factor, 0.0)
    carried = memory_matrix
    outputs = []
    for position in range(FRESH_PLACES):
        carried = decays[:, position, :, :, None] * carried + key_gate[:, position, :, :, None] * z_input[:, position, :, None, :]
        outputs.append(jnp.einsum('bhd,bhdv->bhv', query[:, position], carried, precision=lax.Precision.HIGHEST))
    heads_out = jnp.stack(outputs, axis=1)
    heads_out = heads_out * lax.rsqrt(lax.optimization_barrier(jnp.mean(heads_out * heads_out, axis=-1, keepdims=True)) + epsilon) * lane_result_rescale
    live_rows = living.reshape(PLACE_TOTAL)
    normed = jnp.where(live_rows[:, None], heads_out.reshape(PLACE_TOTAL, WIDTH) * jax.nn.silu(z_outgate), 0.0).astype(jnp.bfloat16)
    group_width = WIDTH // N_TP
    attended = jnp.zeros((PLACE_TOTAL, D), jnp.float32)
    for group in range(N_TP):
        head_partial = jnp.dot(normed[:, group * group_width:(group + 1) * group_width], result_matrix[group * group_width:(group + 1) * group_width], preferred_element_type=jnp.float32).astype(jnp.bfloat16)
        attended = attended + head_partial.astype(jnp.float32)
    residual = (tokens_wide + attended).astype(jnp.bfloat16)
    resid_wide = residual.astype(jnp.float32)
    second_scale = lax.rsqrt(lax.optimization_barrier(jnp.mean(resid_wide * resid_wide, axis=1)) + epsilon)
    second_in = (resid_wide * later_rescale_vector * second_scale[:, None]).astype(jnp.bfloat16)
    gated = jnp.dot(second_in, mixer_switch_matrix, preferred_element_type=jnp.float32)
    upward = jnp.dot(second_in, widening_matrix, preferred_element_type=jnp.float32)
    hidden = (jax.nn.silu(gated) * upward).astype(jnp.bfloat16)
    down_terms = jnp.dot(hidden, narrowing_matrix, preferred_element_type=jnp.float32)
    mixed = jnp.where(live_rows[:, None], resid_wide + down_terms, 0.0).astype(jnp.bfloat16)
    return (mixed, carried)
```

```python
import functools

import jax
import jax.numpy as jnp
from jax import lax
from jax.experimental import pallas as pl
from jax.experimental.pallas import tpu as pltpu
from jax.sharding import Mesh
from jax.sharding import PartitionSpec as P

D = 4096
HEAD = 128
FRESH_PLACES = 8
KV = ("kv_0", "kv_1")
TP = ("tp_0", "tp_1")
KV_TP = ("kv_0", "kv_1", "tp_0", "tp_1")


epsilon = 1e-06


def joined_along(pieces, dim):
    pieces = jnp.moveaxis(pieces, 0, dim)
    shape = pieces.shape
    return pieces.reshape(*shape[:dim], shape[dim] * shape[dim + 1], *shape[dim + 2 :])


def copy_for_each(x, axis):
    devices = lax.axis_size(axis)
    return lax.all_to_all(jnp.broadcast_to(x[None], (devices, *x.shape)), axis, 0, 0, tiled=True)


def gather_directly(x, axis, dim):
    return joined_along(copy_for_each(x, axis), dim)


def split_up(x, dim, devices):
    before, after = (x.shape[:dim], x.shape[dim + 1 :])
    return jnp.moveaxis(x.reshape(*before, devices, -1, *after), dim, 0)


def sum_at_owner(x, axis, dim):
    devices = lax.axis_size(axis)
    pieces = lax.all_to_all(split_up(x, dim, devices), axis, 0, 0, tiled=True)
    return jnp.sum(pieces, axis=0)


def own_rows(terms, axes):
    total = terms.astype(jnp.bfloat16)
    for axis in axes:
        total = lax.psum_scatter(total, axis, scatter_dimension=0, tiled=True)
    return total.astype(jnp.float32)


def sent_and_summed(x, axis, dim):
    devices = lax.axis_size(axis)
    pieces = lax.all_to_all(split_up(x, dim, devices), axis, 0, 0, tiled=True)
    return jnp.sum(pieces.astype(jnp.float32), axis=0)


def one_axis_at_a_time(x, axes):
    return functools.reduce(lax.psum, axes, x)


def sum_in_two_steps(x, axes, dim):
    far, near = axes
    pieces = split_up(x, dim, lax.axis_size(far))
    nearer = sent_and_summed(pieces, near, dim + 1)
    arrived = lax.all_to_all(
        nearer.astype(jnp.bfloat16), far, split_axis=0, concat_axis=0, tiled=True
    )
    return arrived.astype(jnp.float32).sum(axis=0)


MESH = pl.DeviceIdType.MESH
EPS = 1e-06
F32 = jnp.float32
BF = jnp.bfloat16
PARTS = ((0, 3, "xyz"), (3, 3, "yzx"), (6, 2, "zxy"))


def my_position():
    return dict(
        z=lax.axis_index("kv_0"),
        y=lax.axis_index("kv_1"),
        x=lax.axis_index("tp_0"),
        c=lax.axis_index("tp_1"),
    )


def device_at(at, **moved):
    there = dict(at, **moved)
    return (there["z"], there["y"], there["x"], there["c"])


def plane_offsets():
    return [(dz, dy) for dz in range(4) for dy in range(4) if dz or dy]


def line_offsets():
    return [(dx, dc) for dx in range(4) for dc in range(2) if dx or dc]


def plane_peer(at, dz, dy):
    return device_at(at, z=(at["z"] + dz) % 4, y=(at["y"] + dy) % 4)


def line_peer(at, dx, dc):
    return device_at(at, x=(at["x"] + dx) % 4, c=(at["c"] + dc) % 2)


def meet(peers):
    barrier = pltpu.get_barrier_semaphore()
    for peer in peers:
        pl.semaphore_signal(barrier, inc=1, device_id=peer, device_id_type=MESH)
    pl.semaphore_wait(barrier, len(peers))


def send(src, dst, sems, i, peer):
    copy = pltpu.make_async_remote_copy(
        src_ref=src,
        dst_ref=dst,
        send_sem=sems[0].at[i],
        recv_sem=sems[1].at[i],
        device_id=peer,
        device_id_type=MESH,
    )
    copy.start()
    return copy


def row_of(column, rows):
    eye = lax.broadcasted_iota(jnp.int32, (rows, 128), 0) == lax.broadcasted_iota(
        jnp.int32, (rows, 128), 1
    )
    return jnp.sum(jnp.where(eye, column, 0.0), axis=0, keepdims=True)


def column_of(row, rows):
    eye = lax.broadcasted_iota(jnp.int32, (rows, 128), 0) == lax.broadcasted_iota(
        jnp.int32, (rows, 128), 1
    )
    return jnp.sum(jnp.where(eye, row, 0.0), axis=1, keepdims=True)


def halves(length):
    return pl.ds(0, length // 2), pl.ds(length // 2, length - length // 2)


def gather_phase(at, bufs, phase, sems, base):
    first = []
    for p, (_, _, order) in enumerate(PARTS):
        axis = order[phase]
        pre = tuple(at[a] for a in order[:phase:-1])
        m = at[axis]
        up, down = (m + 1) % 4, (m + 3) % 4
        own = bufs[p].at[(*pre, m)]
        i = base + 4 * p
        first.append((
            send(own, own, sems, i, device_at(at, **{axis: up})),
            send(own, own, sems, i + 1, device_at(at, **{axis: down})),
        ))
    second = []
    for p, (_, _, order) in enumerate(PARTS):
        axis = order[phase]
        pre = tuple(at[a] for a in order[:phase:-1])
        m = at[axis]
        up, down = (m + 1) % 4, (m + 3) % 4
        lo, hi = halves(bufs[p].shape[len(pre) + 1])
        i = base + 4 * p
        first[p][0].wait_recv()
        from_down = bufs[p].at[(*pre, down, lo)]
        a = send(from_down, from_down, sems, i + 2, device_at(at, **{axis: up}))
        first[p][1].wait_recv()
        from_up = bufs[p].at[(*pre, up, hi)]
        b = send(from_up, from_up, sems, i + 3, device_at(at, **{axis: down}))
        second.append((a, b))
    for p in range(3):
        for copy in first[p]:
            copy.wait_send()
        for copy in second[p]:
            copy.wait()


def add_into(ref, idx, terms):
    total = ref[idx].astype(F32)
    for term in terms:
        total = total + term.astype(F32)
    ref[idx] = total.astype(BF)


def reduce_phase(at, bufs, phase, one_up, one_down, two_up, two_down, sems, base):
    early = []
    for p, (_, _, order) in enumerate(PARTS):
        axis = order[phase]
        pre = tuple(at[a] for a in order[:phase:-1])
        m = at[axis]
        up, down, far = (m + 1) % 4, (m + 3) % 4, (m + 2) % 4
        to_up, to_down = device_at(at, **{axis: up}), device_at(at, **{axis: down})
        lo, hi = halves(bufs[p].shape[len(pre) + 1])
        i = base + 6 * p
        early.append((
            send(bufs[p].at[(*pre, far, lo)], one_up[p], sems, i, to_up),
            send(bufs[p].at[(*pre, far, hi)], one_down[p], sems, i + 1, to_down),
            send(bufs[p].at[(*pre, up, hi)], two_up[p].at[hi], sems, i + 2, to_up),
            send(bufs[p].at[(*pre, down, lo)], two_down[p].at[lo], sems, i + 3, to_down),
        ))
    late = []
    for p, (_, _, order) in enumerate(PARTS):
        axis = order[phase]
        pre = tuple(at[a] for a in order[:phase:-1])
        m = at[axis]
        up, down = (m + 1) % 4, (m + 3) % 4
        to_up, to_down = device_at(at, **{axis: up}), device_at(at, **{axis: down})
        lo, hi = halves(bufs[p].shape[len(pre) + 1])
        i = base + 6 * p
        early[p][0].wait_recv()
        add_into(bufs[p], (*pre, up, lo), [one_up[p][...]])
        a = send(bufs[p].at[(*pre, up, lo)], two_up[p].at[lo], sems, i + 4, to_up)
        early[p][1].wait_recv()
        add_into(bufs[p], (*pre, down, hi), [one_down[p][...]])
        b = send(bufs[p].at[(*pre, down, hi)], two_down[p].at[hi], sems, i + 5, to_down)
        late.append((a, b))
    for p, (_, _, order) in enumerate(PARTS):
        axis = order[phase]
        pre = tuple(at[a] for a in order[:phase:-1])
        for copy in early[p][2:]:
            copy.wait_recv()
        for copy in late[p]:
            copy.wait_recv()
        for copy in (*early[p], *late[p]):
            copy.wait_send()
        add_into(bufs[p], (*pre, at[axis]), [two_up[p][...], two_down[p][...]])


def mixer_kernel(
    normed_ref, packed_ref, x_ref, result_ref, gain_ref, gate_ref, wide_ref, narrow_ref,
    out_ref,
    heads, partial, arrived, gains, residual_ref, squares, squares_sum, squares_line,
    weights, narrow, total, ga, gb, gc,
    *rest,
):
    (pa, pb, pc), rest = rest[:3], rest[3:]
    receive, rest = rest[:36], rest[36:]
    ypack, yarrive, sends, recvs = rest
    sems = (sends, recvs)
    at = my_position()
    kv = 4 * at["z"] + at["y"]
    tp = 2 * at["x"] + at["c"]
    planes, lines = plane_offsets(), line_offsets()
    meet([plane_peer(at, *d) for d in planes] + [line_peer(at, *d) for d in lines])

    copies = [
        send(normed_ref, heads.at[kv], sems, i, plane_peer(at, *d)) for i, d in enumerate(planes)
    ]
    gain_copies = [
        send(gain_ref, gains.at[tp], sems, 15 + i, line_peer(at, *d)) for i, d in enumerate(lines)
    ]
    partner = line_peer(at, 0, 1)
    zeros = jnp.zeros((256, 128 - 86), BF)

    def widen(k, carry):
        rows = pl.ds(pl.multiple_of(k * 256, 256), 256)
        weights[0, k] = jnp.concatenate(
            [gate_ref[rows, :], zeros, wide_ref[rows, :], zeros], axis=1
        )
        cols = rows
        narrow[0, :, cols] = jnp.concatenate(
            [narrow_ref[:, cols], jnp.zeros((128 - 86, 256), BF)], axis=0
        )
        return carry

    lax.fori_loop(0, 16, widen, 0)
    weight_copy = send(weights.at[0], weights.at[1], sems, 22, partner)
    narrow_copy = send(narrow.at[0], narrow.at[1], sems, 23, partner)
    heads[pl.ds(kv, 1)] = normed_ref[...][None]
    gains[pl.ds(tp, 1)] = gain_ref[...][None]

    place = packed_ref[0:1, :]

    def chosen(start, rows):
        want = lax.broadcasted_iota(jnp.int32, (rows, 1024), 0) + start
        return jnp.where(want == place, 1.0, 0.0).astype(BF)

    own_rows = jnp.dot(chosen(64 * tp, 64), x_ref[...], preferred_element_type=F32)

    for copy in copies:
        copy.wait()
    all_heads = heads[...].reshape(1024, 256)
    for part in range(2):
        live = jnp.dot(chosen(256 * part, 256), all_heads, preferred_element_type=F32).astype(BF)
        partial[4 * part : 4 * part + 4] = (
            jnp.dot(live, result_ref[...], preferred_element_type=F32)
            .astype(BF)
            .reshape(4, 64, 256)
        )
    copies = []
    for i, (dx, dc) in enumerate(lines):
        peer = line_peer(at, dx, dc)
        copies.append(
            send(partial.at[2 * peer[2] + peer[3]], arrived.at[i], sems, 24 + i, peer)
        )
    for copy in gain_copies:
        copy.wait()
    gain = jnp.concatenate([gains[t, 0:1, 0:32] for t in range(8)], axis=1)
    attended = partial[tp].astype(F32)
    for i, copy in enumerate(copies):
        copy.wait()
        attended = attended + arrived[i].astype(F32)
    residual = (own_rows + attended).astype(BF).astype(F32)
    residual_ref[...] = residual
    own_squares = jnp.sum(residual * residual, axis=1, keepdims=True)
    squares[0] = jnp.broadcast_to(row_of(own_squares, 64), (8, 128))
    square_copies = [
        send(squares.at[0], squares.at[1 + i], sems, 31 + i, plane_peer(at, *d))
        for i, d in enumerate(planes)
    ]
    tile = (residual * gain).astype(BF)
    blocks = [tile[16 * i : 16 * i + 16, 128 * h : 128 * h + 128] for h in range(2) for i in range(4)]
    bufs = (ga, gb, gc)
    for p, (start, count, order) in enumerate(PARTS):
        idx = tuple(at[a] for a in order[::-1])
        for b in range(count):
            bufs[p][(*idx, b)] = blocks[start + b]
    gather_phase(at, bufs, 0, sems, 46)
    gather_phase(at, bufs, 1, sems, 58)
    for copy in square_copies:
        copy.wait()
    own_sum = jnp.sum(squares[...], axis=0)
    squares_sum[...] = own_sum
    squares_line[pl.ds(at["x"], 1)] = own_sum[None]
    line_copies = [
        send(squares_sum, squares_line.at[at["x"]], sems, 82 + dx - 1, line_peer(at, dx, 0))
        for dx in (1, 2, 3)
    ]
    gather_phase(at, bufs, 2, sems, 70)
    for copy in line_copies:
        copy.wait()
    weight_copy.wait()
    narrow_copy.wait()

    def rows_at(zz, yy):
        a, b, c = ga[zz, yy], gb[:, zz, yy], gc[yy, :, zz]
        v = jnp.concatenate([a, b, c], axis=1)
        return jnp.concatenate(
            [v[:, 0:4].reshape(256, 128), v[:, 4:8].reshape(256, 128)], axis=1
        )

    def widening(k, carry):
        lhs = rows_at(k // 4, k % 4)
        for core in range(2):
            term = jnp.dot(lhs, weights[core, k], preferred_element_type=F32)

            @pl.when(k == 0)
            def _():
                total[core] = term

            @pl.when(k > 0)
            def _():
                total[core] += term

        return carry

    lax.fori_loop(0, 16, widening, 0)
    scale = lax.rsqrt(
        jnp.concatenate([column_of(squares_line[g, 0:1, :], 64) for g in range(4)], axis=0)
        / 4096
        + EPS
    )
    hidden = []
    for core in range(2):
        gated = total[core, :, 0:128] * scale
        upward = total[core, :, 128:256] * scale
        hidden.append((gated * jax.nn.sigmoid(gated) * upward).astype(BF))
    hidden = jnp.concatenate(hidden, axis=1)
    pbufs = (pa, pb, pc)

    def narrowing(k, carry):
        cols = pl.ds(pl.multiple_of(k * 256, 256), 256)
        rhs = jnp.concatenate([narrow[0, :, cols], narrow[1, :, cols]], axis=0)
        term = jnp.dot(hidden, rhs, preferred_element_type=F32).astype(BF)
        v = jnp.concatenate(
            [term[:, 0:128].reshape(4, 4, 16, 128), term[:, 128:256].reshape(4, 4, 16, 128)], axis=1
        )
        zz, yy = k // 4, k % 4
        pa[zz, yy] = v[:, 0:3]
        pb[:, zz, yy] = v[:, 3:6]
        pc[yy, :, zz] = v[:, 6:8]
        return carry

    lax.fori_loop(0, 16, narrowing, 0)
    for n, phase in enumerate((2, 1, 0)):
        r = receive[12 * n : 12 * n + 12]
        reduce_phase(at, pbufs, phase, r[0:3], r[3:6], r[6:9], r[9:12], sems, 85 + 18 * n)
    sums = []
    for p, (start, count, order) in enumerate(PARTS):
        idx = tuple(at[a] for a in order[::-1])
        for b in range(count):
            sums.append(pbufs[p][(*idx, b)].astype(F32))
    mixed = []
    for h in range(2):
        for i in range(4):
            res = residual_ref[16 * i : 16 * i + 16, 128 * h : 128 * h + 128]
            mixed.append((res + sums[4 * h + i]).astype(BF))
    for t in range(8):
        h, lane = t // 4, 32 * (t % 4)
        ypack[t] = jnp.concatenate(
            [mixed[4 * h + i][:, lane : lane + 32] for i in range(4)], axis=1
        )
    copies = []
    for i, (dx, dc) in enumerate(lines):
        peer = line_peer(at, dx, dc)
        copies.append(
            send(ypack.at[2 * peer[2] + peer[3]], yarrive.at[tp], sems, 139 + i, peer)
        )
    yarrive[pl.ds(tp, 1)] = ypack[pl.ds(tp, 1)]
    for copy in copies:
        copy.wait()
    out_ref[...] = yarrive[...]


def mixer(normed, packed, x, result, gain, gate, wide, narrow):
    vmem = pl.BlockSpec(memory_space=pltpu.VMEM)
    counts = [count for _, count, _ in PARTS]
    boxes = [pltpu.VMEM((4, 4, 4, count, 16, 128), BF) for count in counts]
    receive = []
    for phase in (2, 1, 0):
        lead = (4,) * phase
        shapes = [(*lead, count, 16, 128) for count in counts]
        low = [pltpu.VMEM((s[0] // 2, *s[1:]), BF) for s in shapes]
        high = [pltpu.VMEM((s[0] - s[0] // 2, *s[1:]), BF) for s in shapes]
        full = [pltpu.VMEM(s, BF) for s in shapes]
        receive += low + high + full + full
    return pl.pallas_call(
        mixer_kernel,
        out_shape=jax.ShapeDtypeStruct((8, 16, 128), BF),
        in_specs=[vmem] * 8,
        out_specs=vmem,
        scratch_shapes=[
            pltpu.VMEM((16, 64, 256), BF),
            pltpu.VMEM((8, 64, 256), BF),
            pltpu.VMEM((7, 64, 256), BF),
            pltpu.VMEM((8, 8, 128), F32),
            pltpu.VMEM((64, 256), F32),
            pltpu.VMEM((16, 8, 128), F32),
            pltpu.VMEM((8, 128), F32),
            pltpu.VMEM((4, 8, 128), F32),
            pltpu.VMEM((2, 16, 256, 256), BF),
            pltpu.VMEM((2, 128, 4096), BF),
            pltpu.VMEM((2, 256, 256), F32),
            *boxes,
            *boxes,
            *receive,
            pltpu.VMEM((8, 16, 128), BF),
            pltpu.VMEM((8, 16, 128), BF),
            pltpu.SemaphoreType.DMA((146,)),
            pltpu.SemaphoreType.DMA((146,)),
        ],
        compiler_params=pltpu.CompilerParams(
            collective_id=0, has_side_effects=True, vmem_limit_bytes=48 * 1024 * 1024
        ),
        name="mixer",
    )(normed, packed, x, result, gain, gate, wide, narrow)


def spread_kernel(packed_ref, mixed_ref, out_ref):
    place = packed_ref[0:1, :]
    total = jnp.zeros((1024, 32), F32)
    j = lax.broadcasted_iota(jnp.int32, (128, 1024), 0)
    rows = 64 * (j // 16) + j % 16
    for a in range(4):
        chosen = jnp.where(rows + 16 * a == place, 1.0, 0.0).astype(BF)
        piece = mixed_ref[...].reshape(128, 128)[:, 32 * a : 32 * a + 32]
        total = total + lax.dot_general(
            chosen, piece, (((0,), (0,)), ((), ())), preferred_element_type=F32
        )
    out_ref[...] = total.astype(BF)


def spread(packed, mixed):
    vmem = pl.BlockSpec(memory_space=pltpu.VMEM)
    return pl.pallas_call(
        spread_kernel,
        out_shape=jax.ShapeDtypeStruct((1024, 32), BF),
        in_specs=[vmem] * 2,
        out_specs=vmem,
        name="spread",
    )(packed, mixed)


def places_of_live_rows(lengths):
    order = jnp.arange(128, dtype=jnp.int32)
    starts = jnp.sum(jnp.where(order[:, None] < order[None, :], lengths[:, None], 0), axis=0)
    slot = jnp.arange(FRESH_PLACES, dtype=jnp.int32)[None, :]
    place = jnp.where(slot < lengths[:, None], starts[:, None] + slot, -1)
    return jnp.broadcast_to(place.reshape(1, 1024), (8, 1024))


def local(
    residual_entries,
    fresh_extents,
    memory_matrix,
    initial_rescale_vector,
    probe_matrix,
    retain_matrix,
    content_matrix,
    result_switch_matrix,
    retain_lower_limit,
    extra_shrink_log,
    lane_result_rescale,
    result_matrix,
    later_rescale_vector,
    mixer_switch_matrix,
    widening_matrix,
    narrowing_matrix,
):
    sequences_per_device = memory_matrix.shape[0]
    heads_per_device = memory_matrix.shape[1]
    rows_dev = sequences_per_device * FRESH_PLACES
    all_rows = residual_entries.shape[0]
    kv_index = lax.axis_index(KV)
    tokens_wide = residual_entries.astype(jnp.float32)
    columns = gather_directly(residual_entries, TP, 1)
    col_wide = columns.astype(jnp.float32)
    own_squares = sum_at_owner(jnp.sum(col_wide * col_wide, axis=1), KV, 0)
    first_scale = lax.rsqrt(own_squares / D + epsilon)
    scaled = (columns.astype(jnp.float32) * initial_rescale_vector).astype(jnp.bfloat16)
    projected = (
        own_rows(
            jnp.concatenate(
                [
                    jnp.dot(scaled, weight, preferred_element_type=jnp.float32)
                    for weight in (
                        probe_matrix,
                        retain_matrix,
                        content_matrix,
                        result_switch_matrix,
                    )
                ],
                axis=1,
            ),
            KV,
        )
        * first_scale[:, None]
    )
    width_dev = probe_matrix.shape[1]
    shape_four = (sequences_per_device, FRESH_PLACES, heads_per_device, HEAD)
    z_query = projected[:, :width_dev]
    z_forget = projected[:, width_dev : 2 * width_dev].reshape(shape_four)
    z_input = projected[:, 2 * width_dev : 3 * width_dev].reshape(shape_four)
    z_outgate = projected[:, 3 * width_dev :]
    own_lengths = lax.dynamic_slice_in_dim(
        fresh_extents, kv_index * sequences_per_device, sequences_per_device
    )
    living = jnp.arange(FRESH_PLACES, dtype=jnp.int32)[None, :] < own_lengths[:, None]
    query = jax.nn.silu(z_query).reshape(shape_four)
    bounds = retain_lower_limit.reshape(heads_per_device, HEAD)
    retain_factor = bounds + (1.0 - bounds) * jax.nn.sigmoid(z_forget)
    shrink_exponent = jnp.log(retain_factor) + extra_shrink_log.reshape(
        sequences_per_device, FRESH_PLACES, heads_per_device, 1
    )
    decays = jnp.where(living[:, :, None, None], jnp.exp(shrink_exponent), 1.0)
    key_gate = jnp.where(living[:, :, None, None], 1.0 - retain_factor, 0.0)
    carried = memory_matrix
    outputs = []
    for position in range(FRESH_PLACES):
        carried = (
            decays[:, position, :, :, None] * carried
            + key_gate[:, position, :, :, None] * z_input[:, position, :, None, :]
        )
        outputs.append(
            jnp.einsum(
                "bhd,bhdv->bhv", query[:, position], carried, precision=lax.Precision.HIGHEST
            )
        )
    heads_out = jnp.stack(outputs, axis=1)
    heads_out = (
        heads_out
        * lax.rsqrt(jnp.mean(heads_out * heads_out, axis=-1, keepdims=True) + epsilon)
        * lane_result_rescale
    )
    normed = jnp.where(
        living.reshape(rows_dev)[:, None],
        heads_out.reshape(rows_dev, width_dev) * jax.nn.silu(z_outgate),
        0.0,
    ).astype(jnp.bfloat16)
    packed = places_of_live_rows(fresh_extents)
    gain = jnp.broadcast_to(jnp.pad(later_rescale_vector, (0, 96))[None], (8, 128))
    mixed = mixer(
        normed,
        packed,
        columns,
        result_matrix,
        gain,
        mixer_switch_matrix,
        widening_matrix,
        narrowing_matrix,
    )
    return (spread(packed, mixed), carried)


def solution(mesh):
    torus = Mesh(mesh.devices.reshape(4, 4, 4, 2), ("kv_0", "kv_1", "tp_0", "tp_1"))
    placed = (
        P(None, KV_TP),
        P(),
        P(KV, TP, None, None),
        P(KV),
        P(KV, TP),
        P(KV, TP),
        P(KV, TP),
        P(KV, TP),
        P(TP),
        P(KV, TP),
        P(),
        P(TP, KV),
        P(KV_TP),
        P(None, KV_TP),
        P(None, KV_TP),
        P(KV_TP, None),
    )
    return jax.shard_map(
        local,
        mesh=torus,
        in_specs=placed,
        out_specs=(P(None, KV_TP), P(KV, TP, None, None)),
        check_vma=False,
    )
```

```python
import jax
import jax.numpy as jnp
from jax import lax
from jax.experimental import pallas as pl
from jax.experimental.pallas import tpu as pltpu
from jax.sharding import Mesh
from jax.sharding import PartitionSpec as P

KV = ("kv_0", "kv_1")
TP = ("tp_0", "tp_1")
KV_TP = ("kv_0", "kv_1", "tp_0", "tp_1")
MESH = pl.DeviceIdType.MESH
EPS = 1e-06
F32 = jnp.float32
BF = jnp.bfloat16
PARTS = ((0, 3), (3, 3), (6, 2))
ORDERS = ("xyz", "yzx", "zxy")
PLANE_ORDERS = ("zy", "yz")


def my_position():
    return dict(
        z=lax.axis_index("kv_0"),
        y=lax.axis_index("kv_1"),
        x=lax.axis_index("tp_0"),
        c=lax.axis_index("tp_1"),
    )


def device_at(at, **moved):
    there = dict(at, **moved)
    return (there["z"], there["y"], there["x"], there["c"])


def plane_offsets():
    return [(dz, dy) for dz in range(4) for dy in range(4) if dz or dy]


def line_offsets():
    return [(dx, dc) for dx in range(4) for dc in range(2) if dx or dc]


def plane_peer(at, dz, dy):
    return device_at(at, z=(at["z"] + dz) % 4, y=(at["y"] + dy) % 4)


def line_peer(at, dx, dc):
    return device_at(at, x=(at["x"] + dx) % 4, c=(at["c"] + dc) % 2)


def meet(peers):
    barrier = pltpu.get_barrier_semaphore()
    for peer in peers:
        pl.semaphore_signal(barrier, inc=1, device_id=peer, device_id_type=MESH)
    pl.semaphore_wait(barrier, len(peers))


def send(src, dst, sems, i, peer):
    copy = pltpu.make_async_remote_copy(
        src_ref=src,
        dst_ref=dst,
        send_sem=sems[0].at[i],
        recv_sem=sems[1].at[i],
        device_id=peer,
        device_id_type=MESH,
    )
    copy.start()
    return copy


def times(a, b, dims=((1,), (1,))):
    return lax.dot_general(a, b, (dims, ((), ())), preferred_element_type=F32)


def row_of(column, rows):
    eye = lax.broadcasted_iota(jnp.int32, (rows, 128), 0) == lax.broadcasted_iota(
        jnp.int32, (rows, 128), 1
    )
    return jnp.sum(jnp.where(eye, column, 0.0), axis=0, keepdims=True)


def column_of(row, rows):
    eye = lax.broadcasted_iota(jnp.int32, (rows, 128), 0) == lax.broadcasted_iota(
        jnp.int32, (rows, 128), 1
    )
    return jnp.sum(jnp.where(eye, row, 0.0), axis=1, keepdims=True)


def picks(place, start, rows):
    want = lax.broadcasted_iota(jnp.int32, (rows, 1024), 0) + start
    return jnp.where(want == place, 1.0, 0.0).astype(BF)


def halves(length):
    return pl.ds(0, length // 2), pl.ds(length // 2, length - length // 2)


def gather_phase(at, bufs, parts, phase, sems, base):
    first = []
    for p, order in enumerate(parts):
        axis = order[phase]
        pre = tuple(at[a] for a in order[:phase:-1])
        m = at[axis]
        up, down = (m + 1) % 4, (m + 3) % 4
        own = bufs[p].at[(*pre, m)]
        i = base + 4 * p
        first.append((
            send(own, own, sems, i, device_at(at, **{axis: up})),
            send(own, own, sems, i + 1, device_at(at, **{axis: down})),
        ))
    second = []
    for p, order in enumerate(parts):
        axis = order[phase]
        pre = tuple(at[a] for a in order[:phase:-1])
        m = at[axis]
        up, down = (m + 1) % 4, (m + 3) % 4
        lo, hi = halves(bufs[p].shape[len(pre) + 1])
        i = base + 4 * p
        first[p][0].wait_recv()
        from_down = bufs[p].at[(*pre, down, lo)]
        a = send(from_down, from_down, sems, i + 2, device_at(at, **{axis: up}))
        first[p][1].wait_recv()
        from_up = bufs[p].at[(*pre, up, hi)]
        b = send(from_up, from_up, sems, i + 3, device_at(at, **{axis: down}))
        second.append((a, b))
    for p in range(len(parts)):
        for copy in first[p]:
            copy.wait_send()
        for copy in second[p]:
            copy.wait()


def add_into(ref, idx, terms):
    total = ref[idx].astype(F32)
    for term in terms:
        total = total + term.astype(F32)
    ref[idx] = total.astype(BF)


def reduce_phase(at, bufs, parts, phase, one_up, one_down, two_up, two_down, sems, base, keep=True):
    early = []
    for p, order in enumerate(parts):
        axis = order[phase]
        pre = tuple(at[a] for a in order[:phase:-1])
        m = at[axis]
        up, down, far = (m + 1) % 4, (m + 3) % 4, (m + 2) % 4
        to_up, to_down = device_at(at, **{axis: up}), device_at(at, **{axis: down})
        lo, hi = halves(bufs[p].shape[len(pre) + 1])
        i = base + 6 * p
        early.append((
            send(bufs[p].at[(*pre, far, lo)], one_up[p], sems, i, to_up),
            send(bufs[p].at[(*pre, far, hi)], one_down[p], sems, i + 1, to_down),
            send(bufs[p].at[(*pre, up, hi)], two_up[p].at[hi], sems, i + 2, to_up),
            send(bufs[p].at[(*pre, down, lo)], two_down[p].at[lo], sems, i + 3, to_down),
        ))
    late = []
    for p, order in enumerate(parts):
        axis = order[phase]
        pre = tuple(at[a] for a in order[:phase:-1])
        m = at[axis]
        up, down = (m + 1) % 4, (m + 3) % 4
        to_up, to_down = device_at(at, **{axis: up}), device_at(at, **{axis: down})
        lo, hi = halves(bufs[p].shape[len(pre) + 1])
        i = base + 6 * p
        early[p][0].wait_recv()
        add_into(bufs[p], (*pre, up, lo), [one_up[p][...]])
        a = send(bufs[p].at[(*pre, up, lo)], two_up[p].at[lo], sems, i + 4, to_up)
        early[p][1].wait_recv()
        add_into(bufs[p], (*pre, down, hi), [one_down[p][...]])
        b = send(bufs[p].at[(*pre, down, hi)], two_down[p].at[hi], sems, i + 5, to_down)
        late.append((a, b))
    sums = []
    for p, order in enumerate(parts):
        axis = order[phase]
        pre = tuple(at[a] for a in order[:phase:-1])
        for copy in early[p][2:]:
            copy.wait_recv()
        for copy in late[p]:
            copy.wait_recv()
        for copy in (*early[p], *late[p]):
            copy.wait_send()
        own = (*pre, at[axis])
        total = bufs[p][own].astype(F32) + two_up[p][...].astype(F32) + two_down[p][...].astype(F32)
        if keep:
            bufs[p][own] = total.astype(BF)
        sums.append(total)
    return sums


def mixer_kernel(
    normed_ref, packed_ref, x_ref, result_ref, gain_ref, gate_ref, wide_ref, narrow_ref,
    out_ref,
    heads, partial, arrived, own_gain, gains, residual_ref, squares, squares_sum, squares_line,
    weights, narrow, total, ga, gb, gc,
    *rest,
):
    (pa, pb, pc), rest = rest[:3], rest[3:]
    receive, rest = rest[:36], rest[36:]
    ypack, yarrive, sends, recvs = rest
    sems = (sends, recvs)
    at = my_position()
    kv = 4 * at["z"] + at["y"]
    tp = 2 * at["x"] + at["c"]
    planes, lines = plane_offsets(), line_offsets()
    meet([plane_peer(at, *d) for d in planes] + [line_peer(at, *d) for d in lines])

    copies = [
        send(normed_ref, heads.at[kv], sems, i, plane_peer(at, *d)) for i, d in enumerate(planes)
    ]
    own_gain[...] = jnp.broadcast_to(
        jnp.concatenate([gain_ref[...], jnp.zeros((1, 96), F32)], axis=1), (8, 128)
    )
    gain_copies = [
        send(own_gain, gains.at[tp], sems, 15 + i, line_peer(at, *d)) for i, d in enumerate(lines)
    ]
    partner = line_peer(at, 0, 1)
    for slot, start in ((0, 80), (1, 96)):
        weights[slot, :, start:128] = jnp.zeros((2, 128 - start, 4096), BF)
        narrow[slot, start:128] = jnp.zeros((128 - start, 4096), BF)
    weights[0, 0, 0:86] = gate_ref[...]
    weights[0, 1, 0:86] = wide_ref[...]
    narrow[0, 0:86] = narrow_ref[...]
    weight_copy = send(weights.at[0, :, 0:96], weights.at[1, :, 0:96], sems, 22, partner)
    narrow_copy = send(narrow.at[0, 0:96], narrow.at[1, 0:96], sems, 23, partner)
    heads[pl.ds(kv, 1)] = normed_ref[...][None]
    gains[pl.ds(tp, 1)] = own_gain[...][None]

    place = packed_ref[0:1, :]

    def chosen(start, rows):
        return picks(place, start, rows)

    for copy in copies:
        copy.wait()
    all_heads = heads[...].reshape(1024, 256)
    for part in range(2):
        live = jnp.dot(chosen(256 * part, 256), all_heads, preferred_element_type=F32).astype(BF)
        partial[4 * part : 4 * part + 4] = (
            jnp.dot(live, result_ref[...], preferred_element_type=F32)
            .astype(BF)
            .reshape(4, 64, 256)
        )
    copies = []
    for i, (dx, dc) in enumerate(lines):
        peer = line_peer(at, dx, dc)
        copies.append(
            send(partial.at[2 * peer[2] + peer[3]], arrived.at[i], sems, 24 + i, peer)
        )
    for copy in gain_copies:
        copy.wait()
    gain = jnp.concatenate([gains[t, 0:1, 0:32] for t in range(8)], axis=1)
    attended = partial[tp].astype(F32)
    for i, copy in enumerate(copies):
        copy.wait()
        attended = attended + arrived[i].astype(F32)
    residual = (x_ref[...].astype(F32) + attended).astype(BF).astype(F32)
    residual_ref[...] = residual
    own_squares = jnp.sum(residual * residual, axis=1, keepdims=True)
    squares[0] = jnp.broadcast_to(row_of(own_squares, 64), (8, 128))
    square_copies = [
        send(squares.at[0], squares.at[1 + i], sems, 31 + i, plane_peer(at, *d))
        for i, d in enumerate(planes)
    ]
    tile = (residual * gain).astype(BF)
    blocks = [tile[16 * i : 16 * i + 16, 128 * h : 128 * h + 128] for h in range(2) for i in range(4)]
    bufs = (ga, gb, gc)
    for p, ((start, count), order) in enumerate(zip(PARTS, ORDERS)):
        idx = tuple(at[a] for a in order[::-1])
        for b in range(count):
            bufs[p][(*idx, b)] = blocks[start + b]
    gather_phase(at, bufs, ORDERS, 0, sems, 46)
    gather_phase(at, bufs, ORDERS, 1, sems, 58)
    for copy in square_copies:
        copy.wait()
    own_sum = jnp.sum(squares[...], axis=0)
    squares_sum[...] = own_sum
    squares_line[pl.ds(at["x"], 1)] = own_sum[None]
    line_copies = [
        send(squares_sum, squares_line.at[at["x"]], sems, 82 + dx - 1, line_peer(at, dx, 0))
        for dx in (1, 2, 3)
    ]
    gather_phase(at, bufs, ORDERS, 2, sems, 70)
    for copy in line_copies:
        copy.wait()
    weight_copy.wait()
    narrow_copy.wait()

    def rows_at(zz, yy):
        a, b, c = ga[zz, yy], gb[:, zz, yy], gc[yy, :, zz]
        v = jnp.concatenate([a, b, c], axis=1)
        return jnp.concatenate(
            [v[:, 0:4].reshape(256, 128), v[:, 4:8].reshape(256, 128)], axis=1
        )

    def widening(k, carry):
        lhs = rows_at(k // 4, k % 4)
        cols = pl.ds(pl.multiple_of(k * 256, 256), 256)
        for core in range(2):
            term = times(lhs, weights[core, :, :, cols].reshape(256, 256))

            @pl.when(k == 0)
            def _():
                total[core] = term

            @pl.when(k > 0)
            def _():
                total[core] += term

        return carry

    lax.fori_loop(0, 16, widening, 0)
    scale = lax.rsqrt(
        jnp.concatenate([column_of(squares_line[g, 0:1, :], 64) for g in range(4)], axis=0)
        / 4096
        + EPS
    )
    hidden = []
    for core in range(2):
        gated = total[core, :, 0:128] * scale
        upward = total[core, :, 128:256] * scale
        hidden.append((gated * jax.nn.sigmoid(gated) * upward).astype(BF))
    hidden = jnp.concatenate(hidden, axis=1)
    pbufs = (pa, pb, pc)

    def narrowing(k, carry):
        cols = pl.ds(pl.multiple_of(k * 256, 256), 256)
        rhs = jnp.concatenate([narrow[0, :, cols], narrow[1, :, cols]], axis=0)
        term = jnp.dot(hidden, rhs, preferred_element_type=F32).astype(BF)
        v = jnp.concatenate(
            [term[:, 0:128].reshape(4, 4, 16, 128), term[:, 128:256].reshape(4, 4, 16, 128)], axis=1
        )
        zz, yy = k // 4, k % 4
        pa[zz, yy] = v[:, 0:3]
        pb[:, zz, yy] = v[:, 3:6]
        pc[yy, :, zz] = v[:, 6:8]
        return carry

    lax.fori_loop(0, 16, narrowing, 0)
    for n, phase in enumerate((2, 1, 0)):
        r = receive[12 * n : 12 * n + 12]
        sums = reduce_phase(
            at, pbufs, ORDERS, phase, r[0:3], r[3:6], r[6:9], r[9:12], sems, 85 + 18 * n, phase > 0
        )
    sums = jnp.concatenate(sums, axis=0)
    mixed = []
    for h in range(2):
        for i in range(4):
            res = residual_ref[16 * i : 16 * i + 16, 128 * h : 128 * h + 128]
            mixed.append((res + sums[4 * h + i]).astype(BF))
    for t in range(8):
        h, lane = t // 4, 32 * (t % 4)
        ypack[t] = jnp.concatenate(
            [mixed[4 * h + i][:, lane : lane + 32] for i in range(4)], axis=1
        )
    copies = []
    for i, (dx, dc) in enumerate(lines):
        peer = line_peer(at, dx, dc)
        copies.append(
            send(ypack.at[2 * peer[2] + peer[3]], yarrive.at[tp], sems, 139 + i, peer)
        )
    yarrive[pl.ds(tp, 1)] = ypack[pl.ds(tp, 1)]
    for copy in copies:
        copy.wait()
    out_ref[...] = yarrive[...]


def mixer(normed, packed, x, result, gain, gate, wide, narrow):
    vmem = pl.BlockSpec(memory_space=pltpu.VMEM)
    counts = [count for _, count in PARTS]
    boxes = [pltpu.VMEM((4, 4, 4, count, 16, 128), BF) for count in counts]
    receive = []
    for phase in (2, 1, 0):
        lead = (4,) * phase
        shapes = [(*lead, count, 16, 128) for count in counts]
        low = [pltpu.VMEM((s[0] // 2, *s[1:]), BF) for s in shapes]
        high = [pltpu.VMEM((s[0] - s[0] // 2, *s[1:]), BF) for s in shapes]
        full = [pltpu.VMEM(s, BF) for s in shapes]
        receive += low + high + full + full
    return pl.pallas_call(
        mixer_kernel,
        out_shape=jax.ShapeDtypeStruct((8, 16, 128), BF),
        in_specs=[vmem] * 8,
        out_specs=vmem,
        scratch_shapes=[
            pltpu.VMEM((16, 64, 256), BF),
            pltpu.VMEM((8, 64, 256), BF),
            pltpu.VMEM((7, 64, 256), BF),
            pltpu.VMEM((8, 128), F32),
            pltpu.VMEM((8, 8, 128), F32),
            pltpu.VMEM((64, 256), F32),
            pltpu.VMEM((16, 8, 128), F32),
            pltpu.VMEM((8, 128), F32),
            pltpu.VMEM((4, 8, 128), F32),
            pltpu.VMEM((2, 2, 128, 4096), BF),
            pltpu.VMEM((2, 128, 4096), BF),
            pltpu.VMEM((2, 256, 256), F32),
            *boxes,
            *boxes,
            *receive,
            pltpu.VMEM((8, 16, 128), BF),
            pltpu.VMEM((8, 16, 128), BF),
            pltpu.SemaphoreType.DMA((146,)),
            pltpu.SemaphoreType.DMA((146,)),
        ],
        compiler_params=pltpu.CompilerParams(
            collective_id=0, has_side_effects=True, vmem_limit_bytes=48 * 1024 * 1024
        ),
        name="mixer",
    )(normed, packed, x, result, gain, gate, wide, narrow)


def spread_kernel(packed_ref, mixed_ref, out_ref):
    place = packed_ref[0:1, :]
    total = jnp.zeros((32, 1024), F32)
    j = lax.broadcasted_iota(jnp.int32, (128, 1024), 0)
    rows = 64 * (j // 16) + j % 16
    for a in range(4):
        chosen = jnp.where(rows + 16 * a == place, 1.0, 0.0).astype(BF)
        piece = mixed_ref[...].reshape(128, 128)[:, 32 * a : 32 * a + 32]
        total = total + times(piece, chosen, ((0,), (0,)))
    out_ref[...] = total.astype(BF)


def spread(packed, mixed):
    vmem = pl.BlockSpec(memory_space=pltpu.VMEM)
    return pl.pallas_call(
        spread_kernel,
        out_shape=jax.ShapeDtypeStruct((32, 1024), BF),
        in_specs=[vmem] * 2,
        out_specs=vmem,
        name="spread",
    )(packed, mixed)


def front_kernel(
    x_ref, lengths_ref, gain_ref, wq_ref, wf_ref, wi_ref, wo_ref,
    z_ref, xt_ref, packed_ref,
    cols, scaled, squares, squares_in, pa, pb, *rest,
):
    receive, (sends, recvs) = rest[:16], rest[16:]
    sems = (sends, recvs)
    at = my_position()
    kv = 4 * at["z"] + at["y"]
    tp = 2 * at["x"] + at["c"]
    planes, lines = plane_offsets(), line_offsets()
    meet([plane_peer(at, *d) for d in planes] + [line_peer(at, *d) for d in lines])
    copies = [
        send(x_ref, cols.at[tp], sems, i, line_peer(at, *d)) for i, d in enumerate(lines)
    ]
    cols[pl.ds(tp, 1)] = x_ref[...][None]
    lengths = jnp.broadcast_to(lengths_ref[...], (8, 128)).astype(F32).astype(BF)
    s = lax.broadcasted_iota(jnp.int32, (128, 1024), 0)
    owner = lax.broadcasted_iota(jnp.int32, (128, 1024), 1) // 8
    start = times(lengths, jnp.where(s < owner, 1.0, 0.0).astype(BF), ((1,), (0,)))
    length = times(lengths, jnp.where(s == owner, 1.0, 0.0).astype(BF), ((1,), (0,)))
    slot = lax.broadcasted_iota(jnp.int32, (8, 1024), 1) % 8
    place = jnp.where(
        slot < length.astype(jnp.int32), start.astype(jnp.int32) + slot, -1
    )
    packed_ref[...] = place
    gain = jnp.concatenate(
        [column_of(gain_ref[:, 0:128], 128), column_of(gain_ref[:, 128:256], 128)], axis=0
    )
    mine = picks(place[0:1, :], 64 * tp, 64)
    for copy in copies:
        copy.wait()
    xt_ref[...] = times(mine, cols[...].reshape(256, 1024)).astype(BF)
    for k in range(8):
        lanes = slice(128 * k, 128 * k + 128)
        v = cols[:, :, lanes].reshape(256, 128).astype(F32)
        scaled[:, lanes] = (v * gain).astype(BF)
        squares[k] = jnp.broadcast_to(jnp.sum(v * v, axis=0, keepdims=True), (8, 128))
    square_copies = []
    for i, (dz, dy) in enumerate(planes):
        peer = plane_peer(at, dz, dy)
        square_copies.append(
            send(squares.at[(4 * peer[0] + peer[1]) // 2], squares_in.at[i], sems, 7 + i, peer)
        )

    def project(a, carry):
        lhs = scaled[:, pl.ds(pl.multiple_of(256 * a, 256), 256)]
        for n, (first, second) in enumerate(((wq_ref, wf_ref), (wi_ref, wo_ref))):
            for half, weight in enumerate((first, second)):
                lanes = slice(256 * half, 256 * half + 256)
                v = times(lhs, weight[...], ((0,), (0,))).astype(BF).reshape(4, 64, 256)
                if n == 0:
                    pa[:, a, :, lanes] = v
                else:
                    pb[a, :, :, lanes] = v
        return carry

    lax.fori_loop(0, 4, project, 0)
    bufs = (pa, pb)
    r = receive
    reduce_phase(at, bufs, PLANE_ORDERS, 1, r[0:2], r[2:4], r[4:6], r[6:8], sems, 22)
    r = receive[8:]
    sums = reduce_phase(
        at, bufs, PLANE_ORDERS, 0, r[0:2], r[2:4], r[4:6], r[6:8], sems, 34, False
    )
    for copy in square_copies:
        copy.wait()
    total = jnp.sum(squares_in[...], axis=0) + squares[kv // 2]
    shift = 64 * (kv % 2)
    eye = lax.broadcasted_iota(jnp.int32, (64, 128), 1) == shift + lax.broadcasted_iota(
        jnp.int32, (64, 128), 0
    )
    own = jnp.sum(jnp.where(eye, total[0:1, :], 0.0), axis=1, keepdims=True)
    scale = lax.rsqrt(own / 4096 + EPS)
    z_ref[:, 0:512] = sums[0] * scale
    z_ref[:, 512:1024] = sums[1] * scale


def front(x, lengths, gain, wq, wf, wi, wo):
    vmem = pl.BlockSpec(memory_space=pltpu.VMEM)
    receive = []
    for phase in (1, 0):
        shape = (*(4,) * phase, 64, 512)
        half = pltpu.VMEM((shape[0] // 2, *shape[1:]), BF)
        receive += [half] * 4 + [pltpu.VMEM(shape, BF)] * 4
    return pl.pallas_call(
        front_kernel,
        out_shape=(
            jax.ShapeDtypeStruct((64, 1024), F32),
            jax.ShapeDtypeStruct((64, 256), BF),
            jax.ShapeDtypeStruct((8, 1024), jnp.int32),
        ),
        in_specs=[vmem] * 7,
        out_specs=(vmem,) * 3,
        scratch_shapes=[
            pltpu.VMEM((8, 32, 1024), BF),
            pltpu.VMEM((256, 1024), BF),
            pltpu.VMEM((8, 8, 128), F32),
            pltpu.VMEM((15, 8, 128), F32),
            pltpu.VMEM((4, 4, 64, 512), BF),
            pltpu.VMEM((4, 4, 64, 512), BF),
            *receive,
            pltpu.SemaphoreType.DMA((46,)),
            pltpu.SemaphoreType.DMA((46,)),
        ],
        compiler_params=pltpu.CompilerParams(
            collective_id=1, has_side_effects=True, vmem_limit_bytes=32 * 1024 * 1024
        ),
        name="front",
    )(x, lengths, gain, wq, wf, wi, wo)


def recurrence_kernel(
    z_ref, bound_ref, shrink_ref, lengths_ref, lane_gain_ref, state_ref,
    normed_ref, new_ref,
    decay, gate, query, output,
):
    step = pl.program_id(0)
    kv = 4 * lax.axis_index("kv_0") + lax.axis_index("kv_1")
    row = lax.broadcasted_iota(jnp.int32, (64, 128), 0)
    lane = lax.broadcasted_iota(jnp.int32, (64, 128), 1)
    length = jnp.sum(
        jnp.where(lane == 8 * kv + row // 8, lengths_ref[...].astype(F32), 0.0),
        axis=1,
        keepdims=True,
    )
    live = (row[:, 0:1] % 8).astype(F32) < length

    @pl.when(step == 0)
    def _():
        bound = bound_ref[...]
        retain = bound + (1.0 - bound) * jax.nn.sigmoid(z_ref[:, 256:512])
        for h in range(2):
            lanes = slice(128 * h, 128 * h + 128)
            shrink = jnp.sum(
                jnp.where(lane[:, 0:64] == row[:, 0:64], shrink_ref[h : h + 1, :], 0.0),
                axis=1,
                keepdims=True,
            )
            kept = jnp.exp(jnp.log(retain[:, lanes]) + shrink)
            decay[:, lanes] = jnp.where(live, kept, 1.0)
            gate[:, lanes] = jnp.where(live, 1.0 - retain[:, lanes], 0.0)
        zq = z_ref[:, 0:256]
        query[...] = zq * jax.nn.sigmoid(zq)

    rows = pl.ds(pl.multiple_of(8 * step, 8), 8)
    for h in range(2):
        lanes = slice(128 * h, 128 * h + 128)
        d, k, q = decay[rows, lanes].T, gate[rows, lanes].T, query[rows, lanes].T
        value = z_ref[rows, 512 + 128 * h : 640 + 128 * h]
        state = state_ref[0, h]
        outs = []
        for j in range(8):
            state = d[:, j : j + 1] * state + k[:, j : j + 1] * value[j : j + 1, :]
            outs.append(jnp.sum(q[:, j : j + 1] * state, axis=0, keepdims=True))
        new_ref[0, h] = state
        output[rows, lanes] = jnp.concatenate(outs, axis=0)

    @pl.when(step == 7)
    def _():
        for h in range(2):
            lanes = slice(128 * h, 128 * h + 128)
            o = output[:, lanes]
            zo = z_ref[:, 768 + 128 * h : 896 + 128 * h]
            o = o * lax.rsqrt(jnp.mean(o * o, axis=1, keepdims=True) + EPS) * lane_gain_ref[...]
            normed_ref[:, lanes] = jnp.where(live, o * (zo * jax.nn.sigmoid(zo)), 0.0).astype(BF)


def recurrence(z, bound, shrink, lengths, lane_gain, state):
    def whole(*shape):
        return pl.BlockSpec(shape, lambda s: (0,) * len(shape))

    one = pl.BlockSpec((1, 2, 128, 128), lambda s: (s, 0, 0, 0))
    return pl.pallas_call(
        recurrence_kernel,
        out_shape=(
            jax.ShapeDtypeStruct((64, 256), BF),
            jax.ShapeDtypeStruct((8, 2, 128, 128), F32),
        ),
        grid=(8,),
        in_specs=[whole(64, 1024), whole(1, 256), whole(2, 64), whole(1, 128), whole(1, 128), one],
        out_specs=(whole(64, 256), one),
        scratch_shapes=[pltpu.VMEM((64, 256), F32)] * 4,
        name="recurrence",
    )(z, bound, shrink, lengths, lane_gain, state)


def local(
    residual_entries,
    fresh_extents,
    memory_matrix,
    initial_rescale_vector,
    probe_matrix,
    retain_matrix,
    content_matrix,
    result_switch_matrix,
    retain_lower_limit,
    extra_shrink_log,
    lane_result_rescale,
    result_matrix,
    later_rescale_vector,
    mixer_switch_matrix,
    widening_matrix,
    narrowing_matrix,
):
    lengths = fresh_extents.reshape(1, 128)
    z, xt, packed = front(
        residual_entries.T,
        lengths,
        initial_rescale_vector.reshape(1, 256),
        probe_matrix,
        retain_matrix,
        content_matrix,
        result_switch_matrix,
    )
    normed, carried = recurrence(
        z,
        retain_lower_limit.reshape(1, 256),
        extra_shrink_log.T,
        lengths,
        lane_result_rescale.reshape(1, 128),
        memory_matrix,
    )
    mixed = mixer(
        normed,
        packed,
        xt,
        result_matrix,
        later_rescale_vector.reshape(1, 32),
        mixer_switch_matrix.T,
        widening_matrix.T,
        narrowing_matrix,
    )
    return (spread(packed, mixed).T, carried)


def solution(mesh):
    torus = Mesh(mesh.devices.reshape(4, 4, 4, 2), ("kv_0", "kv_1", "tp_0", "tp_1"))
    placed = (
        P(None, KV_TP),
        P(),
        P(KV, TP, None, None),
        P(KV),
        P(KV, TP),
        P(KV, TP),
        P(KV, TP),
        P(KV, TP),
        P(TP),
        P(KV, TP),
        P(),
        P(TP, KV),
        P(KV_TP),
        P(None, KV_TP),
        P(None, KV_TP),
        P(KV_TP, None),
    )
    return jax.shard_map(
        local,
        mesh=torus,
        in_specs=placed,
        out_specs=(P(None, KV_TP), P(KV, TP, None, None)),
        check_vma=False,
    )
```

```python
import jax
import jax.numpy as jnp
from jax import lax
from jax.experimental import pallas as pl
from jax.experimental.pallas import tpu as pltpu
from jax.sharding import Mesh
from jax.sharding import PartitionSpec as P

KV = ("kv_0", "kv_1")
TP = ("tp_0", "tp_1")
KV_TP = ("kv_0", "kv_1", "tp_0", "tp_1")
MESH = pl.DeviceIdType.MESH
EPS = 1e-06
F32 = jnp.float32
BF = jnp.bfloat16
PARTS = ((0, 3), (3, 3), (6, 2))
ORDERS = ("xyz", "yzx", "zxy")
PLANE_ORDERS = ("zy", "yz")


def my_position():
    return dict(
        z=lax.axis_index("kv_0"),
        y=lax.axis_index("kv_1"),
        x=lax.axis_index("tp_0"),
        c=lax.axis_index("tp_1"),
    )


def device_at(at, **moved):
    there = dict(at, **moved)
    return (there["z"], there["y"], there["x"], there["c"])


def plane_offsets():
    return [(dz, dy) for dz in range(4) for dy in range(4) if dz or dy]


def line_offsets():
    return [(dx, dc) for dx in range(4) for dc in range(2) if dx or dc]


def plane_peer(at, dz, dy):
    return device_at(at, z=(at["z"] + dz) % 4, y=(at["y"] + dy) % 4)


def line_peer(at, dx, dc):
    return device_at(at, x=(at["x"] + dx) % 4, c=(at["c"] + dc) % 2)


def meet(peers):
    barrier = pltpu.get_barrier_semaphore()
    for peer in peers:
        pl.semaphore_signal(barrier, inc=1, device_id=peer, device_id_type=MESH)
    pl.semaphore_wait(barrier, len(peers))


def send(src, dst, sems, i, peer):
    copy = pltpu.make_async_remote_copy(
        src_ref=src,
        dst_ref=dst,
        send_sem=sems[0].at[i],
        recv_sem=sems[1].at[i],
        device_id=peer,
        device_id_type=MESH,
    )
    copy.start()
    return copy


def times(a, b, dims=((1,), (1,))):
    return lax.dot_general(a, b, (dims, ((), ())), preferred_element_type=F32)


def row_of(column, rows):
    eye = lax.broadcasted_iota(jnp.int32, (rows, 128), 0) == lax.broadcasted_iota(
        jnp.int32, (rows, 128), 1
    )
    return jnp.sum(jnp.where(eye, column, 0.0), axis=0, keepdims=True)


def column_of(row, rows):
    eye = lax.broadcasted_iota(jnp.int32, (rows, 128), 0) == lax.broadcasted_iota(
        jnp.int32, (rows, 128), 1
    )
    return jnp.sum(jnp.where(eye, row, 0.0), axis=1, keepdims=True)


def picks(place, start, rows):
    want = lax.broadcasted_iota(jnp.int32, (rows, 1024), 0) + start
    return jnp.where(want == place, 1.0, 0.0).astype(BF)


def halves(length):
    return pl.ds(0, length // 2), pl.ds(length // 2, length - length // 2)


def gather_phase(at, bufs, parts, phase, sems, base):
    first = []
    for p, order in enumerate(parts):
        axis = order[phase]
        pre = tuple(at[a] for a in order[:phase:-1])
        m = at[axis]
        up, down = (m + 1) % 4, (m + 3) % 4
        own = bufs[p].at[(*pre, m)]
        i = base + 4 * p
        first.append((
            send(own, own, sems, i, device_at(at, **{axis: up})),
            send(own, own, sems, i + 1, device_at(at, **{axis: down})),
        ))
    second = []
    for p, order in enumerate(parts):
        axis = order[phase]
        pre = tuple(at[a] for a in order[:phase:-1])
        m = at[axis]
        up, down = (m + 1) % 4, (m + 3) % 4
        lo, hi = halves(bufs[p].shape[len(pre) + 1])
        i = base + 4 * p
        first[p][0].wait_recv()
        from_down = bufs[p].at[(*pre, down, lo)]
        a = send(from_down, from_down, sems, i + 2, device_at(at, **{axis: up}))
        first[p][1].wait_recv()
        from_up = bufs[p].at[(*pre, up, hi)]
        b = send(from_up, from_up, sems, i + 3, device_at(at, **{axis: down}))
        second.append((a, b))
    for p in range(len(parts)):
        for copy in first[p]:
            copy.wait_send()
        for copy in second[p]:
            copy.wait()


def add_into(ref, idx, terms):
    total = ref[idx].astype(F32)
    for term in terms:
        total = total + term.astype(F32)
    ref[idx] = total.astype(BF)


def reduce_phase(at, bufs, parts, phase, one_up, one_down, two_up, two_down, sems, base, keep=True):
    early = []
    for p, order in enumerate(parts):
        axis = order[phase]
        pre = tuple(at[a] for a in order[:phase:-1])
        m = at[axis]
        up, down, far = (m + 1) % 4, (m + 3) % 4, (m + 2) % 4
        to_up, to_down = device_at(at, **{axis: up}), device_at(at, **{axis: down})
        lo, hi = halves(bufs[p].shape[len(pre) + 1])
        i = base + 6 * p
        early.append((
            send(bufs[p].at[(*pre, far, lo)], one_up[p], sems, i, to_up),
            send(bufs[p].at[(*pre, far, hi)], one_down[p], sems, i + 1, to_down),
            send(bufs[p].at[(*pre, up, hi)], two_up[p].at[hi], sems, i + 2, to_up),
            send(bufs[p].at[(*pre, down, lo)], two_down[p].at[lo], sems, i + 3, to_down),
        ))
    late = []
    for p, order in enumerate(parts):
        axis = order[phase]
        pre = tuple(at[a] for a in order[:phase:-1])
        m = at[axis]
        up, down = (m + 1) % 4, (m + 3) % 4
        to_up, to_down = device_at(at, **{axis: up}), device_at(at, **{axis: down})
        lo, hi = halves(bufs[p].shape[len(pre) + 1])
        i = base + 6 * p
        early[p][0].wait_recv()
        add_into(bufs[p], (*pre, up, lo), [one_up[p][...]])
        a = send(bufs[p].at[(*pre, up, lo)], two_up[p].at[lo], sems, i + 4, to_up)
        early[p][1].wait_recv()
        add_into(bufs[p], (*pre, down, hi), [one_down[p][...]])
        b = send(bufs[p].at[(*pre, down, hi)], two_down[p].at[hi], sems, i + 5, to_down)
        late.append((a, b))
    sums = []
    for p, order in enumerate(parts):
        axis = order[phase]
        pre = tuple(at[a] for a in order[:phase:-1])
        for copy in early[p][2:]:
            copy.wait_recv()
        for copy in late[p]:
            copy.wait_recv()
        for copy in (*early[p], *late[p]):
            copy.wait_send()
        own = (*pre, at[axis])
        total = bufs[p][own].astype(F32) + two_up[p][...].astype(F32) + two_down[p][...].astype(F32)
        if keep:
            bufs[p][own] = total.astype(BF)
        sums.append(total)
    return sums


def mixer_kernel(
    normed_ref, packed_ref, x_ref, result_ref, gain_ref, gate_ref, wide_ref, narrow_ref,
    out_ref,
    heads, partial, arrived, own_gain, gains, residual_ref, squares, squares_sum, squares_line,
    weights, narrow, total, ga, gb, gc,
    *rest,
):
    (pa, pb, pc), rest = rest[:3], rest[3:]
    receive, rest = rest[:36], rest[36:]
    ypack, yarrive, result, staged, sends, recvs, local = rest
    sems = (sends, recvs)
    at = my_position()
    kv = 4 * at["z"] + at["y"]
    tp = 2 * at["x"] + at["c"]
    planes, lines = plane_offsets(), line_offsets()
    for slot, start in ((0, 80), (1, 96)):
        weights[slot, :, start:128] = jnp.zeros((2, 128 - start, 4096), BF)
        narrow[slot, start:128] = jnp.zeros((128 - start, 4096), BF)
    local_copies = []
    for n, (src, dst) in enumerate((
        (gate_ref, staged.at[0]),
        (wide_ref, staged.at[1]),
        (narrow_ref, staged.at[2]),
        (result_ref, result),
    )):
        copy = pltpu.make_async_copy(src, dst, local.at[n])
        copy.start()
        local_copies.append(copy)
    meet([plane_peer(at, *d) for d in planes] + [line_peer(at, *d) for d in lines])

    copies = [
        send(normed_ref, heads.at[kv], sems, i, plane_peer(at, *d)) for i, d in enumerate(planes)
    ]
    own_gain[...] = jnp.broadcast_to(
        jnp.concatenate([gain_ref[...], jnp.zeros((1, 96), F32)], axis=1), (8, 128)
    )
    gain_copies = [
        send(own_gain, gains.at[tp], sems, 15 + i, line_peer(at, *d)) for i, d in enumerate(lines)
    ]
    partner = line_peer(at, 0, 1)
    for copy in local_copies:
        copy.wait()
    weights[0, :, 0:86] = staged[0:2]
    narrow[0, 0:86] = staged[2]
    weight_copy = send(weights.at[0, :, 0:96], weights.at[1, :, 0:96], sems, 22, partner)
    narrow_copy = send(narrow.at[0, 0:96], narrow.at[1, 0:96], sems, 23, partner)
    heads[pl.ds(kv, 1)] = normed_ref[...][None]
    gains[pl.ds(tp, 1)] = own_gain[...][None]

    place = packed_ref[0:1, :]

    def chosen(start, rows):
        return picks(place, start, rows)

    for copy in copies:
        copy.wait()
    all_heads = heads[...].reshape(1024, 256)
    for part in range(2):
        live = jnp.dot(chosen(256 * part, 256), all_heads, preferred_element_type=F32).astype(BF)
        partial[4 * part : 4 * part + 4] = (
            jnp.dot(live, result[...], preferred_element_type=F32)
            .astype(BF)
            .reshape(4, 64, 256)
        )
    copies = []
    for i, (dx, dc) in enumerate(lines):
        peer = line_peer(at, dx, dc)
        copies.append(
            send(partial.at[2 * peer[2] + peer[3]], arrived.at[i], sems, 24 + i, peer)
        )
    for copy in gain_copies:
        copy.wait()
    gain = jnp.concatenate([gains[t, 0:1, 0:32] for t in range(8)], axis=1)
    attended = partial[tp].astype(F32)
    for i, copy in enumerate(copies):
        copy.wait()
        attended = attended + arrived[i].astype(F32)
    residual = (x_ref[...].astype(F32) + attended).astype(BF).astype(F32)
    residual_ref[...] = residual
    own_squares = jnp.sum(residual * residual, axis=1, keepdims=True)
    squares[0] = jnp.broadcast_to(row_of(own_squares, 64), (8, 128))
    square_copies = [
        send(squares.at[0], squares.at[1 + i], sems, 31 + i, plane_peer(at, *d))
        for i, d in enumerate(planes)
    ]
    tile = (residual * gain).astype(BF)
    blocks = [tile[16 * i : 16 * i + 16, 128 * h : 128 * h + 128] for h in range(2) for i in range(4)]
    bufs = (ga, gb, gc)
    for p, ((start, count), order) in enumerate(zip(PARTS, ORDERS)):
        idx = tuple(at[a] for a in order[::-1])
        for b in range(count):
            bufs[p][(*idx, b)] = blocks[start + b]
    gather_phase(at, bufs, ORDERS, 0, sems, 46)
    gather_phase(at, bufs, ORDERS, 1, sems, 58)
    for copy in square_copies:
        copy.wait()
    own_sum = jnp.sum(squares[...], axis=0)
    squares_sum[...] = own_sum
    squares_line[pl.ds(at["x"], 1)] = own_sum[None]
    line_copies = [
        send(squares_sum, squares_line.at[at["x"]], sems, 82 + dx - 1, line_peer(at, dx, 0))
        for dx in (1, 2, 3)
    ]
    gather_phase(at, bufs, ORDERS, 2, sems, 70)
    for copy in line_copies:
        copy.wait()
    weight_copy.wait()
    narrow_copy.wait()

    def rows_at(zz, yy):
        a, b, c = ga[zz, yy], gb[:, zz, yy], gc[yy, :, zz]
        v = jnp.concatenate([a, b, c], axis=1)
        return jnp.concatenate(
            [v[:, 0:4].reshape(256, 128), v[:, 4:8].reshape(256, 128)], axis=1
        )

    total[...] = jnp.zeros_like(total)

    def widening(zz, carry):
        lhs = jnp.concatenate([rows_at(zz, yy) for yy in range(4)], axis=1)
        cols = pl.ds(pl.multiple_of(zz * 1024, 1024), 1024)
        for core in range(2):
            total[core] += times(lhs, weights[core, :, :, cols].reshape(256, 1024))
        return carry

    lax.fori_loop(0, 4, widening, 0)
    scale = lax.rsqrt(
        jnp.concatenate([column_of(squares_line[g, 0:1, :], 64) for g in range(4)], axis=0)
        / 4096
        + EPS
    )
    hidden = []
    for core in range(2):
        gated = total[core, :, 0:128] * scale
        upward = total[core, :, 128:256] * scale
        hidden.append((gated * jax.nn.sigmoid(gated) * upward).astype(BF))
    hidden = jnp.concatenate(hidden, axis=1)
    pbufs = (pa, pb, pc)

    def narrowing(k, carry):
        cols = pl.ds(pl.multiple_of(k * 256, 256), 256)
        rhs = jnp.concatenate([narrow[0, :, cols], narrow[1, :, cols]], axis=0)
        term = jnp.dot(hidden, rhs, preferred_element_type=F32).astype(BF)
        v = jnp.concatenate(
            [term[:, 0:128].reshape(4, 4, 16, 128), term[:, 128:256].reshape(4, 4, 16, 128)], axis=1
        )
        zz, yy = k // 4, k % 4
        pa[zz, yy] = v[:, 0:3]
        pb[:, zz, yy] = v[:, 3:6]
        pc[yy, :, zz] = v[:, 6:8]
        return carry

    lax.fori_loop(0, 16, narrowing, 0)
    for n, phase in enumerate((2, 1, 0)):
        r = receive[12 * n : 12 * n + 12]
        sums = reduce_phase(
            at, pbufs, ORDERS, phase, r[0:3], r[3:6], r[6:9], r[9:12], sems, 85 + 18 * n, phase > 0
        )
    sums = jnp.concatenate(sums, axis=0)
    mixed = []
    for h in range(2):
        for i in range(4):
            res = residual_ref[16 * i : 16 * i + 16, 128 * h : 128 * h + 128]
            mixed.append((res + sums[4 * h + i]).astype(BF))
    for t in range(8):
        h, lane = t // 4, 32 * (t % 4)
        ypack[t] = jnp.concatenate(
            [mixed[4 * h + i][:, lane : lane + 32] for i in range(4)], axis=1
        )
    copies = []
    for i, (dx, dc) in enumerate(lines):
        peer = line_peer(at, dx, dc)
        copies.append(
            send(ypack.at[2 * peer[2] + peer[3]], yarrive.at[tp], sems, 139 + i, peer)
        )
    yarrive[pl.ds(tp, 1)] = ypack[pl.ds(tp, 1)]
    for copy in copies:
        copy.wait()
    out_ref[...] = yarrive[...]


def mixer(normed, packed, x, result, gain, gate, wide, narrow):
    vmem = pl.BlockSpec(memory_space=pltpu.VMEM)
    far = pl.BlockSpec(memory_space=pltpu.HBM)
    counts = [count for _, count in PARTS]
    boxes = [pltpu.VMEM((4, 4, 4, count, 16, 128), BF) for count in counts]
    receive = []
    for phase in (2, 1, 0):
        lead = (4,) * phase
        shapes = [(*lead, count, 16, 128) for count in counts]
        low = [pltpu.VMEM((s[0] // 2, *s[1:]), BF) for s in shapes]
        high = [pltpu.VMEM((s[0] - s[0] // 2, *s[1:]), BF) for s in shapes]
        full = [pltpu.VMEM(s, BF) for s in shapes]
        receive += low + high + full + full
    return pl.pallas_call(
        mixer_kernel,
        out_shape=jax.ShapeDtypeStruct((8, 16, 128), BF),
        in_specs=[vmem, vmem, vmem, far, vmem, far, far, far],
        out_specs=vmem,
        scratch_shapes=[
            pltpu.VMEM((16, 64, 256), BF),
            pltpu.VMEM((8, 64, 256), BF),
            pltpu.VMEM((7, 64, 256), BF),
            pltpu.VMEM((8, 128), F32),
            pltpu.VMEM((8, 8, 128), F32),
            pltpu.VMEM((64, 256), F32),
            pltpu.VMEM((16, 8, 128), F32),
            pltpu.VMEM((8, 128), F32),
            pltpu.VMEM((4, 8, 128), F32),
            pltpu.VMEM((2, 2, 128, 4096), BF),
            pltpu.VMEM((2, 128, 4096), BF),
            pltpu.VMEM((2, 256, 256), F32),
            *boxes,
            *boxes,
            *receive,
            pltpu.VMEM((8, 16, 128), BF),
            pltpu.VMEM((8, 16, 128), BF),
            pltpu.VMEM((256, 256), BF),
            pltpu.VMEM((3, 86, 4096), BF),
            pltpu.SemaphoreType.DMA((146,)),
            pltpu.SemaphoreType.DMA((146,)),
            pltpu.SemaphoreType.DMA((4,)),
        ],
        compiler_params=pltpu.CompilerParams(
            collective_id=0, has_side_effects=True, vmem_limit_bytes=67043328
        ),
        name="mixer",
    )(normed, packed, x, result, gain, gate, wide, narrow)


def spread_kernel(packed_ref, mixed_ref, out_ref):
    place = packed_ref[0:1, :]
    total = jnp.zeros((32, 1024), F32)
    j = lax.broadcasted_iota(jnp.int32, (128, 1024), 0)
    rows = 64 * (j // 16) + j % 16
    for a in range(4):
        chosen = jnp.where(rows + 16 * a == place, 1.0, 0.0).astype(BF)
        piece = mixed_ref[...].reshape(128, 128)[:, 32 * a : 32 * a + 32]
        total = total + times(piece, chosen, ((0,), (0,)))
    out_ref[...] = total.astype(BF)


def spread(packed, mixed):
    vmem = pl.BlockSpec(memory_space=pltpu.VMEM)
    return pl.pallas_call(
        spread_kernel,
        out_shape=jax.ShapeDtypeStruct((32, 1024), BF),
        in_specs=[vmem] * 2,
        out_specs=vmem,
        name="spread",
    )(packed, mixed)


def front_kernel(
    x_ref, lengths_ref, gain_ref, wq_ref, wf_ref, wi_ref, wo_ref,
    z_ref, xt_ref, packed_ref,
    cols, scaled, squares, squares_in, pa, pb, weights, *rest,
):
    receive, (sends, recvs, local) = rest[:16], rest[16:]
    sems = (sends, recvs)
    at = my_position()
    kv = 4 * at["z"] + at["y"]
    tp = 2 * at["x"] + at["c"]
    planes, lines = plane_offsets(), line_offsets()
    own_copy = pltpu.make_async_copy(x_ref, cols.at[tp], local.at[0])
    own_copy.start()
    weight_copies = []
    for n, ref in enumerate((wq_ref, wf_ref, wi_ref, wo_ref)):
        copy = pltpu.make_async_copy(ref, weights.at[n], local.at[1 + n])
        copy.start()
        weight_copies.append(copy)
    meet([plane_peer(at, *d) for d in planes] + [line_peer(at, *d) for d in lines])
    own_copy.wait()
    copies = [
        send(cols.at[tp], cols.at[tp], sems, i, line_peer(at, *d)) for i, d in enumerate(lines)
    ]
    lengths = jnp.broadcast_to(lengths_ref[...], (8, 128)).astype(F32).astype(BF)
    s = lax.broadcasted_iota(jnp.int32, (128, 1024), 0)
    owner = lax.broadcasted_iota(jnp.int32, (128, 1024), 1) // 8
    start = times(lengths, jnp.where(s < owner, 1.0, 0.0).astype(BF), ((1,), (0,)))
    length = times(lengths, jnp.where(s == owner, 1.0, 0.0).astype(BF), ((1,), (0,)))
    slot = lax.broadcasted_iota(jnp.int32, (8, 1024), 1) % 8
    place = jnp.where(
        slot < length.astype(jnp.int32), start.astype(jnp.int32) + slot, -1
    )
    packed_ref[...] = place
    gain = jnp.concatenate(
        [column_of(gain_ref[:, 0:128], 128), column_of(gain_ref[:, 128:256], 128)], axis=0
    )
    mine = picks(place[0:1, :], 64 * tp, 64)
    for copy in copies:
        copy.wait()
    xt_ref[...] = times(mine, cols[...].reshape(256, 1024)).astype(BF)
    for k in range(8):
        lanes = slice(128 * k, 128 * k + 128)
        v = cols[:, :, lanes].reshape(256, 128).astype(F32)
        scaled[:, lanes] = (v * gain).astype(BF)
        squares[k] = jnp.broadcast_to(jnp.sum(v * v, axis=0, keepdims=True), (8, 128))
    square_copies = []
    for i, (dz, dy) in enumerate(planes):
        peer = plane_peer(at, dz, dy)
        square_copies.append(
            send(squares.at[(4 * peer[0] + peer[1]) // 2], squares_in.at[i], sems, 7 + i, peer)
        )

    def project(a, carry):
        lhs = scaled[:, pl.ds(pl.multiple_of(256 * a, 256), 256)]
        for n in range(2):
            for half in range(2):
                lanes = slice(256 * half, 256 * half + 256)
                v = times(lhs, weights[2 * n + half], ((0,), (0,))).astype(BF).reshape(4, 64, 256)
                if n == 0:
                    pa[:, a, :, lanes] = v
                else:
                    pb[a, :, :, lanes] = v
        return carry

    for copy in weight_copies:
        copy.wait()
    lax.fori_loop(0, 4, project, 0)
    bufs = (pa, pb)
    r = receive
    reduce_phase(at, bufs, PLANE_ORDERS, 1, r[0:2], r[2:4], r[4:6], r[6:8], sems, 22)
    r = receive[8:]
    sums = reduce_phase(
        at, bufs, PLANE_ORDERS, 0, r[0:2], r[2:4], r[4:6], r[6:8], sems, 34, False
    )
    for copy in square_copies:
        copy.wait()
    total = jnp.sum(squares_in[...], axis=0) + squares[kv // 2]
    shift = 64 * (kv % 2)
    eye = lax.broadcasted_iota(jnp.int32, (64, 128), 1) == shift + lax.broadcasted_iota(
        jnp.int32, (64, 128), 0
    )
    own = jnp.sum(jnp.where(eye, total[0:1, :], 0.0), axis=1, keepdims=True)
    scale = lax.rsqrt(own / 4096 + EPS)
    z_ref[:, 0:512] = sums[0] * scale
    z_ref[:, 512:1024] = sums[1] * scale


def front(x, lengths, gain, wq, wf, wi, wo):
    vmem = pl.BlockSpec(memory_space=pltpu.VMEM)
    far = pl.BlockSpec(memory_space=pltpu.HBM)
    receive = []
    for phase in (1, 0):
        shape = (*(4,) * phase, 64, 512)
        half = pltpu.VMEM((shape[0] // 2, *shape[1:]), BF)
        receive += [half] * 4 + [pltpu.VMEM(shape, BF)] * 4
    return pl.pallas_call(
        front_kernel,
        out_shape=(
            jax.ShapeDtypeStruct((64, 1024), F32),
            jax.ShapeDtypeStruct((64, 256), BF),
            jax.ShapeDtypeStruct((8, 1024), jnp.int32),
        ),
        in_specs=[far, vmem, vmem, far, far, far, far],
        out_specs=(vmem,) * 3,
        scratch_shapes=[
            pltpu.VMEM((8, 32, 1024), BF),
            pltpu.VMEM((256, 1024), BF),
            pltpu.VMEM((8, 8, 128), F32),
            pltpu.VMEM((15, 8, 128), F32),
            pltpu.VMEM((4, 4, 64, 512), BF),
            pltpu.VMEM((4, 4, 64, 512), BF),
            pltpu.VMEM((4, 256, 256), BF),
            *receive,
            pltpu.SemaphoreType.DMA((46,)),
            pltpu.SemaphoreType.DMA((46,)),
            pltpu.SemaphoreType.DMA((5,)),
        ],
        compiler_params=pltpu.CompilerParams(
            collective_id=1, has_side_effects=True, vmem_limit_bytes=67043328
        ),
        name="front",
    )(x, lengths, gain, wq, wf, wi, wo)


def split(v):
    high = v.astype(BF)
    return high, (v - high.astype(F32)).astype(BF)


def recurrence_kernel(
    z_ref, bound_ref, shrink_ref, lengths_ref, lane_gain_ref, state_ref,
    normed_ref, new_ref,
    query, kept, gate, output,
):
    kv = 4 * lax.axis_index("kv_0") + lax.axis_index("kv_1")
    row = lax.broadcasted_iota(jnp.int32, (64, 128), 0)
    lane = lax.broadcasted_iota(jnp.int32, (64, 128), 1)
    length = jnp.sum(
        jnp.where(lane == 8 * kv + row // 8, lengths_ref[...].astype(F32), 0.0),
        axis=1,
        keepdims=True,
    )
    live = (row[:, 0:1] % 8).astype(F32) < length
    slot = lax.broadcasted_iota(jnp.int32, (8, 8, 128), 1)
    for h in range(2):
        lanes = slice(128 * h, 128 * h + 128)
        bound = bound_ref[:, lanes]
        retain = bound + (1.0 - bound) * jax.nn.sigmoid(z_ref[:, 256 + 128 * h : 384 + 128 * h])
        shrink = jnp.sum(
            jnp.where(lane[:, 0:64] == row[:, 0:64], shrink_ref[h : h + 1, :], 0.0),
            axis=1,
            keepdims=True,
        )
        decay = jnp.where(live, jnp.exp(jnp.log(retain) + shrink), 1.0).reshape(8, 8, 128)
        key = jnp.where(live, 1.0 - retain, 0.0).reshape(8, 8, 128)
        zq = z_ref[:, lanes]
        q = (zq * jax.nn.sigmoid(zq)).reshape(8, 8, 128)
        value = z_ref[:, 512 + 128 * h : 640 + 128 * h].reshape(8, 8, 128)
        between = q
        out = jnp.sum(q * key, axis=2, keepdims=True) * value
        for back in range(1, 8):
            between = between * (decay if back == 1 else pltpu.roll(decay, back - 1, 1))
            weight = jnp.sum(between * pltpu.roll(key, back, 1), axis=2, keepdims=True)
            out = out + jnp.where(slot >= back, weight * pltpu.roll(value, back, 1), 0.0)
        output[:, lanes] = out.reshape(64, 128)
        before, after = decay, jnp.where(slot < 7, pltpu.roll(decay, 7, 1), 1.0)
        for step in (1, 2, 4):
            before = before * jnp.where(slot >= step, pltpu.roll(before, step, 1), 1.0)
            after = after * jnp.where(slot + step < 8, pltpu.roll(after, 8 - step, 1), 1.0)
        query[:, lanes] = (q * before).reshape(64, 128)
        kept[:, lanes] = before.reshape(64, 128)
        gate[:, lanes] = (key * after).reshape(64, 128)

    def sequence(n, carry):
        rows = pl.ds(pl.multiple_of(8 * n, 8), 8)
        for h in range(2):
            lanes = slice(128 * h, 128 * h + 128)
            state = state_ref[n, h]
            s_high, s_low = split(state)
            q_high, q_low = split(query[rows, lanes])
            lhs = jnp.concatenate(
                [
                    jnp.concatenate([q_high, q_high], axis=1),
                    jnp.concatenate([q_low, jnp.zeros_like(q_low)], axis=1),
                ],
                axis=0,
            )
            o = times(lhs, jnp.concatenate([s_high, s_low], axis=0), ((1,), (0,)))
            output[rows, lanes] += o[0:8] + o[8:16]
            k_high, k_low = split(gate[rows, lanes])
            v_high, v_low = split(z_ref[rows, 512 + 128 * h : 640 + 128 * h])
            added = times(
                jnp.concatenate([k_high, k_high, k_low], axis=0),
                jnp.concatenate([v_high, v_low, v_high], axis=0),
                ((0,), (0,)),
            )
            new_ref[n, h] = column_of(kept[rows, lanes][7:8, :], 128) * state + added
        return carry

    lax.fori_loop(0, 8, sequence, 0)
    for h in range(2):
        lanes = slice(128 * h, 128 * h + 128)
        o = output[:, lanes]
        zo = z_ref[:, 768 + 128 * h : 896 + 128 * h]
        o = o * lax.rsqrt(jnp.mean(o * o, axis=1, keepdims=True) + EPS) * lane_gain_ref[...]
        normed_ref[:, lanes] = jnp.where(live, o * (zo * jax.nn.sigmoid(zo)), 0.0).astype(BF)


def recurrence(z, bound, shrink, lengths, lane_gain, state):
    vmem = pl.BlockSpec(memory_space=pltpu.VMEM)
    return pl.pallas_call(
        recurrence_kernel,
        out_shape=(
            jax.ShapeDtypeStruct((64, 256), BF),
            jax.ShapeDtypeStruct((8, 2, 128, 128), F32),
        ),
        in_specs=[vmem] * 6,
        out_specs=(vmem, vmem),
        scratch_shapes=[pltpu.VMEM((64, 256), F32)] * 4,
        name="recurrence",
    )(z, bound, shrink, lengths, lane_gain, state)


def local(
    residual_entries,
    fresh_extents,
    memory_matrix,
    initial_rescale_vector,
    probe_matrix,
    retain_matrix,
    content_matrix,
    result_switch_matrix,
    retain_lower_limit,
    extra_shrink_log,
    lane_result_rescale,
    result_matrix,
    later_rescale_vector,
    mixer_switch_matrix,
    widening_matrix,
    narrowing_matrix,
):
    lengths = fresh_extents.reshape(1, 128)
    z, xt, packed = front(
        residual_entries.T,
        lengths,
        initial_rescale_vector.reshape(1, 256),
        probe_matrix,
        retain_matrix,
        content_matrix,
        result_switch_matrix,
    )
    normed, carried = recurrence(
        z,
        retain_lower_limit.reshape(1, 256),
        extra_shrink_log.T,
        lengths,
        lane_result_rescale.reshape(1, 128),
        memory_matrix,
    )
    mixed = mixer(
        normed,
        packed,
        xt,
        result_matrix,
        later_rescale_vector.reshape(1, 32),
        mixer_switch_matrix.T,
        widening_matrix.T,
        narrowing_matrix,
    )
    return (spread(packed, mixed).T, carried)


def solution(mesh):
    torus = Mesh(mesh.devices.reshape(4, 4, 4, 2), ("kv_0", "kv_1", "tp_0", "tp_1"))
    placed = (
        P(None, KV_TP),
        P(),
        P(KV, TP, None, None),
        P(KV),
        P(KV, TP),
        P(KV, TP),
        P(KV, TP),
        P(KV, TP),
        P(TP),
        P(KV, TP),
        P(),
        P(TP, KV),
        P(KV_TP),
        P(None, KV_TP),
        P(None, KV_TP),
        P(KV_TP, None),
    )
    return jax.shard_map(
        local,
        mesh=torus,
        in_specs=placed,
        out_specs=(P(None, KV_TP), P(KV, TP, None, None)),
        check_vma=False,
    )
```

```python
import jax
import jax.numpy as jnp
from jax import lax
from jax.experimental import pallas as pl
from jax.experimental.pallas import tpu as pltpu
from jax.sharding import Mesh
from jax.sharding import PartitionSpec as P

KV = ("kv_0", "kv_1")
TP = ("tp_0", "tp_1")
KV_TP = ("kv_0", "kv_1", "tp_0", "tp_1")
MESH = pl.DeviceIdType.MESH
EPS = 1e-06
F32 = jnp.float32
BF = jnp.bfloat16
PARTS = ((0, 3), (3, 3), (6, 2))
ORDERS = ("xyz", "yzx", "zxy")
PLANE_ORDERS = ("zy", "yz")


def my_position():
    return dict(
        z=lax.axis_index("kv_0"),
        y=lax.axis_index("kv_1"),
        x=lax.axis_index("tp_0"),
        c=lax.axis_index("tp_1"),
    )


def device_at(at, **moved):
    there = dict(at, **moved)
    return (there["z"], there["y"], there["x"], there["c"])


def plane_offsets():
    return [(dz, dy) for dz in range(4) for dy in range(4) if dz or dy]


def line_offsets():
    return [(dx, dc) for dx in range(4) for dc in range(2) if dx or dc]


def plane_peer(at, dz, dy):
    return device_at(at, z=(at["z"] + dz) % 4, y=(at["y"] + dy) % 4)


def line_peer(at, dx, dc):
    return device_at(at, x=(at["x"] + dx) % 4, c=(at["c"] + dc) % 2)


def meet(peers):
    barrier = pltpu.get_barrier_semaphore()
    for peer in peers:
        pl.semaphore_signal(barrier, inc=1, device_id=peer, device_id_type=MESH)
    pl.semaphore_wait(barrier, len(peers))


class Sender:
    def __init__(self, sends, recvs):
        self.sends, self.recvs, self.used = sends, recvs, 0

    def __call__(self, src, dst, peer):
        i = self.used
        self.used = i + 1
        return start_copy(src, dst, self.sends.at[i], self.recvs.at[i], peer)


def start_copy(src, dst, send_sem, recv_sem, peer):
    copy = pltpu.make_async_remote_copy(
        src_ref=src,
        dst_ref=dst,
        send_sem=send_sem,
        recv_sem=recv_sem,
        device_id=peer,
        device_id_type=MESH,
    )
    copy.start()
    return copy


def times(a, b, dims=((1,), (1,))):
    return lax.dot_general(a, b, (dims, ((), ())), preferred_element_type=F32)


def row_of(column, rows):
    eye = lax.broadcasted_iota(jnp.int32, (rows, 128), 0) == lax.broadcasted_iota(
        jnp.int32, (rows, 128), 1
    )
    return jnp.sum(jnp.where(eye, column, 0.0), axis=0, keepdims=True)


def column_of(row, rows):
    eye = lax.broadcasted_iota(jnp.int32, (rows, 128), 0) == lax.broadcasted_iota(
        jnp.int32, (rows, 128), 1
    )
    return jnp.sum(jnp.where(eye, row, 0.0), axis=1, keepdims=True)


def picks(place, start, rows):
    want = lax.broadcasted_iota(jnp.int32, (rows, 1024), 0) + start
    return jnp.where(want == place, 1.0, 0.0).astype(BF)


def halves(length):
    return pl.ds(0, length // 2), pl.ds(length // 2, length - length // 2)


def gather_plane(at, bufs, orders, send):
    copies = []
    for p, order in enumerate(orders):
        a, b, c = order
        own = bufs[p].at[at[c], at[b], at[a]]
        for db, da in plane_offsets():
            there = {a: (at[a] + da) % 4, b: (at[b] + db) % 4}
            copies.append(send(own, own, device_at(at, **there)))
    return copies


def gather_line(at, bufs, orders, send):
    first = []
    for p, order in enumerate(orders):
        axis = order[-1]
        m = at[axis]
        own = bufs[p].at[m]
        first.append((
            send(own, own, device_at(at, **{axis: (m + 1) % 4})),
            send(own, own, device_at(at, **{axis: (m + 3) % 4})),
        ))
    second = []
    for p, order in enumerate(orders):
        axis = order[-1]
        m = at[axis]
        up, down = (m + 1) % 4, (m + 3) % 4
        lo, hi = halves(bufs[p].shape[1])
        first[p][0].wait_recv()
        from_down = bufs[p].at[down, lo]
        second.append(send(from_down, from_down, device_at(at, **{axis: up})))
        first[p][1].wait_recv()
        from_up = bufs[p].at[up, hi]
        second.append(send(from_up, from_up, device_at(at, **{axis: down})))
    for pair in first:
        for copy in pair:
            copy.wait_send()
    for copy in second:
        copy.wait()


def add_into(ref, idx, term):
    ref[idx] = (ref[idx].astype(F32) + term.astype(F32)).astype(BF)


def reduce_line(at, bufs, axes, pres, received, send, keep=True):
    early = []
    for p, (axis, pre) in enumerate(zip(axes, pres)):
        one_up, one_down, two_up, two_down = received[p]
        m = at[axis]
        up, down, away = (m + 1) % 4, (m + 3) % 4, (m + 2) % 4
        to_up, to_down = device_at(at, **{axis: up}), device_at(at, **{axis: down})
        lo, hi = halves(bufs[p].shape[len(pre) + 1])
        early.append((
            send(bufs[p].at[(*pre, away, lo)], one_up, to_up),
            send(bufs[p].at[(*pre, away, hi)], one_down, to_down),
            send(bufs[p].at[(*pre, up, hi)], two_up.at[hi], to_up),
            send(bufs[p].at[(*pre, down, lo)], two_down.at[lo], to_down),
        ))
    yield
    late = []
    for p, (axis, pre) in enumerate(zip(axes, pres)):
        one_up, one_down, two_up, two_down = received[p]
        m = at[axis]
        up, down = (m + 1) % 4, (m + 3) % 4
        to_up, to_down = device_at(at, **{axis: up}), device_at(at, **{axis: down})
        lo, hi = halves(bufs[p].shape[len(pre) + 1])
        early[p][0].wait_recv()
        add_into(bufs[p], (*pre, up, lo), one_up[...])
        a = send(bufs[p].at[(*pre, up, lo)], two_up.at[lo], to_up)
        early[p][1].wait_recv()
        add_into(bufs[p], (*pre, down, hi), one_down[...])
        late.append((a, send(bufs[p].at[(*pre, down, hi)], two_down.at[hi], to_down)))
    yield
    sums = []
    for p, (axis, pre) in enumerate(zip(axes, pres)):
        for copy in early[p][2:]:
            copy.wait_recv()
        for copy in late[p]:
            copy.wait_recv()
        for copy in (*early[p], *late[p]):
            copy.wait_send()
        own = (*pre, at[axis])
        total = bufs[p][own].astype(F32)
        for ref in received[p][2:]:
            total = total + ref[...].astype(F32)
        if keep:
            bufs[p][own] = total.astype(BF)
        sums.append(total)
    yield sums


def all_of(steps):
    for result in steps:
        pass
    return result


def reduce_plane(at, bufs, orders, received, send):
    copies = []
    for p, order in enumerate(orders):
        a, b, c = order
        for n, (db, da) in enumerate(plane_offsets()):
            there = {a: (at[a] + da) % 4, b: (at[b] + db) % 4}
            block = bufs[p].at[at[c], there[b], there[a]]
            copies.append(send(block, received[p].at[n], device_at(at, **there)))
    sums = []
    for copy in copies:
        copy.wait()
    for p, order in enumerate(orders):
        a, b, c = order
        total = bufs[p][at[c], at[b], at[a]].astype(F32)
        for n in range(15):
            total = total + received[p][n].astype(F32)
        sums.append(total)
    return sums


def split(v):
    high = v.astype(BF)
    return high, (v - high.astype(F32)).astype(BF)


INPUTS = (
    "x", "lengths", "gain", "wq", "wf", "wi", "wo", "bound", "shrink", "lane_gain", "state",
    "result", "later_gain", "gate", "wide", "narrow",
)
IN_HBM = ("x", "wq", "wf", "wi", "wo", "state", "result", "gate", "wide", "narrow")


def line_shapes(lead, tail, parts):
    shapes = []
    for count in parts:
        shape = (*lead, *((count,) if count else ()), *tail)
        half = shape[0] // 2
        shapes += [(half, *shape[1:]), (shape[0] - half, *shape[1:]), shape, shape]
    return shapes


def scratch():
    counts = [count for _, count in PARTS]
    boxes = [(4, 4, 4, count, 16, 128) for count in counts]
    named = [
        ("cols", (8, 32, 1024), BF),
        ("scaled", (256, 1024), BF),
        ("squares", (8, 8, 128), F32),
        ("squares_in", (15, 8, 128), F32),
        ("front_weights", (4, 256, 256), BF),
        ("pa", (4, 4, 64, 512), BF),
        ("pb", (4, 4, 64, 512), BF),
        ("z", (64, 1024), F32),
        ("query", (64, 256), F32),
        ("kept", (64, 256), F32),
        ("key", (64, 256), F32),
        ("output", (64, 256), F32),
        ("state_in", (8, 2, 128, 128), F32),
        ("state_out", (8, 2, 128, 128), F32),
        ("chosen", (512, 1024), BF),
        ("heads", (16, 64, 256), BF),
        ("partial", (8, 64, 256), BF),
        ("arrived", (7, 64, 256), BF),
        ("own_gain", (8, 128), F32),
        ("gains", (8, 8, 128), F32),
        ("own_rows", (64, 256), F32),
        ("residual", (64, 256), F32),
        ("later_squares", (16, 8, 128), F32),
        ("squares_sum", (8, 128), F32),
        ("squares_line", (4, 8, 128), F32),
        ("weights", (2, 2, 128, 4096), BF),
        ("narrows", (2, 128, 4096), BF),
        ("staged", (3, 86, 4096), BF),
        ("result_in", (256, 256), BF),
        ("total", (2, 256, 256), F32),
        ("ypack", (8, 16, 128), BF),
        ("yarrive", (8, 16, 128), BF),
    ]
    groups = [
        ("gathered", boxes),
        ("terms", boxes),
        ("front_one", line_shapes((4, 64), (512,), (0, 0))),
        ("front_two", line_shapes((64,), (512,), (0, 0))),
        ("mixer_line", line_shapes((4, 4), (16, 128), counts)),
        ("mixer_plane", [(15, count, 16, 128) for count in counts]),
    ]
    flat = [pltpu.VMEM(shape, kind) for _, shape, kind in named]
    for _, shapes in groups:
        flat += [pltpu.VMEM(shape, BF) for shape in shapes]
    return named, groups, flat


def layer_kernel(*refs):
    named, groups, flat = scratch()
    ref = dict(zip(INPUTS, refs))
    mixed_out, state_result = refs[len(INPUTS) : len(INPUTS) + 2]
    rest = refs[len(INPUTS) + 2 :]
    ref.update(zip(["_" + name for name, _, _ in named], rest))
    rest = rest[len(named) :]
    group = {}
    for name, shapes in groups:
        group[name], rest = rest[: len(shapes)], rest[len(shapes) :]
    sends, recvs, local = rest
    send = Sender(sends, recvs)
    at = my_position()
    kv = 4 * at["z"] + at["y"]
    tp = 2 * at["x"] + at["c"]
    planes, lines = plane_offsets(), line_offsets()
    fours = lambda refs: [refs[i : i + 4] for i in range(0, len(refs), 4)]

    def fetch(n, src, dst):
        copy = pltpu.make_async_copy(src, dst, local.at[n])
        copy.start()
        return copy

    cols = ref["_cols"]
    x_copy = fetch(0, ref["x"], cols.at[tp])
    front_copies = [
        fetch(1 + n, ref[name], ref["_front_weights"].at[n])
        for n, name in enumerate(("wq", "wf", "wi", "wo"))
    ]
    weight_copies = [
        fetch(5 + n, ref[name], ref["_staged"].at[n])
        for n, name in enumerate(("gate", "wide", "narrow"))
    ]
    state_copy = fetch(8, ref["state"], ref["_state_in"])
    result_copy = fetch(9, ref["result"], ref["_result_in"])
    meet([plane_peer(at, *d) for d in planes] + [line_peer(at, *d) for d in lines])

    x_copy.wait()
    copies = [send(cols.at[tp], cols.at[tp], line_peer(at, *d)) for d in lines]
    own_gain, gains = ref["_own_gain"], ref["_gains"]
    own_gain[...] = jnp.broadcast_to(
        jnp.concatenate([ref["later_gain"][...], jnp.zeros((1, 96), F32)], axis=1), (8, 128)
    )
    gain_copies = [send(own_gain, gains.at[tp], line_peer(at, *d)) for d in lines]
    gains[pl.ds(tp, 1)] = own_gain[...][None]

    lengths = jnp.broadcast_to(ref["lengths"][...], (8, 128)).astype(F32).astype(BF)
    s = lax.broadcasted_iota(jnp.int32, (128, 1024), 0)
    owner = lax.broadcasted_iota(jnp.int32, (128, 1024), 1) // 8
    start = times(lengths, jnp.where(s < owner, 1.0, 0.0).astype(BF), ((1,), (0,)))
    length = times(lengths, jnp.where(s == owner, 1.0, 0.0).astype(BF), ((1,), (0,)))
    slot = lax.broadcasted_iota(jnp.int32, (8, 1024), 1) % 8
    place = jnp.where(slot < length.astype(jnp.int32), start.astype(jnp.int32) + slot, -1)[0:1]
    for part in range(4):
        ref["_chosen"][128 * part : 128 * part + 128] = picks(place, 128 * part, 128)
    gain = jnp.concatenate(
        [column_of(ref["gain"][:, 0:128], 128), column_of(ref["gain"][:, 128:256], 128)], axis=0
    )
    weights, narrows, staged = ref["_weights"], ref["_narrows"], ref["_staged"]
    for n, first in ((0, 80), (1, 96)):
        weights[n, :, first:128] = jnp.zeros((2, 128 - first, 4096), BF)
        narrows[n, first:128] = jnp.zeros((128 - first, 4096), BF)
    for copy in weight_copies:
        copy.wait()
    weights[0, :, 0:86] = staged[0:2]
    narrows[0, 0:86] = staged[2]

    for copy in copies:
        copy.wait()
    partner = line_peer(at, 0, 1)
    weight_sends = [
        send(weights.at[0, :, 0:96], weights.at[1, :, 0:96], partner),
        send(narrows.at[0, 0:96], narrows.at[1, 0:96], partner),
    ]
    scaled, squares = ref["_scaled"], ref["_squares"]
    for k in range(8):
        lanes = slice(128 * k, 128 * k + 128)
        v = cols[:, :, lanes].reshape(256, 128).astype(F32)
        scaled[:, lanes] = (v * gain).astype(BF)
        squares[k] = jnp.broadcast_to(jnp.sum(v * v, axis=0, keepdims=True), (8, 128))
    for copy in front_copies:
        copy.wait()
    pa, pb = ref["_pa"], ref["_pb"]

    def project(n):
        def body(a, carry):
            lhs = scaled[:, pl.ds(pl.multiple_of(256 * a, 256), 256)]
            for half in range(2):
                lanes = slice(256 * half, 256 * half + 256)
                weight = ref["_front_weights"][2 * n + half]
                v = times(lhs, weight, ((0,), (0,))).astype(BF).reshape(4, 64, 256)
                if n == 0:
                    pa[:, a, :, lanes] = v
                else:
                    pb[a, :, :, lanes] = v
            return carry

        lax.fori_loop(0, 4, body, 0)

    one, two = fours(group["front_one"]), fours(group["front_two"])
    project(0)
    steps_a = reduce_line(at, (pa,), ("y",), ((),), one[0:1], send)
    next(steps_a)
    project(1)
    steps_b = reduce_line(at, (pb,), ("z",), ((),), one[1:2], send)
    next(steps_b)
    square_copies = []
    for i, (dz, dy) in enumerate(planes):
        peer = plane_peer(at, dz, dy)
        block = squares.at[(4 * peer[0] + peer[1]) // 2]
        square_copies.append(send(block, ref["_squares_in"].at[i], peer))
    ref["_own_rows"][...] = times(picks(place, 64 * tp, 64), cols[...].reshape(256, 1024))
    next(steps_a)
    next(steps_b)
    next(steps_a)
    steps_a = reduce_line(at, (pa,), ("z",), ((at["y"],),), two[0:1], send, False)
    next(steps_a)
    next(steps_b)
    steps_b = reduce_line(at, (pb,), ("y",), ((at["z"],),), two[1:2], send, False)
    next(steps_b)
    row = lax.broadcasted_iota(jnp.int32, (64, 128), 0)
    lane = lax.broadcasted_iota(jnp.int32, (64, 128), 1)
    length = jnp.sum(
        jnp.where(lane == 8 * kv + row // 8, ref["lengths"][...].astype(F32), 0.0),
        axis=1,
        keepdims=True,
    )
    live = (row[:, 0:1] % 8).astype(F32) < length
    for copy in square_copies:
        copy.wait()
    total = jnp.sum(ref["_squares_in"][...], axis=0) + squares[kv // 2]
    own = jnp.sum(
        jnp.where(lane == 64 * (kv % 2) + row, total[0:1, :], 0.0), axis=1, keepdims=True
    )
    scale = lax.rsqrt(own / 4096 + EPS)
    next(steps_a)
    next(steps_b)
    z = ref["_z"]
    z[:, 0:512] = next(steps_a)[0] * scale
    z[:, 512:1024] = next(steps_b)[0] * scale

    query, kept, keys, output = ref["_query"], ref["_kept"], ref["_key"], ref["_output"]
    slot = lax.broadcasted_iota(jnp.int32, (8, 8, 128), 1)
    for h in range(2):
        lanes = slice(128 * h, 128 * h + 128)
        bound = ref["bound"][:, lanes]
        retain = bound + (1.0 - bound) * jax.nn.sigmoid(z[:, 256 + 128 * h : 384 + 128 * h])
        shrink = jnp.sum(
            jnp.where(lane[:, 0:64] == row[:, 0:64], ref["shrink"][h : h + 1, :], 0.0),
            axis=1,
            keepdims=True,
        )
        decay = jnp.where(live, jnp.exp(jnp.log(retain) + shrink), 1.0).reshape(8, 8, 128)
        key = jnp.where(live, 1.0 - retain, 0.0).reshape(8, 8, 128)
        zq = z[:, lanes]
        q = (zq * jax.nn.sigmoid(zq)).reshape(8, 8, 128)
        value = z[:, 512 + 128 * h : 640 + 128 * h].reshape(8, 8, 128)
        between = q
        out = jnp.sum(q * key, axis=2, keepdims=True) * value
        for back in range(1, 8):
            between = between * (decay if back == 1 else pltpu.roll(decay, back - 1, 1))
            weight = jnp.sum(between * pltpu.roll(key, back, 1), axis=2, keepdims=True)
            out = out + jnp.where(slot >= back, weight * pltpu.roll(value, back, 1), 0.0)
        output[:, lanes] = out.reshape(64, 128)
        before, after = decay, jnp.where(slot < 7, pltpu.roll(decay, 7, 1), 1.0)
        for step in (1, 2, 4):
            before = before * jnp.where(slot >= step, pltpu.roll(before, step, 1), 1.0)
            after = after * jnp.where(slot + step < 8, pltpu.roll(after, 8 - step, 1), 1.0)
        query[:, lanes] = (q * before).reshape(64, 128)
        kept[:, lanes] = before.reshape(64, 128)
        keys[:, lanes] = (key * after).reshape(64, 128)
    state_copy.wait()
    state_in, state_out = ref["_state_in"], ref["_state_out"]

    def read_state(n, carry):
        rows = pl.ds(pl.multiple_of(8 * n, 8), 8)
        for h in range(2):
            lanes = slice(128 * h, 128 * h + 128)
            s_high, s_low = split(state_in[n, h])
            q_high, q_low = split(query[rows, lanes])
            lhs = jnp.concatenate(
                [
                    jnp.concatenate([q_high, q_high], axis=1),
                    jnp.concatenate([q_low, jnp.zeros_like(q_low)], axis=1),
                ],
                axis=0,
            )
            o = times(lhs, jnp.concatenate([s_high, s_low], axis=0), ((1,), (0,)))
            output[rows, lanes] += o[0:8] + o[8:16]
        return carry

    lax.fori_loop(0, 8, read_state, 0)
    heads = ref["_heads"]
    for h in range(2):
        lanes = slice(128 * h, 128 * h + 128)
        o = output[:, lanes]
        zo = z[:, 768 + 128 * h : 896 + 128 * h]
        o = o * lax.rsqrt(jnp.mean(o * o, axis=1, keepdims=True) + EPS) * ref["lane_gain"][...]
        heads[kv, :, lanes] = jnp.where(live, o * (zo * jax.nn.sigmoid(zo)), 0.0).astype(BF)
    copies = [send(heads.at[kv], heads.at[kv], plane_peer(at, *d)) for d in planes]

    def write_state(n, carry):
        rows = pl.ds(pl.multiple_of(8 * n, 8), 8)
        for h in range(2):
            lanes = slice(128 * h, 128 * h + 128)
            k_high, k_low = split(keys[rows, lanes])
            v_high, v_low = split(z[rows, 512 + 128 * h : 640 + 128 * h])
            added = times(
                jnp.concatenate([k_high, k_high, k_low], axis=0),
                jnp.concatenate([v_high, v_low, v_high], axis=0),
                ((0,), (0,)),
            )
            state_out[n, h] = column_of(kept[rows, lanes][7:8, :], 128) * state_in[n, h] + added
        return carry

    lax.fori_loop(0, 8, write_state, 0)
    new_copy = fetch(10, state_out, state_result)
    result_copy.wait()
    for copy in gain_copies:
        copy.wait()
    gain = jnp.concatenate([gains[t, 0:1, 0:32] for t in range(8)], axis=1)
    for copy in copies:
        copy.wait()

    partial, arrived, result = ref["_partial"], ref["_arrived"], ref["_result_in"]
    all_heads = heads[...].reshape(1024, 256)
    for part in range(2):
        picked = ref["_chosen"][256 * part : 256 * part + 256]
        packed = times(picked, all_heads, ((1,), (0,))).astype(BF)
        partial[4 * part : 4 * part + 4] = (
            times(packed, result[...], ((1,), (0,))).astype(BF).reshape(4, 64, 256)
        )
    copies = []
    for i, (dx, dc) in enumerate(lines):
        peer = line_peer(at, dx, dc)
        copies.append(send(partial.at[2 * peer[2] + peer[3]], arrived.at[i], peer))
    attended = partial[tp].astype(F32)
    for i, copy in enumerate(copies):
        copy.wait()
        attended = attended + arrived[i].astype(F32)
    residual = (ref["_own_rows"][...] + attended).astype(BF).astype(F32)
    tile = (residual * gain).astype(BF)
    blocks = [
        tile[16 * i : 16 * i + 16, 128 * h : 128 * h + 128] for h in range(2) for i in range(4)
    ]
    gathered = group["gathered"]
    for p, ((first, count), order) in enumerate(zip(PARTS, ORDERS)):
        idx = tuple(at[a] for a in order[::-1])
        for b in range(count):
            gathered[p][(*idx, b)] = blocks[first + b]
    copies = gather_plane(at, gathered, ORDERS, send)
    ref["_residual"][...] = residual
    later = ref["_later_squares"]
    own_squares = jnp.sum(residual * residual, axis=1, keepdims=True)
    later[0] = jnp.broadcast_to(row_of(own_squares, 64), (8, 128))
    square_copies = [
        send(later.at[0], later.at[1 + i], plane_peer(at, *d)) for i, d in enumerate(planes)
    ]
    for copy in copies:
        copy.wait()
    for copy in square_copies:
        copy.wait()
    squares_sum, squares_line = ref["_squares_sum"], ref["_squares_line"]
    own_sum = jnp.sum(later[...], axis=0)
    squares_sum[...] = own_sum
    squares_line[pl.ds(at["x"], 1)] = own_sum[None]
    line_copies = [
        send(squares_sum, squares_line.at[at["x"]], line_peer(at, dx, 0)) for dx in (1, 2, 3)
    ]
    gather_line(at, gathered, ORDERS, send)
    for copy in (*line_copies, *weight_sends):
        copy.wait()

    ga, gb, gc = gathered
    total = ref["_total"]

    def rows_at(zz, yy):
        v = jnp.concatenate([ga[zz, yy], gb[:, zz, yy], gc[yy, :, zz]], axis=1)
        return jnp.concatenate(
            [v[:, 0:4].reshape(256, 128), v[:, 4:8].reshape(256, 128)], axis=1
        )

    total[...] = jnp.zeros_like(total)

    def widening(zz, carry):
        lhs = jnp.concatenate([rows_at(zz, yy) for yy in range(4)], axis=1)
        cols = pl.ds(pl.multiple_of(zz * 1024, 1024), 1024)
        for core in range(2):
            total[core] += times(lhs, weights[core, :, :, cols].reshape(256, 1024))
        return carry

    lax.fori_loop(0, 4, widening, 0)
    scale = lax.rsqrt(
        jnp.concatenate([column_of(squares_line[g, 0:1, :], 64) for g in range(4)], axis=0)
        / 4096
        + EPS
    )
    hidden = []
    for core in range(2):
        gated = total[core, :, 0:128] * scale
        upward = total[core, :, 128:256] * scale
        hidden.append((gated * jax.nn.sigmoid(gated) * upward).astype(BF))
    hidden = jnp.concatenate(hidden, axis=1)
    ta, tb, tc = group["terms"]

    def narrowing(k, carry):
        cols = pl.ds(pl.multiple_of(k * 256, 256), 256)
        rhs = jnp.concatenate([narrows[0, :, cols], narrows[1, :, cols]], axis=0)
        term = times(hidden, rhs, ((1,), (0,))).astype(BF)
        v = jnp.concatenate(
            [term[:, 0:128].reshape(4, 4, 16, 128), term[:, 128:256].reshape(4, 4, 16, 128)], axis=1
        )
        zz, yy = k // 4, k % 4
        ta[zz, yy] = v[:, 0:3]
        tb[:, zz, yy] = v[:, 3:6]
        tc[yy, :, zz] = v[:, 6:8]
        return carry

    lax.fori_loop(0, 16, narrowing, 0)
    all_of(
        reduce_line(
            at, group["terms"], [order[-1] for order in ORDERS], ((),) * 3,
            fours(group["mixer_line"]), send,
        )
    )
    sums = reduce_plane(at, group["terms"], ORDERS, group["mixer_plane"], send)
    sums = jnp.concatenate(sums, axis=0)

    mixed = []
    for h in range(2):
        for i in range(4):
            res = ref["_residual"][16 * i : 16 * i + 16, 128 * h : 128 * h + 128]
            mixed.append((res + sums[4 * h + i]).astype(BF))
    ypack, yarrive = ref["_ypack"], ref["_yarrive"]
    for t in range(8):
        h, first = t // 4, 32 * (t % 4)
        ypack[t] = jnp.concatenate(
            [mixed[4 * h + i][:, first : first + 32] for i in range(4)], axis=1
        )
    copies = []
    for dx, dc in lines:
        peer = line_peer(at, dx, dc)
        copies.append(send(ypack.at[2 * peer[2] + peer[3]], yarrive.at[tp], peer))
    yarrive[pl.ds(tp, 1)] = ypack[pl.ds(tp, 1)]
    for copy in copies:
        copy.wait()
    spread = jnp.zeros((32, 1024), F32)
    j = lax.broadcasted_iota(jnp.int32, (128, 1024), 0)
    rows = 64 * (j // 16) + j % 16
    for a in range(4):
        chosen = jnp.where(rows + 16 * a == place, 1.0, 0.0).astype(BF)
        piece = yarrive[...].reshape(128, 128)[:, 32 * a : 32 * a + 32]
        spread = spread + times(piece, chosen, ((0,), (0,)))
    mixed_out[...] = spread.astype(BF)
    new_copy.wait()
    assert send.used <= sends.shape[0]


def layer(*arguments):
    vmem = pl.BlockSpec(memory_space=pltpu.VMEM)
    far = pl.BlockSpec(memory_space=pltpu.HBM)
    copies = 260
    return pl.pallas_call(
        layer_kernel,
        out_shape=(
            jax.ShapeDtypeStruct((32, 1024), BF),
            jax.ShapeDtypeStruct((8, 2, 128, 128), F32),
        ),
        in_specs=[far if name in IN_HBM else vmem for name in INPUTS],
        out_specs=(vmem, far),
        scratch_shapes=[
            *scratch()[2],
            pltpu.SemaphoreType.DMA((copies,)),
            pltpu.SemaphoreType.DMA((copies,)),
            pltpu.SemaphoreType.DMA((11,)),
        ],
        compiler_params=pltpu.CompilerParams(
            collective_id=0, has_side_effects=True, vmem_limit_bytes=67043328
        ),
        name="layer",
    )(*arguments)


def local(
    residual_entries,
    fresh_extents,
    memory_matrix,
    initial_rescale_vector,
    probe_matrix,
    retain_matrix,
    content_matrix,
    result_switch_matrix,
    retain_lower_limit,
    extra_shrink_log,
    lane_result_rescale,
    result_matrix,
    later_rescale_vector,
    mixer_switch_matrix,
    widening_matrix,
    narrowing_matrix,
):
    mixed, carried = layer(
        residual_entries.T,
        fresh_extents.reshape(1, 128),
        initial_rescale_vector.reshape(1, 256),
        probe_matrix,
        retain_matrix,
        content_matrix,
        result_switch_matrix,
        retain_lower_limit.reshape(1, 256),
        extra_shrink_log.T,
        lane_result_rescale.reshape(1, 128),
        memory_matrix,
        result_matrix,
        later_rescale_vector.reshape(1, 32),
        mixer_switch_matrix.T,
        widening_matrix.T,
        narrowing_matrix,
    )
    return (mixed.T, carried)


def solution(mesh):
    torus = Mesh(mesh.devices.reshape(4, 4, 4, 2), ("kv_0", "kv_1", "tp_0", "tp_1"))
    placed = (
        P(None, KV_TP),
        P(),
        P(KV, TP, None, None),
        P(KV),
        P(KV, TP),
        P(KV, TP),
        P(KV, TP),
        P(KV, TP),
        P(TP),
        P(KV, TP),
        P(),
        P(TP, KV),
        P(KV_TP),
        P(None, KV_TP),
        P(None, KV_TP),
        P(KV_TP, None),
    )
    return jax.shard_map(
        local,
        mesh=torus,
        in_specs=placed,
        out_specs=(P(None, KV_TP), P(KV, TP, None, None)),
        check_vma=False,
    )
```

```python
import functools

import jax
import jax.numpy as jnp
from jax import lax
from jax.experimental import pallas as pl
from jax.experimental.pallas import tpu as pltpu
from jax.sharding import Mesh
from jax.sharding import PartitionSpec as P

KV = ("kv_0", "kv_1")
TP = ("tp_0", "tp_1")
KV_TP = ("kv_0", "kv_1", "tp_0", "tp_1")
MESH = pl.DeviceIdType.MESH
EPS = 1e-06
F32 = jnp.float32
BF = jnp.bfloat16
PARTS = ((0, 3), (3, 3), (6, 2))
ORDERS = ("xyz", "yzx", "zxy")
PLANE_ORDERS = ("zy", "yz")


def my_position():
    return dict(
        z=lax.axis_index("kv_0"),
        y=lax.axis_index("kv_1"),
        x=lax.axis_index("tp_0"),
        c=lax.axis_index("tp_1"),
    )


def device_at(at, **moved):
    there = dict(at, **moved)
    return (there["z"], there["y"], there["x"], there["c"])


def plane_offsets():
    return [(dz, dy) for dz in range(4) for dy in range(4) if dz or dy]


def line_offsets():
    return [(dx, dc) for dx in range(4) for dc in range(2) if dx or dc]


def plane_peer(at, dz, dy):
    return device_at(at, z=(at["z"] + dz) % 4, y=(at["y"] + dy) % 4)


def line_peer(at, dx, dc):
    return device_at(at, x=(at["x"] + dx) % 4, c=(at["c"] + dc) % 2)


def meet(peers):
    barrier = pltpu.get_barrier_semaphore()
    for peer in peers:
        pl.semaphore_signal(barrier, inc=1, device_id=peer, device_id_type=MESH)
    pl.semaphore_wait(barrier, len(peers))


class Sender:
    def __init__(self, sends, recvs):
        self.sends, self.recvs, self.used = sends, recvs, 0

    def __call__(self, src, dst, peer):
        i = self.used
        self.used = i + 1
        return start_copy(src, dst, self.sends.at[i], self.recvs.at[i], peer)


def start_copy(src, dst, send_sem, recv_sem, peer):
    copy = pltpu.make_async_remote_copy(
        src_ref=src,
        dst_ref=dst,
        send_sem=send_sem,
        recv_sem=recv_sem,
        device_id=peer,
        device_id_type=MESH,
    )
    copy.start()
    return copy


def times(a, b, dims=((1,), (1,))):
    return lax.dot_general(a, b, (dims, ((), ())), preferred_element_type=F32)


def row_of(column, rows):
    eye = lax.broadcasted_iota(jnp.int32, (rows, 128), 0) == lax.broadcasted_iota(
        jnp.int32, (rows, 128), 1
    )
    return jnp.sum(jnp.where(eye, column, 0.0), axis=0, keepdims=True)


def column_of(row, rows):
    eye = lax.broadcasted_iota(jnp.int32, (rows, 128), 0) == lax.broadcasted_iota(
        jnp.int32, (rows, 128), 1
    )
    return jnp.sum(jnp.where(eye, row, 0.0), axis=1, keepdims=True)


def picks(place, start, rows):
    want = lax.broadcasted_iota(jnp.int32, (rows, 1024), 0) + start
    return jnp.where(want == place, 1.0, 0.0).astype(BF)


def halves(length):
    return pl.ds(0, length // 2), pl.ds(length // 2, length - length // 2)


def gather_plane(at, bufs, orders, send):
    copies = [[] for _ in orders]
    for p, order in enumerate(orders):
        a, b, c = order
        own = bufs[p].at[at[c], at[b], at[a]]
        for db, da in plane_offsets():
            there = {a: (at[a] + da) % 4, b: (at[b] + db) % 4}
            copies[p].append(send(own, own, device_at(at, **there)))
    return copies


def gather_line(at, bufs, orders, ready, send):
    first = []
    for p, order in enumerate(orders):
        for copy in ready[p]:
            copy.wait_recv()
        axis = order[-1]
        m = at[axis]
        own = bufs[p].at[m]
        first.append((
            send(own, own, device_at(at, **{axis: (m + 1) % 4})),
            send(own, own, device_at(at, **{axis: (m + 3) % 4})),
        ))
    yield
    second = []
    for p, order in enumerate(orders):
        axis = order[-1]
        m = at[axis]
        up, down = (m + 1) % 4, (m + 3) % 4
        lo, hi = halves(bufs[p].shape[1])
        first[p][0].wait_recv()
        from_down = bufs[p].at[down, lo]
        second.append(send(from_down, from_down, device_at(at, **{axis: up})))
        first[p][1].wait_recv()
        from_up = bufs[p].at[up, hi]
        second.append(send(from_up, from_up, device_at(at, **{axis: down})))
    for part in (*ready, *first):
        for copy in part:
            copy.wait_send()
    for copy in second:
        copy.wait()
    yield


def add_into(ref, idx, term):
    ref[idx] = (ref[idx].astype(F32) + term.astype(F32)).astype(BF)


def reduce_line(at, bufs, axes, pres, received, send, keep=True, after=None):
    early = []
    for p, (axis, pre) in enumerate(zip(axes, pres)):
        one_up, one_down, two_up, two_down = received[p]
        m = at[axis]
        up, down, away = (m + 1) % 4, (m + 3) % 4, (m + 2) % 4
        to_up, to_down = device_at(at, **{axis: up}), device_at(at, **{axis: down})
        lo, hi = halves(bufs[p].shape[len(pre) + 1])
        early.append((
            send(bufs[p].at[(*pre, away, lo)], one_up, to_up),
            send(bufs[p].at[(*pre, away, hi)], one_down, to_down),
            send(bufs[p].at[(*pre, up, hi)], two_up.at[hi], to_up),
            send(bufs[p].at[(*pre, down, lo)], two_down.at[lo], to_down),
        ))
    yield
    late = []
    for p, (axis, pre) in enumerate(zip(axes, pres)):
        one_up, one_down, two_up, two_down = received[p]
        m = at[axis]
        up, down = (m + 1) % 4, (m + 3) % 4
        to_up, to_down = device_at(at, **{axis: up}), device_at(at, **{axis: down})
        lo, hi = halves(bufs[p].shape[len(pre) + 1])
        early[p][0].wait_recv()
        add_into(bufs[p], (*pre, up, lo), one_up[...])
        a = send(bufs[p].at[(*pre, up, lo)], two_up.at[lo], to_up)
        early[p][1].wait_recv()
        add_into(bufs[p], (*pre, down, hi), one_down[...])
        late.append((a, send(bufs[p].at[(*pre, down, hi)], two_down.at[hi], to_down)))
    yield
    sums = []
    for p, (axis, pre) in enumerate(zip(axes, pres)):
        for copy in early[p][2:]:
            copy.wait_recv()
        for copy in late[p]:
            copy.wait_recv()
        own = (*pre, at[axis])
        total = bufs[p][own].astype(F32)
        for ref in received[p][2:]:
            total = total + ref[...].astype(F32)
        if keep:
            bufs[p][own] = total.astype(BF)
        sums.append(total)
        if after:
            after(p)
    for p in range(len(axes)):
        for copy in (*early[p], *late[p]):
            copy.wait_send()
    yield sums


def reduce_torus(at, bufs, orders, line_received, plane_received, send):
    copies = []

    def to_plane(p):
        a, b, c = orders[p]
        copies.append([])
        for n, (db, da) in enumerate(plane_offsets()):
            there = {a: (at[a] + da) % 4, b: (at[b] + db) % 4}
            block = bufs[p].at[at[c], there[b], there[a]]
            copies[p].append(send(block, plane_received[p].at[n], device_at(at, **there)))

    axes = [order[-1] for order in orders]
    for _ in reduce_line(at, bufs, axes, ((),) * 3, line_received, send, True, to_plane):
        pass
    sums = []
    for p, order in enumerate(orders):
        a, b, c = order
        total = bufs[p][at[c], at[b], at[a]].astype(F32)
        for n, copy in enumerate(copies[p]):
            copy.wait()
            total = total + plane_received[p][n].astype(F32)
        sums.append(total)
    return sums


def split(v):
    high = v.astype(BF)
    return high, (v - high.astype(F32)).astype(BF)


INPUTS = (
    "x", "lengths", "gain", "wq", "wf", "wi", "wo", "bound", "shrink", "lane_gain", "state",
    "result", "later_gain", "gate", "wide", "narrow",
)
IN_HBM = ("x", "wq", "wf", "wi", "wo", "state", "result", "gate", "wide", "narrow")


def line_shapes(lead, tail, parts):
    shapes = []
    for count in parts:
        shape = (*lead, *((count,) if count else ()), *tail)
        half = shape[0] // 2
        shapes += [(half, *shape[1:]), (shape[0] - half, *shape[1:]), shape, shape]
    return shapes


def scratch():
    counts = [count for _, count in PARTS]
    boxes = [(4, 4, 4, count, 16, 128) for count in counts]
    named = [
        ("cols", (8, 32, 1024), BF),
        ("scaled", (1024, 256), BF),
        ("squares", (8, 8, 128), F32),
        ("squares_in", (15, 8, 128), F32),
        ("front_weights", (2, 256, 512), BF),
        ("pa", (4, 4, 64, 512), BF),
        ("pb", (4, 4, 64, 512), BF),
        ("z", (64, 1024), F32),
        ("query", (64, 256), F32),
        ("kept", (64, 256), F32),
        ("key", (64, 256), F32),
        ("output", (64, 256), F32),
        ("state_in", (8, 2, 128, 128), F32),
        ("state_out", (8, 2, 128, 128), F32),
        ("chosen", (512, 1024), BF),
        ("heads", (16, 2, 64, 128), BF),
        ("partial", (8, 64, 256), BF),
        ("arrived", (7, 64, 256), BF),
        ("own_gain", (8, 128), F32),
        ("gains", (8, 8, 128), F32),
        ("own_rows", (64, 256), F32),
        ("residual", (64, 256), F32),
        ("later_squares", (16, 8, 128), F32),
        ("squares_sum", (8, 128), F32),
        ("squares_line", (4, 8, 128), F32),
        ("weights", (2, 2, 128, 4096), BF),
        ("narrows", (2, 128, 4096), BF),
        ("staged", (3, 86, 4096), BF),
        ("result_in", (256, 256), BF),
        ("total", (2, 256, 256), F32),
        ("ypack", (8, 16, 128), BF),
        ("yarrive", (8, 16, 128), BF),
    ]
    groups = [
        ("gathered", boxes),
        ("terms", boxes),
        ("front_one", line_shapes((4, 64), (512,), (0, 0))),
        ("front_two", line_shapes((64,), (512,), (0, 0))),
        ("mixer_line", line_shapes((4, 4), (16, 128), counts)),
        ("mixer_plane", [(15, count, 16, 128) for count in counts]),
    ]
    flat = [pltpu.VMEM(shape, kind) for _, shape, kind in named]
    for _, shapes in groups:
        flat += [pltpu.VMEM(shape, BF) for shape in shapes]
    return named, groups, flat


def layer_kernel(*refs):
    named, groups, flat = scratch()
    ref = dict(zip(INPUTS, refs))
    mixed_out, place_out, state_result = refs[len(INPUTS) : len(INPUTS) + 3]
    rest = refs[len(INPUTS) + 3 :]
    ref.update(zip(["_" + name for name, _, _ in named], rest))
    rest = rest[len(named) :]
    group = {}
    for name, shapes in groups:
        group[name], rest = rest[: len(shapes)], rest[len(shapes) :]
    sends, recvs, local, ready = rest
    send = Sender(sends, recvs)
    at = my_position()
    kv = 4 * at["z"] + at["y"]
    tp = 2 * at["x"] + at["c"]
    planes, lines = plane_offsets(), line_offsets()
    fours = lambda refs: [refs[i : i + 4] for i in range(0, len(refs), 4)]

    def fetch(n, src, dst):
        copy = pltpu.make_async_copy(src, dst, local.at[n])
        copy.start()
        return copy

    cols = ref["_cols"]
    x_copy = fetch(0, ref["x"], cols.at[tp])
    front_copies = [
        fetch(1 + n, ref[name], ref["_front_weights"].at[n // 2, :, 256 * (n % 2) : 256 * (n % 2) + 256])
        for n, name in enumerate(("wq", "wf", "wi", "wo"))
    ]
    weight_copies = [
        fetch(5 + n, ref[name], ref["_staged"].at[n])
        for n, name in enumerate(("gate", "wide", "narrow"))
    ]
    state_copy = fetch(8, ref["state"], ref["_state_in"])
    result_copy = fetch(9, ref["result"], ref["_result_in"])
    turns = (1, 2, 3)
    meet(
        [line_peer(at, *d) for d in lines]
        + [plane_peer(at, dz, 0) for dz in turns]
        + [plane_peer(at, 0, dy) for dy in turns]
    )
    for dy in turns:
        pl.semaphore_signal(ready, inc=1, device_id=plane_peer(at, 0, dy), device_id_type=MESH)

    x_copy.wait()
    partner = line_peer(at, 0, 1)
    far_copies = [send(cols.at[tp], cols.at[tp], line_peer(at, dx, 0)) for dx in turns]
    near_copies = [send(cols.at[tp], cols.at[tp], partner)]
    own_gain, gains = ref["_own_gain"], ref["_gains"]
    own_gain[...] = jnp.broadcast_to(
        jnp.concatenate([ref["later_gain"][...], jnp.zeros((1, 96), F32)], axis=1), (8, 128)
    )
    gain_copies = [send(own_gain, gains.at[tp], line_peer(at, *d)) for d in lines]
    gains[pl.ds(tp, 1)] = own_gain[...][None]

    lengths = jnp.broadcast_to(ref["lengths"][...], (8, 128)).astype(F32).astype(BF)
    s = lax.broadcasted_iota(jnp.int32, (128, 1024), 0)
    owner = lax.broadcasted_iota(jnp.int32, (128, 1024), 1) // 8
    start = times(lengths, jnp.where(s < owner, 1.0, 0.0).astype(BF), ((1,), (0,)))
    length = times(lengths, jnp.where(s == owner, 1.0, 0.0).astype(BF), ((1,), (0,)))
    slot = lax.broadcasted_iota(jnp.int32, (8, 1024), 1) % 8
    place = jnp.where(slot < length.astype(jnp.int32), start.astype(jnp.int32) + slot, -1)
    place_out[...] = place
    place = place[0:1]
    for part in range(4):
        ref["_chosen"][128 * part : 128 * part + 128] = picks(place, 128 * part, 128)
    gain = jnp.concatenate(
        [column_of(ref["gain"][:, 0:128], 128), column_of(ref["gain"][:, 128:256], 128)], axis=0
    )
    weights, narrows, staged = ref["_weights"], ref["_narrows"], ref["_staged"]
    for n, first in ((0, 80), (1, 96)):
        weights[n, :, first:128] = jnp.zeros((2, 128 - first, 4096), BF)
        narrows[n, first:128] = jnp.zeros((128 - first, 4096), BF)
    for copy in weight_copies:
        copy.wait()
    weights[0, :, 0:86] = staged[0:2]
    narrows[0, 0:86] = staged[2]

    for dx, copy in zip(turns, far_copies):
        copy.wait()
        came = 2 * ((at["x"] + 4 - dx) % 4) + at["c"]
        near_copies.append(send(cols.at[came], cols.at[came], partner))
    for copy in near_copies:
        copy.wait()
    weight_sends = [
        send(weights.at[0, :, 0:96], weights.at[1, :, 0:96], partner),
        send(narrows.at[0, 0:96], narrows.at[1, 0:96], partner),
    ]
    scaled, squares = ref["_scaled"], ref["_squares"]
    for k in range(8):
        lanes = slice(128 * k, 128 * k + 128)
        v = cols[:, :, lanes].reshape(256, 128).astype(F32)
        scaled[lanes, :] = (v * gain).T.astype(BF)
        squares[k] = jnp.broadcast_to(jnp.sum(v * v, axis=0, keepdims=True), (8, 128))
    for copy in front_copies:
        copy.wait()
    pa, pb = ref["_pa"], ref["_pb"]

    def project(n):
        def body(a, carry):
            lhs = scaled[pl.ds(pl.multiple_of(256 * a, 256), 256), :]
            v = times(lhs, ref["_front_weights"][n], ((1,), (0,))).astype(BF).reshape(4, 64, 512)
            if n == 0:
                pa[:, a] = v
            else:
                pb[a] = v
            return carry

        lax.fori_loop(0, 4, body, 0)

    one, two = fours(group["front_one"]), fours(group["front_two"])
    project(0)
    steps_a = reduce_line(at, (pa,), ("y",), ((),), one[0:1], send)
    next(steps_a)
    project(1)
    steps_b = reduce_line(at, (pb,), ("z",), ((),), one[1:2], send)
    next(steps_b)
    pl.semaphore_wait(ready, 3)
    square_copies = []
    for i, (dz, dy) in enumerate(planes):
        peer = plane_peer(at, dz, dy)
        block = squares.at[(4 * peer[0] + peer[1]) // 2]
        square_copies.append(send(block, ref["_squares_in"].at[i], peer))
    ref["_own_rows"][...] = times(picks(place, 64 * tp, 64), cols[...].reshape(256, 1024))
    next(steps_a)
    next(steps_b)
    next(steps_a)
    steps_a = reduce_line(at, (pa,), ("z",), ((at["y"],),), two[0:1], send, False)
    next(steps_a)
    next(steps_b)
    steps_b = reduce_line(at, (pb,), ("y",), ((at["z"],),), two[1:2], send, False)
    next(steps_b)
    row = lax.broadcasted_iota(jnp.int32, (64, 128), 0)
    lane = lax.broadcasted_iota(jnp.int32, (64, 128), 1)
    length = jnp.sum(
        jnp.where(lane == 8 * kv + row // 8, ref["lengths"][...].astype(F32), 0.0),
        axis=1,
        keepdims=True,
    )
    live = (row[:, 0:1] % 8).astype(F32) < length
    for copy in square_copies:
        copy.wait()
    total = jnp.sum(ref["_squares_in"][...], axis=0) + squares[kv // 2]
    own = jnp.sum(
        jnp.where(lane == 64 * (kv % 2) + row, total[0:1, :], 0.0), axis=1, keepdims=True
    )
    scale = lax.rsqrt(own / 4096 + EPS)
    next(steps_a)
    next(steps_b)
    z = ref["_z"]
    z[:, 0:512] = next(steps_a)[0] * scale
    z[:, 512:1024] = next(steps_b)[0] * scale

    query, kept, keys, output = ref["_query"], ref["_kept"], ref["_key"], ref["_output"]
    slot = lax.broadcasted_iota(jnp.int32, (8, 8, 128), 1)
    state_in, state_out, heads = ref["_state_in"], ref["_state_out"], ref["_heads"]

    def read_state(h, n, carry):
        rows = pl.ds(pl.multiple_of(8 * n, 8), 8)
        lanes = slice(128 * h, 128 * h + 128)
        s_high, s_low = split(state_in[n, h])
        q_high, q_low = split(query[rows, lanes])
        lhs = jnp.concatenate(
            [
                jnp.concatenate([q_high, q_high], axis=1),
                jnp.concatenate([q_low, jnp.zeros_like(q_low)], axis=1),
            ],
            axis=0,
        )
        o = times(lhs, jnp.concatenate([s_high, s_low], axis=0), ((1,), (0,)))
        output[rows, lanes] += o[0:8] + o[8:16]
        return carry

    copies = []
    for h in range(2):
        lanes = slice(128 * h, 128 * h + 128)
        bound = ref["bound"][:, lanes]
        retain = bound + (1.0 - bound) * jax.nn.sigmoid(z[:, 256 + 128 * h : 384 + 128 * h])
        shrink = jnp.sum(
            jnp.where(lane[:, 0:64] == row[:, 0:64], ref["shrink"][h : h + 1, :], 0.0),
            axis=1,
            keepdims=True,
        )
        decay = jnp.where(live, jnp.exp(jnp.log(retain) + shrink), 1.0).reshape(8, 8, 128)
        key = jnp.where(live, 1.0 - retain, 0.0).reshape(8, 8, 128)
        zq = z[:, lanes]
        q = (zq * jax.nn.sigmoid(zq)).reshape(8, 8, 128)
        value = z[:, 512 + 128 * h : 640 + 128 * h].reshape(8, 8, 128)
        between = q
        out = jnp.sum(q * key, axis=2, keepdims=True) * value
        for back in range(1, 8):
            between = between * (decay if back == 1 else pltpu.roll(decay, back - 1, 1))
            weight = jnp.sum(between * pltpu.roll(key, back, 1), axis=2, keepdims=True)
            out = out + jnp.where(slot >= back, weight * pltpu.roll(value, back, 1), 0.0)
        output[:, lanes] = out.reshape(64, 128)
        before, after = decay, jnp.where(slot < 7, pltpu.roll(decay, 7, 1), 1.0)
        for step in (1, 2, 4):
            before = before * jnp.where(slot >= step, pltpu.roll(before, step, 1), 1.0)
            after = after * jnp.where(slot + step < 8, pltpu.roll(after, 8 - step, 1), 1.0)
        query[:, lanes] = (q * before).reshape(64, 128)
        kept[:, lanes] = before.reshape(64, 128)
        keys[:, lanes] = (key * after).reshape(64, 128)
        if h == 0:
            state_copy.wait()
        lax.fori_loop(0, 8, functools.partial(read_state, h), 0, unroll=2)
        o = output[:, lanes]
        zo = z[:, 768 + 128 * h : 896 + 128 * h]
        o = o * lax.rsqrt(jnp.mean(o * o, axis=1, keepdims=True) + EPS) * ref["lane_gain"][...]
        heads[kv, h] = jnp.where(live, o * (zo * jax.nn.sigmoid(zo)), 0.0).astype(BF)
        own = heads.at[kv, h]
        copies += [send(own, own, plane_peer(at, *d)) for d in planes]
    def write_state(n, carry):
        rows = pl.ds(pl.multiple_of(8 * n, 8), 8)
        for h in range(2):
            lanes = slice(128 * h, 128 * h + 128)
            k_high, k_low = split(keys[rows, lanes])
            v_high, v_low = split(z[rows, 512 + 128 * h : 640 + 128 * h])
            added = times(
                jnp.concatenate([k_high, k_high, k_low], axis=0),
                jnp.concatenate([v_high, v_low, v_high], axis=0),
                ((0,), (0,)),
            )
            state_out[n, h] = column_of(kept[rows, lanes][7:8, :], 128) * state_in[n, h] + added
        return carry

    lax.fori_loop(0, 8, write_state, 0)
    new_copy = fetch(10, state_out, state_result)
    result_copy.wait()
    for copy in gain_copies:
        copy.wait()
    gain = jnp.concatenate([gains[t, 0:1, 0:32] for t in range(8)], axis=1)
    for copy in copies:
        copy.wait()

    partial, arrived, result = ref["_partial"], ref["_arrived"], ref["_result_in"]
    all_heads = jnp.concatenate([heads[:, h].reshape(1024, 128) for h in range(2)], axis=1)
    for part in range(2):
        picked = ref["_chosen"][256 * part : 256 * part + 256]
        packed = times(picked, all_heads, ((1,), (0,))).astype(BF)
        partial[4 * part : 4 * part + 4] = (
            times(packed, result[...], ((1,), (0,))).astype(BF).reshape(4, 64, 256)
        )
    copies = []
    for i, (dx, dc) in enumerate(lines):
        peer = line_peer(at, dx, dc)
        copies.append(send(partial.at[2 * peer[2] + peer[3]], arrived.at[i], peer))
    attended = partial[tp].astype(F32)
    for i, copy in enumerate(copies):
        copy.wait()
        attended = attended + arrived[i].astype(F32)
    residual = (ref["_own_rows"][...] + attended).astype(BF).astype(F32)
    tile = (residual * gain).astype(BF)
    blocks = [
        tile[16 * i : 16 * i + 16, 128 * h : 128 * h + 128] for h in range(2) for i in range(4)
    ]
    gathered = group["gathered"]
    for p, ((first, count), order) in enumerate(zip(PARTS, ORDERS)):
        idx = tuple(at[a] for a in order[::-1])
        for b in range(count):
            gathered[p][(*idx, b)] = blocks[first + b]
    copies = gather_plane(at, gathered, ORDERS, send)
    ref["_residual"][...] = residual
    later = ref["_later_squares"]
    own_squares = jnp.sum(residual * residual, axis=1, keepdims=True)
    later[0] = jnp.broadcast_to(row_of(own_squares, 64), (8, 128))
    square_copies = [
        send(later.at[0], later.at[1 + i], plane_peer(at, *d)) for i, d in enumerate(planes)
    ]
    steps = gather_line(at, gathered, ORDERS, copies, send)
    next(steps)
    for copy in square_copies:
        copy.wait()
    squares_sum, squares_line = ref["_squares_sum"], ref["_squares_line"]
    own_sum = jnp.sum(later[...], axis=0)
    squares_sum[...] = own_sum
    squares_line[pl.ds(at["x"], 1)] = own_sum[None]
    line_copies = [
        send(squares_sum, squares_line.at[at["x"]], line_peer(at, dx, 0)) for dx in (1, 2, 3)
    ]
    next(steps)
    for copy in (*line_copies, *weight_sends):
        copy.wait()

    ga, gb, gc = gathered
    total = ref["_total"]

    def rows_at(zz, yy):
        v = jnp.concatenate([ga[zz, yy], gb[:, zz, yy], gc[yy, :, zz]], axis=1)
        return jnp.concatenate(
            [v[:, 0:4].reshape(256, 128), v[:, 4:8].reshape(256, 128)], axis=1
        )

    total[...] = jnp.zeros_like(total)

    def widening(zz, carry):
        lhs = jnp.concatenate([rows_at(zz, yy) for yy in range(4)], axis=1)
        cols = pl.ds(pl.multiple_of(zz * 1024, 1024), 1024)
        for core in range(2):
            total[core] += times(lhs, weights[core, :, :, cols].reshape(256, 1024))
        return carry

    lax.fori_loop(0, 4, widening, 0)
    scale = lax.rsqrt(
        jnp.concatenate([column_of(squares_line[g, 0:1, :], 64) for g in range(4)], axis=0)
        / 4096
        + EPS
    )
    hidden = []
    for core in range(2):
        gated = total[core, :, 0:128] * scale
        upward = total[core, :, 128:256] * scale
        hidden.append((gated * jax.nn.sigmoid(gated) * upward).astype(BF))
    hidden = jnp.concatenate(hidden, axis=1)
    ta, tb, tc = group["terms"]

    def narrowing(zz, carry):
        cols = pl.ds(pl.multiple_of(zz * 1024, 1024), 1024)
        rhs = jnp.concatenate([narrows[0, :, cols], narrows[1, :, cols]], axis=0)
        term = times(hidden, rhs, ((1,), (0,))).astype(BF)
        for yy in range(4):
            v = jnp.concatenate(
                [
                    term[:, 256 * yy + 128 * h : 256 * yy + 128 * h + 128].reshape(4, 4, 16, 128)
                    for h in range(2)
                ],
                axis=1,
            )
            ta[zz, yy] = v[:, 0:3]
            tb[:, zz, yy] = v[:, 3:6]
            tc[yy, :, zz] = v[:, 6:8]
        return carry

    lax.fori_loop(0, 4, narrowing, 0)
    sums = jnp.concatenate(
        reduce_torus(
            at, group["terms"], ORDERS, fours(group["mixer_line"]), group["mixer_plane"], send
        ),
        axis=0,
    )

    mixed = []
    for h in range(2):
        for i in range(4):
            res = ref["_residual"][16 * i : 16 * i + 16, 128 * h : 128 * h + 128]
            mixed.append((res + sums[4 * h + i]).astype(BF))
    ypack, yarrive = ref["_ypack"], ref["_yarrive"]
    for t in range(8):
        h, first = t // 4, 32 * (t % 4)
        ypack[t] = jnp.concatenate(
            [mixed[4 * h + i][:, first : first + 32] for i in range(4)], axis=1
        )
    copies = []
    for dx, dc in lines:
        peer = line_peer(at, dx, dc)
        copies.append(send(ypack.at[2 * peer[2] + peer[3]], yarrive.at[tp], peer))
    yarrive[pl.ds(tp, 1)] = ypack[pl.ds(tp, 1)]
    for copy in copies:
        copy.wait()
    mixed_out[...] = yarrive[...]
    new_copy.wait()
    assert send.used <= sends.shape[0]


def layer(*arguments):
    vmem = pl.BlockSpec(memory_space=pltpu.VMEM)
    far = pl.BlockSpec(memory_space=pltpu.HBM)
    copies = 280
    return pl.pallas_call(
        layer_kernel,
        out_shape=(
            jax.ShapeDtypeStruct((8, 16, 128), BF),
            jax.ShapeDtypeStruct((8, 1024), jnp.int32),
            jax.ShapeDtypeStruct((8, 2, 128, 128), F32),
        ),
        in_specs=[far if name in IN_HBM else vmem for name in INPUTS],
        out_specs=(vmem, vmem, far),
        scratch_shapes=[
            *scratch()[2],
            pltpu.SemaphoreType.DMA((copies,)),
            pltpu.SemaphoreType.DMA((copies,)),
            pltpu.SemaphoreType.DMA((11,)),
            pltpu.SemaphoreType.REGULAR,
        ],
        compiler_params=pltpu.CompilerParams(
            collective_id=0, has_side_effects=True, vmem_limit_bytes=67043328
        ),
        name="layer",
    )(*arguments)


def finish_kernel(packed_ref, place_ref, state_ref, mixed_ref, new_ref, held, sems):
    take = pltpu.make_async_copy(state_ref, held, sems.at[0])
    take.start()
    j = lax.broadcasted_iota(jnp.int32, (128, 1024), 0)
    rows = 64 * (j // 16) + j % 16 - place_ref[0:1, :]
    packed = packed_ref[...].reshape(128, 128)
    mixed = jnp.zeros((32, 1024), F32)
    for a in range(4):
        chosen = jnp.where(rows == -16 * a, 1.0, 0.0).astype(BF)
        mixed = mixed + times(packed[:, 32 * a : 32 * a + 32], chosen, ((0,), (0,)))
    take.wait()
    give = pltpu.make_async_copy(held, new_ref, sems.at[1])
    give.start()
    mixed_ref[...] = mixed.astype(BF)
    give.wait()


def finish(packed, place, state):
    vmem = pl.BlockSpec(memory_space=pltpu.VMEM)
    far = pl.BlockSpec(memory_space=pltpu.HBM)
    return pl.pallas_call(
        finish_kernel,
        out_shape=(
            jax.ShapeDtypeStruct((32, 1024), BF),
            jax.ShapeDtypeStruct((8, 2, 128, 128), F32),
        ),
        in_specs=[vmem, vmem, far],
        out_specs=(vmem, far),
        scratch_shapes=[pltpu.VMEM((8, 2, 128, 128), F32), pltpu.SemaphoreType.DMA((2,))],
        compiler_params=pltpu.CompilerParams(vmem_limit_bytes=67043328),
        name="finish",
    )(packed, place, state)


def local(
    residual_entries,
    fresh_extents,
    memory_matrix,
    initial_rescale_vector,
    probe_matrix,
    retain_matrix,
    content_matrix,
    result_switch_matrix,
    retain_lower_limit,
    extra_shrink_log,
    lane_result_rescale,
    result_matrix,
    later_rescale_vector,
    mixer_switch_matrix,
    widening_matrix,
    narrowing_matrix,
):
    packed, place, new_state = layer(
        residual_entries.T,
        fresh_extents.reshape(1, 128),
        initial_rescale_vector.reshape(1, 256),
        probe_matrix,
        retain_matrix,
        content_matrix,
        result_switch_matrix,
        retain_lower_limit.reshape(1, 256),
        extra_shrink_log.T,
        lane_result_rescale.reshape(1, 128),
        memory_matrix,
        result_matrix,
        later_rescale_vector.reshape(1, 32),
        mixer_switch_matrix.T,
        widening_matrix.T,
        narrowing_matrix,
    )
    mixed, carried = finish(packed, place, new_state)
    return (mixed.T, carried)


def solution(mesh):
    torus = Mesh(mesh.devices.reshape(4, 4, 4, 2), ("kv_0", "kv_1", "tp_0", "tp_1"))
    placed = (
        P(None, KV_TP),
        P(),
        P(KV, TP, None, None),
        P(KV),
        P(KV, TP),
        P(KV, TP),
        P(KV, TP),
        P(KV, TP),
        P(TP),
        P(KV, TP),
        P(),
        P(TP, KV),
        P(KV_TP),
        P(None, KV_TP),
        P(None, KV_TP),
        P(KV_TP, None),
    )
    return jax.shard_map(
        local,
        mesh=torus,
        in_specs=placed,
        out_specs=(P(None, KV_TP), P(KV, TP, None, None)),
        check_vma=False,
    )
```

```python
import functools

import jax
import jax.numpy as jnp
from jax import lax
from jax.experimental import pallas as pl
from jax.experimental.pallas import tpu as pltpu
from jax.sharding import Mesh
from jax.sharding import PartitionSpec as P

KV = ("kv_0", "kv_1")
TP = ("tp_0", "tp_1")
KV_TP = ("kv_0", "kv_1", "tp_0", "tp_1")
MESH = pl.DeviceIdType.MESH
EPS = 1e-06
F32 = jnp.float32
BF = jnp.bfloat16
PARTS = ((0, 3), (3, 3), (6, 2))
ORDERS = ("xyz", "yzx", "zxy")
ROWS = (0, 1, 3, 2)


def my_position():
    return dict(
        z=lax.axis_index("kv_0"),
        y=lax.axis_index("kv_1"),
        x=lax.axis_index("tp_0"),
        c=lax.axis_index("tp_1"),
    )


def device_at(at, **moved):
    there = dict(at, **moved)
    return (there["z"], there["y"], there["x"], there["c"])


def plane_offsets():
    return [(dz, dy) for dz in range(4) for dy in range(4) if dz or dy]


def line_offsets():
    return [(dx, dc) for dx in range(4) for dc in range(2) if dx or dc]


def plane_peer(at, dz, dy):
    return device_at(at, z=(at["z"] + dz) % 4, y=(at["y"] + dy) % 4)


def line_peer(at, dx, dc):
    return device_at(at, x=(at["x"] + dx) % 4, c=(at["c"] + dc) % 2)


def meet(peers, meanwhile):
    barrier = pltpu.get_barrier_semaphore()
    for peer in peers:
        pl.semaphore_signal(barrier, inc=1, device_id=peer, device_id_type=MESH)
    meanwhile()
    pl.semaphore_wait(barrier, len(peers))


class Sender:
    def __init__(self, sends, recvs):
        self.sends, self.recvs, self.used = sends, recvs, 0

    def __call__(self, src, dst, peer):
        i = self.used
        self.used = i + 1
        return start_copy(src, dst, self.sends.at[i], self.recvs.at[i], peer)


def start_copy(src, dst, send_sem, recv_sem, peer):
    copy = pltpu.make_async_remote_copy(
        src_ref=src,
        dst_ref=dst,
        send_sem=send_sem,
        recv_sem=recv_sem,
        device_id=peer,
        device_id_type=MESH,
    )
    copy.start()
    return copy


def times(a, b, dims=((1,), (1,))):
    return lax.dot_general(a, b, (dims, ((), ())), preferred_element_type=F32)


def row_of(column, rows):
    eye = lax.broadcasted_iota(jnp.int32, (rows, 128), 0) == lax.broadcasted_iota(
        jnp.int32, (rows, 128), 1
    )
    return jnp.sum(jnp.where(eye, column, 0.0), axis=0, keepdims=True)


def column_of(row, rows):
    eye = lax.broadcasted_iota(jnp.int32, (rows, 128), 0) == lax.broadcasted_iota(
        jnp.int32, (rows, 128), 1
    )
    return jnp.sum(jnp.where(eye, row, 0.0), axis=1, keepdims=True)


def picks(place, start, rows):
    want = lax.broadcasted_iota(jnp.int32, (rows, 1024), 0) + start
    return jnp.where(want == place, 1.0, 0.0).astype(BF)


def halves(length):
    return pl.ds(0, length // 2), pl.ds(length // 2, length - length // 2)


def gather_plane(at, bufs, orders, send):
    copies = [{} for _ in orders]
    for db in ROWS:
        for p, order in enumerate(orders):
            a, b, c = order
            own = bufs[p].at[at[c], at[b], at[a]]
            for da in range(4):
                if db or da:
                    there = {a: (at[a] + da) % 4, b: (at[b] + db) % 4}
                    copies[p][db, da] = send(own, own, device_at(at, **there))
    return copies


def gather_line(at, bufs, orders, plane, send):
    first = {}
    for db in ROWS:
        for p, (a, b, c) in enumerate(orders):
            for da in range(4):
                if db or da:
                    plane[p][db, da].wait_recv()
            own = bufs[p].at[at[c], (at[b] + 4 - db) % 4]
            first[p, db] = tuple(
                send(own, own, device_at(at, **{c: (at[c] + turn) % 4})) for turn in (1, 3)
            )
    yield
    second = []
    for db in ROWS:
        for p, (a, b, c) in enumerate(orders):
            for copy in first[p, db]:
                copy.wait_recv()
            turn = 1 if db in (0, 2) else 3
            came = bufs[p].at[(at[c] + 4 - turn) % 4, (at[b] + 4 - db) % 4]
            second.append(send(came, came, device_at(at, **{c: (at[c] + turn) % 4})))
    for part in (*[part.values() for part in plane], *first.values()):
        for copy in part:
            copy.wait_send()
    for copy in second:
        copy.wait()
    yield


def add_into(ref, idx, term):
    ref[idx] = (ref[idx].astype(F32) + term.astype(F32)).astype(BF)


def reduce_line(at, bufs, axes, pres, received, send, keep=True, after=None):
    early = []
    for p, (axis, pre) in enumerate(zip(axes, pres)):
        one_up, one_down, two_up, two_down = received[p]
        m = at[axis]
        up, down, away = (m + 1) % 4, (m + 3) % 4, (m + 2) % 4
        to_up, to_down = device_at(at, **{axis: up}), device_at(at, **{axis: down})
        lo, hi = halves(bufs[p].shape[len(pre) + 1])
        early.append((
            send(bufs[p].at[(*pre, away, lo)], one_up, to_up),
            send(bufs[p].at[(*pre, away, hi)], one_down, to_down),
            send(bufs[p].at[(*pre, up, hi)], two_up.at[hi], to_up),
            send(bufs[p].at[(*pre, down, lo)], two_down.at[lo], to_down),
        ))
    yield
    late = []
    for p, (axis, pre) in enumerate(zip(axes, pres)):
        one_up, one_down, two_up, two_down = received[p]
        m = at[axis]
        up, down = (m + 1) % 4, (m + 3) % 4
        to_up, to_down = device_at(at, **{axis: up}), device_at(at, **{axis: down})
        lo, hi = halves(bufs[p].shape[len(pre) + 1])
        early[p][0].wait_recv()
        add_into(bufs[p], (*pre, up, lo), one_up[...])
        a = send(bufs[p].at[(*pre, up, lo)], two_up.at[lo], to_up)
        early[p][1].wait_recv()
        add_into(bufs[p], (*pre, down, hi), one_down[...])
        late.append((a, send(bufs[p].at[(*pre, down, hi)], two_down.at[hi], to_down)))
    yield
    sums = []
    for p, (axis, pre) in enumerate(zip(axes, pres)):
        for copy in early[p][2:]:
            copy.wait_recv()
        for copy in late[p]:
            copy.wait_recv()
        own = (*pre, at[axis])
        total = bufs[p][own].astype(F32)
        for ref in received[p][2:]:
            total = total + ref[...].astype(F32)
        if keep:
            bufs[p][own] = total.astype(BF)
        sums.append(total)
        if after:
            after(p)
    for p in range(len(axes)):
        for copy in (*early[p], *late[p]):
            copy.wait_send()
    yield sums


def reduce_torus(at, bufs, orders, line_received, plane_received, send):
    early, late, plane = {}, {}, {}
    lo, hi = pl.ds(0, 2), pl.ds(2, 2)

    def row(p, db):
        a, b, c = orders[p]
        m = at[c]
        return c, m, (m + 1) % 4, (m + 3) % 4, (at[b] + db) % 4

    def begin(db):
        for p in range(len(orders)):
            c, m, up, down, r = row(p, db)
            one_up, one_down, two_up, two_down = line_received[p]
            to_up, to_down = device_at(at, **{c: up}), device_at(at, **{c: down})
            away = (m + 2) % 4
            early[p, db] = (
                send(bufs[p].at[away, r, lo], one_up.at[db], to_up),
                send(bufs[p].at[away, r, hi], one_down.at[db], to_down),
                send(bufs[p].at[up, r, hi], two_up.at[db, hi], to_up),
                send(bufs[p].at[down, r, lo], two_down.at[db, lo], to_down),
            )

    def go_on(db):
        for p in range(len(orders)):
            c, m, up, down, r = row(p, db)
            one_up, one_down, two_up, two_down = line_received[p]
            to_up, to_down = device_at(at, **{c: up}), device_at(at, **{c: down})
            early[p, db][0].wait_recv()
            add_into(bufs[p], (up, r, lo), one_up[db])
            first = send(bufs[p].at[up, r, lo], two_up.at[db, lo], to_up)
            early[p, db][1].wait_recv()
            add_into(bufs[p], (down, r, hi), one_down[db])
            late[p, db] = (first, send(bufs[p].at[down, r, hi], two_down.at[db, hi], to_down))

    def end(db):
        for p, (a, b, c) in enumerate(orders):
            _, m, up, down, r = row(p, db)
            two_up, two_down = line_received[p][2:]
            for copy in (*early[p, db][2:], *late[p, db]):
                copy.wait_recv()
            total = bufs[p][m, r].astype(F32) + two_up[db].astype(F32) + two_down[db].astype(F32)
            bufs[p][m, r] = total.astype(BF)
            for da in range(4):
                if db or da:
                    n = 4 * db + da - 1
                    there = {a: (at[a] + da) % 4, b: r}
                    block = bufs[p].at[m, r, there[a]]
                    plane[p, n] = send(block, plane_received[p].at[n], device_at(at, **there))

    rows = ROWS[::-1]
    for db in rows:
        begin(db)
    for db in rows:
        go_on(db)
    for db in rows:
        end(db)
    sums = []
    for p, (a, b, c) in enumerate(orders):
        total = bufs[p][at[c], at[b], at[a]].astype(F32)
        for n in range(14, -1, -1):
            plane[p, n].wait_recv()
            total = total + plane_received[p][n].astype(F32)
        sums.append(total)
    for copies in (*early.values(), *late.values(), plane.values()):
        for copy in copies:
            copy.wait_send()
    return sums


def split(v):
    high = v.astype(BF)
    return high, (v - high.astype(F32)).astype(BF)


INPUTS = (
    "x", "lengths", "gain", "wq", "wf", "wi", "wo", "bound", "shrink", "lane_gain", "state",
    "result", "later_gain", "gate", "wide", "narrow",
)
SMALL = (
    ("lengths", (1, 128), jnp.int32),
    ("gain", (1, 256), F32),
    ("bound", (1, 256), F32),
    ("shrink", (2, 64), F32),
    ("lane_gain", (1, 128), F32),
    ("later_gain", (1, 32), F32),
)


def line_shapes(shape, count):
    shapes = []
    for _ in range(count):
        half = shape[0] // 2
        shapes += [(half, *shape[1:]), (shape[0] - half, *shape[1:]), shape, shape]
    return shapes


def scratch():
    counts = [count for _, count in PARTS]
    boxes = [(4, 4, 4, count, 16, 128) for count in counts]
    named = [
        *[("small_" + name, shape, kind) for name, shape, kind in SMALL],
        ("cols", (8, 32, 1024), BF),
        ("scaled", (1024, 256), BF),
        ("squares", (8, 8, 128), F32),
        ("squares_in", (15, 8, 128), F32),
        ("front_weights", (4, 256, 256), BF),
        ("pa", (2, 4, 4, 64, 256), BF),
        ("pb", (2, 4, 4, 64, 256), BF),
        ("z", (64, 1024), F32),
        ("query", (64, 256), F32),
        ("kept", (64, 256), F32),
        ("key", (64, 256), F32),
        ("output", (64, 256), F32),
        ("state_in", (8, 2, 128, 128), F32),
        ("state_out", (8, 2, 128, 128), F32),
        ("chosen", (512, 1024), BF),
        ("heads", (16, 2, 64, 128), BF),
        ("partial", (8, 64, 256), BF),
        ("arrived", (7, 64, 256), BF),
        ("own_gain", (8, 128), F32),
        ("gains", (8, 8, 128), F32),
        ("own_rows", (64, 256), F32),
        ("residual", (64, 256), F32),
        ("later_squares", (16, 8, 128), F32),
        ("squares_sum", (8, 128), F32),
        ("squares_line", (4, 8, 128), F32),
        ("weights", (2, 2, 128, 4096), BF),
        ("narrows", (2, 128, 4096), BF),
        ("staged", (3, 86, 4096), BF),
        ("result_in", (256, 256), BF),
        ("total", (2, 256, 256), F32),
        ("ypack", (8, 16, 128), BF),
        ("yarrive", (8, 16, 128), BF),
    ]
    groups = [
        ("gathered", boxes),
        ("terms", boxes),
        ("front_one", line_shapes((4, 64, 256), 4)),
        ("front_two", [(3, 64, 256)] * 4),
        (
            "mixer_line",
            [(4, n, count, 16, 128) for count in counts for n in (2, 2, 4, 4)],
        ),
        ("mixer_plane", [(15, count, 16, 128) for count in counts]),
    ]
    flat = [pltpu.VMEM(shape, kind) for _, shape, kind in named]
    for _, shapes in groups:
        flat += [pltpu.VMEM(shape, BF) for shape in shapes]
    return named, groups, flat


def layer_kernel(*refs):
    named, groups, flat = scratch()
    ref = dict(zip(INPUTS, refs))
    mixed_out, place_out, state_result = refs[len(INPUTS) : len(INPUTS) + 3]
    rest = refs[len(INPUTS) + 3 :]
    ref.update(zip(["_" + name for name, _, _ in named], rest))
    rest = rest[len(named) :]
    group = {}
    for name, shapes in groups:
        group[name], rest = rest[: len(shapes)], rest[len(shapes) :]
    sends, recvs, local, ready = rest
    send = Sender(sends, recvs)
    at = my_position()
    kv = 4 * at["z"] + at["y"]
    tp = 2 * at["x"] + at["c"]
    planes, lines = plane_offsets(), line_offsets()
    fours = lambda refs: [refs[i : i + 4] for i in range(0, len(refs), 4)]

    def fetch(n, src, dst):
        copy = pltpu.make_async_copy(src, dst, local.at[n])
        copy.start()
        return copy

    cols = ref["_cols"]
    small_copies = [
        fetch(11 + n, ref[name], ref["_small_" + name]) for n, (name, _, _) in enumerate(SMALL)
    ]
    for name, _, _ in SMALL:
        ref[name] = ref["_small_" + name]
    x_copy = fetch(0, ref["x"], cols.at[tp])
    front_copies = [
        fetch(1 + n, ref[name], ref["_front_weights"].at[n])
        for n, name in enumerate(("wq", "wf", "wi", "wo"))
    ]
    weight_copies = [
        fetch(5 + n, ref[name], ref["_staged"].at[n])
        for n, name in enumerate(("gate", "wide", "narrow"))
    ]
    state_copy = fetch(8, ref["state"], ref["_state_in"])
    result_copy = fetch(9, ref["result"], ref["_result_in"])
    weights, narrows, staged = ref["_weights"], ref["_narrows"], ref["_staged"]

    def pad_weights():
        for n, first in ((0, 80), (1, 96)):
            weights[n, :, first:128] = jnp.zeros((2, 128 - first, 4096), BF)
            narrows[n, first:128] = jnp.zeros((128 - first, 4096), BF)
        for copy in weight_copies:
            copy.wait()
        weights[0, :, 0:86] = staged[0:2]
        narrows[0, 0:86] = staged[2]

    turns = (1, 2, 3)
    meet(
        [line_peer(at, *d) for d in lines]
        + [plane_peer(at, dz, 0) for dz in turns]
        + [plane_peer(at, 0, dy) for dy in turns],
        pad_weights,
    )
    for dy in turns:
        pl.semaphore_signal(ready, inc=1, device_id=plane_peer(at, 0, dy), device_id_type=MESH)

    x_copy.wait()
    partner = line_peer(at, 0, 1)
    far_copies = [send(cols.at[tp], cols.at[tp], line_peer(at, dx, 0)) for dx in turns]
    near_copies = [send(cols.at[tp], cols.at[tp], partner)]
    for copy in small_copies:
        copy.wait()
    own_gain, gains = ref["_own_gain"], ref["_gains"]
    own_gain[...] = jnp.broadcast_to(
        jnp.concatenate([ref["later_gain"][...], jnp.zeros((1, 96), F32)], axis=1), (8, 128)
    )
    gain_copies = [send(own_gain, gains.at[tp], line_peer(at, *d)) for d in lines]
    gains[pl.ds(tp, 1)] = own_gain[...][None]

    lengths = jnp.broadcast_to(ref["lengths"][...], (8, 128)).astype(F32).astype(BF)
    s = lax.broadcasted_iota(jnp.int32, (128, 1024), 0)
    owner = lax.broadcasted_iota(jnp.int32, (128, 1024), 1) // 8
    start = times(lengths, jnp.where(s < owner, 1.0, 0.0).astype(BF), ((1,), (0,)))
    length = times(lengths, jnp.where(s == owner, 1.0, 0.0).astype(BF), ((1,), (0,)))
    slot = lax.broadcasted_iota(jnp.int32, (8, 1024), 1) % 8
    place = jnp.where(slot < length.astype(jnp.int32), start.astype(jnp.int32) + slot, -1)
    place_out[...] = place
    place = place[0:1]
    for part in range(4):
        ref["_chosen"][128 * part : 128 * part + 128] = picks(place, 128 * part, 128)
    gain = jnp.concatenate(
        [column_of(ref["gain"][:, 0:128], 128), column_of(ref["gain"][:, 128:256], 128)], axis=0
    )
    for dx, copy in zip(turns, far_copies):
        copy.wait()
        came = 2 * ((at["x"] + 4 - dx) % 4) + at["c"]
        near_copies.append(send(cols.at[came], cols.at[came], partner))
    for copy in near_copies:
        copy.wait()
    scaled, squares = ref["_scaled"], ref["_squares"]
    for k in range(8):
        lanes = slice(128 * k, 128 * k + 128)
        v = cols[:, :, lanes].reshape(256, 128).astype(F32)
        scaled[lanes, :] = (v * gain).astype(BF).T
        squares[k] = jnp.broadcast_to(jnp.sum(v * v, axis=0, keepdims=True), (8, 128))
    for copy in front_copies:
        copy.wait()
    pa, pb = ref["_pa"], ref["_pb"]

    chunks = ((0, pa.at[0], "yz"), (1, pb.at[0], "zy"), (2, pa.at[1], "yz"), (3, pb.at[1], "zy"))
    one, two = fours(group["front_one"]), group["front_two"]

    def project(n, terms, order):
        def body(a, carry):
            lhs = scaled[pl.ds(pl.multiple_of(256 * a, 256), 256), :]
            v = times(lhs, ref["_front_weights"][n], ((1,), (0,))).astype(BF).reshape(4, 64, 256)
            if order == "yz":
                terms[:, a] = v
            else:
                terms[a] = v
            return carry

        lax.fori_loop(0, 4, body, 0)

    lines_one = []
    for n, terms, order in chunks:
        project(n, terms, order)
        lines_one.append(reduce_line(at, (terms,), order[0], ((),), one[n : n + 1], send))
        next(lines_one[n])
    pl.semaphore_wait(ready, 3)
    square_copies = []
    for i, (dz, dy) in enumerate(planes):
        peer = plane_peer(at, dz, dy)
        block = squares.at[(4 * peer[0] + peer[1]) // 2]
        square_copies.append(send(block, ref["_squares_in"].at[i], peer))
    ref["_own_rows"][...] = times(picks(place, 64 * tp, 64), cols[...].reshape(256, 1024))
    for step in lines_one:
        next(step)
    second = []
    for n, terms, order in chunks:
        next(lines_one[n])
        here, axis = at[order[0]], order[1]
        second.append([])
        for turn in turns:
            there = (at[axis] + turn) % 4
            peer = device_at(at, **{axis: there})
            second[n].append(send(terms.at[here, there], two[n].at[turn - 1], peer))
    row = lax.broadcasted_iota(jnp.int32, (64, 128), 0)
    lane = lax.broadcasted_iota(jnp.int32, (64, 128), 1)
    length = jnp.sum(
        jnp.where(lane == 8 * kv + row // 8, ref["lengths"][...].astype(F32), 0.0),
        axis=1,
        keepdims=True,
    )
    live = (row[:, 0:1] % 8).astype(F32) < length
    for copy in square_copies:
        copy.wait()
    total = jnp.sum(ref["_squares_in"][...], axis=0) + squares[kv // 2]
    own = jnp.sum(
        jnp.where(lane == 64 * (kv % 2) + row, total[0:1, :], 0.0), axis=1, keepdims=True
    )
    scale = lax.rsqrt(own / 4096 + EPS)
    z = ref["_z"]
    for n, terms, order in chunks:
        total = terms[at[order[0]], at[order[1]]].astype(F32)
        for i, copy in enumerate(second[n]):
            copy.wait()
            total = total + two[n][i].astype(F32)
        z[:, 256 * n : 256 * n + 256] = total * scale

    weight_sends = [
        send(weights.at[0, :, 0:96], weights.at[1, :, 0:96], partner),
        send(narrows.at[0, 0:96], narrows.at[1, 0:96], partner),
    ]

    query, kept, keys, output = ref["_query"], ref["_kept"], ref["_key"], ref["_output"]
    slot = lax.broadcasted_iota(jnp.int32, (8, 8, 128), 1)
    state_in, state_out, heads = ref["_state_in"], ref["_state_out"], ref["_heads"]

    def read_state(h, n, carry):
        rows = pl.ds(pl.multiple_of(8 * n, 8), 8)
        lanes = slice(128 * h, 128 * h + 128)
        s_high, s_low = split(state_in[n, h])
        q_high, q_low = split(query[rows, lanes])
        lhs = jnp.concatenate(
            [
                jnp.concatenate([q_high, q_high], axis=1),
                jnp.concatenate([q_low, jnp.zeros_like(q_low)], axis=1),
            ],
            axis=0,
        )
        o = times(lhs, jnp.concatenate([s_high, s_low], axis=0), ((1,), (0,)))
        output[rows, lanes] += o[0:8] + o[8:16]
        return carry

    copies = []
    for h in range(2):
        lanes = slice(128 * h, 128 * h + 128)
        bound = ref["bound"][:, lanes]
        retain = bound + (1.0 - bound) * jax.nn.sigmoid(z[:, 256 + 128 * h : 384 + 128 * h])
        shrink = jnp.sum(
            jnp.where(lane[:, 0:64] == row[:, 0:64], ref["shrink"][h : h + 1, :], 0.0),
            axis=1,
            keepdims=True,
        )
        decay = jnp.where(live, jnp.exp(jnp.log(retain) + shrink), 1.0).reshape(8, 8, 128)
        key = jnp.where(live, 1.0 - retain, 0.0).reshape(8, 8, 128)
        zq = z[:, lanes]
        q = (zq * jax.nn.sigmoid(zq)).reshape(8, 8, 128)
        value = z[:, 512 + 128 * h : 640 + 128 * h].reshape(8, 8, 128)
        between = q
        out = jnp.sum(q * key, axis=2, keepdims=True) * value
        for back in range(1, 8):
            between = between * (decay if back == 1 else pltpu.roll(decay, back - 1, 1))
            weight = jnp.sum(between * pltpu.roll(key, back, 1), axis=2, keepdims=True)
            out = out + jnp.where(slot >= back, weight * pltpu.roll(value, back, 1), 0.0)
        output[:, lanes] = out.reshape(64, 128)
        before, after = decay, jnp.where(slot < 7, pltpu.roll(decay, 7, 1), 1.0)
        for step in (1, 2, 4):
            before = before * jnp.where(slot >= step, pltpu.roll(before, step, 1), 1.0)
            after = after * jnp.where(slot + step < 8, pltpu.roll(after, 8 - step, 1), 1.0)
        query[:, lanes] = (q * before).reshape(64, 128)
        kept[:, lanes] = before.reshape(64, 128)
        keys[:, lanes] = (key * after).reshape(64, 128)
        if h == 0:
            state_copy.wait()
        lax.fori_loop(0, 8, functools.partial(read_state, h), 0, unroll=2)
        o = output[:, lanes]
        zo = z[:, 768 + 128 * h : 896 + 128 * h]
        o = o * lax.rsqrt(jnp.mean(o * o, axis=1, keepdims=True) + EPS) * ref["lane_gain"][...]
        heads[kv, h] = jnp.where(live, o * (zo * jax.nn.sigmoid(zo)), 0.0).astype(BF)
        own = heads.at[kv, h]
        copies += [send(own, own, plane_peer(at, *d)) for d in planes]
    def write_state(n, carry):
        rows = pl.ds(pl.multiple_of(8 * n, 8), 8)
        for h in range(2):
            lanes = slice(128 * h, 128 * h + 128)
            k_high, k_low = split(keys[rows, lanes])
            v_high, v_low = split(z[rows, 512 + 128 * h : 640 + 128 * h])
            added = times(
                jnp.concatenate([k_high, k_high, k_low], axis=0),
                jnp.concatenate([v_high, v_low, v_high], axis=0),
                ((0,), (0,)),
            )
            state_out[n, h] = column_of(kept[rows, lanes][7:8, :], 128) * state_in[n, h] + added
        return carry

    lax.fori_loop(0, 8, write_state, 0)
    new_copy = fetch(10, state_out, state_result)
    result_copy.wait()
    for copy in gain_copies:
        copy.wait()
    gain = jnp.concatenate([gains[t, 0:1, 0:32] for t in range(8)], axis=1)
    for copy in copies:
        copy.wait()

    partial, arrived, result = ref["_partial"], ref["_arrived"], ref["_result_in"]
    all_heads = jnp.concatenate([heads[:, h].reshape(1024, 128) for h in range(2)], axis=1)
    for part in range(2):
        picked = ref["_chosen"][256 * part : 256 * part + 256]
        packed = times(picked, all_heads, ((1,), (0,))).astype(BF)
        partial[4 * part : 4 * part + 4] = (
            times(packed, result[...], ((1,), (0,))).astype(BF).reshape(4, 64, 256)
        )
    copies = []
    for i, (dx, dc) in enumerate(lines):
        peer = line_peer(at, dx, dc)
        copies.append(send(partial.at[2 * peer[2] + peer[3]], arrived.at[i], peer))
    attended = partial[tp].astype(F32)
    for i, copy in enumerate(copies):
        copy.wait()
        attended = attended + arrived[i].astype(F32)
    residual = (ref["_own_rows"][...] + attended).astype(BF).astype(F32)
    tile = (residual * gain).astype(BF)
    blocks = [
        tile[16 * i : 16 * i + 16, 128 * h : 128 * h + 128] for h in range(2) for i in range(4)
    ]
    gathered = group["gathered"]
    for p, ((first, count), order) in enumerate(zip(PARTS, ORDERS)):
        idx = tuple(at[a] for a in order[::-1])
        for b in range(count):
            gathered[p][(*idx, b)] = blocks[first + b]
    copies = gather_plane(at, gathered, ORDERS, send)
    ref["_residual"][...] = residual
    later = ref["_later_squares"]
    own_squares = jnp.sum(residual * residual, axis=1, keepdims=True)
    later[0] = jnp.broadcast_to(row_of(own_squares, 64), (8, 128))
    square_copies = [
        send(later.at[0], later.at[1 + i], plane_peer(at, *d)) for i, d in enumerate(planes)
    ]
    steps = gather_line(at, gathered, ORDERS, copies, send)
    next(steps)
    for copy in square_copies:
        copy.wait()
    squares_sum, squares_line = ref["_squares_sum"], ref["_squares_line"]
    own_sum = jnp.sum(later[...], axis=0)
    squares_sum[...] = own_sum
    squares_line[pl.ds(at["x"], 1)] = own_sum[None]
    line_copies = [
        send(squares_sum, squares_line.at[at["x"]], line_peer(at, dx, 0)) for dx in (1, 2, 3)
    ]
    next(steps)
    for copy in (*line_copies, *weight_sends):
        copy.wait()

    ga, gb, gc = gathered
    total = ref["_total"]

    def rows_at(zz, yy):
        v = jnp.concatenate([ga[zz, yy], gb[:, zz, yy], gc[yy, :, zz]], axis=1)
        return jnp.concatenate(
            [v[:, 0:4].reshape(256, 128), v[:, 4:8].reshape(256, 128)], axis=1
        )

    total[...] = jnp.zeros_like(total)

    def widening(zz, carry):
        lhs = jnp.concatenate([rows_at(zz, yy) for yy in range(4)], axis=1)
        cols = pl.ds(pl.multiple_of(zz * 1024, 1024), 1024)
        for core in range(2):
            total[core] += times(lhs, weights[core, :, :, cols].reshape(256, 1024))
        return carry

    lax.fori_loop(0, 4, widening, 0)
    scale = lax.rsqrt(
        jnp.concatenate([column_of(squares_line[g, 0:1, :], 64) for g in range(4)], axis=0)
        / 4096
        + EPS
    )
    hidden = []
    for core in range(2):
        gated = total[core, :, 0:128] * scale
        upward = total[core, :, 128:256] * scale
        hidden.append((gated * jax.nn.sigmoid(gated) * upward).astype(BF))
    hidden = jnp.concatenate(hidden, axis=1)
    ta, tb, tc = group["terms"]

    def narrowing(zz, carry):
        cols = pl.ds(pl.multiple_of(zz * 1024, 1024), 1024)
        rhs = jnp.concatenate([narrows[0, :, cols], narrows[1, :, cols]], axis=0)
        term = times(hidden, rhs, ((1,), (0,))).astype(BF)
        for yy in range(4):
            v = jnp.concatenate(
                [
                    term[:, 256 * yy + 128 * h : 256 * yy + 128 * h + 128].reshape(4, 4, 16, 128)
                    for h in range(2)
                ],
                axis=1,
            )
            ta[zz, yy] = v[:, 0:3]
            tb[:, zz, yy] = v[:, 3:6]
            tc[yy, :, zz] = v[:, 6:8]
        return carry

    lax.fori_loop(0, 4, narrowing, 0)
    sums = jnp.concatenate(
        reduce_torus(
            at, group["terms"], ORDERS, fours(group["mixer_line"]), group["mixer_plane"], send
        ),
        axis=0,
    )

    mixed = []
    for h in range(2):
        for i in range(4):
            res = ref["_residual"][16 * i : 16 * i + 16, 128 * h : 128 * h + 128]
            mixed.append((res + sums[4 * h + i]).astype(BF))
    ypack, yarrive = ref["_ypack"], ref["_yarrive"]
    for t in range(8):
        h, first = t // 4, 32 * (t % 4)
        ypack[t] = jnp.concatenate(
            [mixed[4 * h + i][:, first : first + 32] for i in range(4)], axis=1
        )
    copies = []
    for dx, dc in lines:
        peer = line_peer(at, dx, dc)
        copies.append(send(ypack.at[2 * peer[2] + peer[3]], yarrive.at[tp], peer))
    yarrive[pl.ds(tp, 1)] = ypack[pl.ds(tp, 1)]
    for copy in copies:
        copy.wait()
    mixed_out[...] = yarrive[...]
    new_copy.wait()
    assert send.used <= sends.shape[0]


def layer(*arguments):
    vmem = pl.BlockSpec(memory_space=pltpu.VMEM)
    far = pl.BlockSpec(memory_space=pltpu.HBM)
    copies = 400
    return pl.pallas_call(
        layer_kernel,
        out_shape=(
            jax.ShapeDtypeStruct((8, 16, 128), BF),
            jax.ShapeDtypeStruct((8, 1024), jnp.int32),
            jax.ShapeDtypeStruct((8, 2, 128, 128), F32),
        ),
        in_specs=[far] * len(INPUTS),
        out_specs=(vmem, vmem, far),
        scratch_shapes=[
            *scratch()[2],
            pltpu.SemaphoreType.DMA((copies,)),
            pltpu.SemaphoreType.DMA((copies,)),
            pltpu.SemaphoreType.DMA((17,)),
            pltpu.SemaphoreType.REGULAR,
        ],
        compiler_params=pltpu.CompilerParams(
            collective_id=0, has_side_effects=True, vmem_limit_bytes=67043328
        ),
        name="layer",
    )(*arguments)


def finish_kernel(packed_ref, place_ref, state_ref, mixed_ref, new_ref, held, packed, place, out, sems):
    takes = []
    for n, (src, dst) in enumerate(((packed_ref, packed), (place_ref, place))):
        takes.append(pltpu.make_async_copy(src, dst, sems.at[n]))
        takes[n].start()
    for n in range(4):
        half = pl.ds(2 * n, 2)
        takes.append(pltpu.make_async_copy(state_ref.at[half], held.at[half], sems.at[2 + n]))
        takes[2 + n].start()
    takes[0].wait()
    takes[1].wait()
    j = lax.broadcasted_iota(jnp.int32, (128, 1024), 0)
    rows = 64 * (j // 16) + j % 16 - place[0:1, :]
    gives = []
    mixed = jnp.zeros((32, 1024), F32)
    for a in range(4):
        takes[2 + a].wait()
        half = pl.ds(2 * a, 2)
        gives.append(pltpu.make_async_copy(held.at[half], new_ref.at[half], sems.at[6 + a]))
        gives[a].start()
        chosen = jnp.where(rows == -16 * a, 1.0, 0.0).astype(BF)
        piece = packed[...].reshape(128, 128)[:, 32 * a : 32 * a + 32]
        mixed = mixed + times(piece, chosen, ((0,), (0,)))
    out[...] = mixed.astype(BF)
    give = pltpu.make_async_copy(out, mixed_ref, sems.at[10])
    give.start()
    for copy in gives:
        copy.wait()
    give.wait()


def finish(packed, place, state):
    far = pl.BlockSpec(memory_space=pltpu.HBM)
    return pl.pallas_call(
        finish_kernel,
        out_shape=(
            jax.ShapeDtypeStruct((32, 1024), BF),
            jax.ShapeDtypeStruct((8, 2, 128, 128), F32),
        ),
        in_specs=[far] * 3,
        out_specs=(far, far),
        scratch_shapes=[
            pltpu.VMEM((8, 2, 128, 128), F32),
            pltpu.VMEM((8, 16, 128), BF),
            pltpu.VMEM((8, 1024), jnp.int32),
            pltpu.VMEM((32, 1024), BF),
            pltpu.SemaphoreType.DMA((11,)),
        ],
        compiler_params=pltpu.CompilerParams(vmem_limit_bytes=67043328),
        name="finish",
    )(packed, place, state)


def local(
    residual_entries,
    fresh_extents,
    memory_matrix,
    initial_rescale_vector,
    probe_matrix,
    retain_matrix,
    content_matrix,
    result_switch_matrix,
    retain_lower_limit,
    extra_shrink_log,
    lane_result_rescale,
    result_matrix,
    later_rescale_vector,
    mixer_switch_matrix,
    widening_matrix,
    narrowing_matrix,
):
    packed, place, new_state = layer(
        residual_entries.T,
        fresh_extents.reshape(1, 128),
        initial_rescale_vector.reshape(1, 256),
        probe_matrix,
        retain_matrix,
        content_matrix,
        result_switch_matrix,
        retain_lower_limit.reshape(1, 256),
        extra_shrink_log.T,
        lane_result_rescale.reshape(1, 128),
        memory_matrix,
        result_matrix,
        later_rescale_vector.reshape(1, 32),
        mixer_switch_matrix.T,
        widening_matrix.T,
        narrowing_matrix,
    )
    mixed, carried = finish(packed, place, new_state)
    return (mixed.T, carried)


def solution(mesh):
    torus = Mesh(mesh.devices.reshape(4, 4, 4, 2), ("kv_0", "kv_1", "tp_0", "tp_1"))
    placed = (
        P(None, KV_TP),
        P(),
        P(KV, TP, None, None),
        P(KV),
        P(KV, TP),
        P(KV, TP),
        P(KV, TP),
        P(KV, TP),
        P(TP),
        P(KV, TP),
        P(),
        P(TP, KV),
        P(KV_TP),
        P(None, KV_TP),
        P(None, KV_TP),
        P(KV_TP, None),
    )
    return jax.shard_map(
        local,
        mesh=torus,
        in_specs=placed,
        out_specs=(P(None, KV_TP), P(KV, TP, None, None)),
        check_vma=False,
    )
```

```python
import functools

import jax
import jax.numpy as jnp
from jax import lax
from jax.experimental import pallas as pl
from jax.experimental.pallas import tpu as pltpu
from jax.sharding import Mesh
from jax.sharding import PartitionSpec as P

KV = ("kv_0", "kv_1")
TP = ("tp_0", "tp_1")
KV_TP = ("kv_0", "kv_1", "tp_0", "tp_1")
MESH = pl.DeviceIdType.MESH
EPS = 1e-06
F32 = jnp.float32
BF = jnp.bfloat16
PARTS = ((0, 3), (3, 3), (6, 2))
ORDERS = ("xyz", "yzx", "zxy")
ROWS = (0, 1, 3, 2)


def my_position():
    return dict(
        z=lax.axis_index("kv_0"),
        y=lax.axis_index("kv_1"),
        x=lax.axis_index("tp_0"),
        c=lax.axis_index("tp_1"),
    )


def device_at(at, **moved):
    there = dict(at, **moved)
    return (there["z"], there["y"], there["x"], there["c"])


def plane_offsets():
    return [(dz, dy) for dz in range(4) for dy in range(4) if dz or dy]


def line_offsets():
    return [(dx, dc) for dx in range(4) for dc in range(2) if dx or dc]


def plane_peer(at, dz, dy):
    return device_at(at, z=(at["z"] + dz) % 4, y=(at["y"] + dy) % 4)


def line_peer(at, dx, dc):
    return device_at(at, x=(at["x"] + dx) % 4, c=(at["c"] + dc) % 2)


def meet(peers, meanwhile):
    barrier = pltpu.get_barrier_semaphore()
    for peer in peers:
        pl.semaphore_signal(barrier, inc=1, device_id=peer, device_id_type=MESH)
    meanwhile()
    pl.semaphore_wait(barrier, len(peers))


class Sender:
    def __init__(self, sends, recvs):
        self.sends, self.recvs, self.used = sends, recvs, 0

    def __call__(self, src, dst, peer):
        i = self.used
        self.used = i + 1
        return start_copy(src, dst, self.sends.at[i], self.recvs.at[i], peer)


def start_copy(src, dst, send_sem, recv_sem, peer):
    copy = pltpu.make_async_remote_copy(
        src_ref=src,
        dst_ref=dst,
        send_sem=send_sem,
        recv_sem=recv_sem,
        device_id=peer,
        device_id_type=MESH,
    )
    copy.start()
    return copy


def times(a, b, dims=((1,), (1,))):
    return lax.dot_general(a, b, (dims, ((), ())), preferred_element_type=F32)


def row_of(column, rows):
    eye = lax.broadcasted_iota(jnp.int32, (rows, 128), 0) == lax.broadcasted_iota(
        jnp.int32, (rows, 128), 1
    )
    return jnp.sum(jnp.where(eye, column, 0.0), axis=0, keepdims=True)


def column_of(row, rows):
    eye = lax.broadcasted_iota(jnp.int32, (rows, 128), 0) == lax.broadcasted_iota(
        jnp.int32, (rows, 128), 1
    )
    return jnp.sum(jnp.where(eye, row, 0.0), axis=1, keepdims=True)


def picks(place, start, rows):
    want = lax.broadcasted_iota(jnp.int32, (rows, 1024), 0) + start
    return jnp.where(want == place, 1.0, 0.0).astype(BF)


def halves(length):
    return pl.ds(0, length // 2), pl.ds(length // 2, length - length // 2)


def gather_plane(at, bufs, orders, send):
    copies = [{} for _ in orders]
    for db in ROWS:
        for p, order in enumerate(orders):
            a, b, c = order
            own = bufs[p].at[at[c], at[b], at[a]]
            for da in range(4):
                if db or da:
                    there = {a: (at[a] + da) % 4, b: (at[b] + db) % 4}
                    copies[p][db, da] = send(own, own, device_at(at, **there))
    return copies


def gather_line(at, bufs, orders, plane, send):
    first = {}
    for db in ROWS:
        for p, (a, b, c) in enumerate(orders):
            for da in range(4):
                if db or da:
                    plane[p][db, da].wait_recv()
            own = bufs[p].at[at[c], (at[b] + 4 - db) % 4]
            first[p, db] = tuple(
                send(own, own, device_at(at, **{c: (at[c] + turn) % 4}))
                for turn in ((1, 3, 2) if db == 2 else (1, 3))
            )
    yield
    second = []
    for db, parts in ((0, ((1, 0, 4),)), (1, ((3, 0, 4),)), (3, ((1, 0, 2), (3, 2, 2)))):
        for p, (a, b, c) in enumerate(orders):
            for copy in first[p, db]:
                copy.wait_recv()
            for turn, start, size in parts:
                came = bufs[p].at[
                    (at[c] + 4 - turn) % 4, (at[b] + 4 - db) % 4, pl.ds(start, size)
                ]
                second.append(send(came, came, device_at(at, **{c: (at[c] + turn) % 4})))
    yield
    for p in range(len(orders)):
        for copy in first[p, 2]:
            copy.wait_recv()
    for part in (*[part.values() for part in plane], *first.values()):
        for copy in part:
            copy.wait_send()
    for copy in second:
        copy.wait()
    yield


def add_into(ref, idx, term):
    ref[idx] = (ref[idx].astype(F32) + term.astype(F32)).astype(BF)


def reduce_line(at, bufs, axes, pres, received, send, keep=True, after=None):
    early = []
    for p, (axis, pre) in enumerate(zip(axes, pres)):
        one_up, one_down, two_up, two_down = received[p]
        m = at[axis]
        up, down, away = (m + 1) % 4, (m + 3) % 4, (m + 2) % 4
        to_up, to_down = device_at(at, **{axis: up}), device_at(at, **{axis: down})
        lo, hi = halves(bufs[p].shape[len(pre) + 1])
        early.append((
            send(bufs[p].at[(*pre, away, lo)], one_up, to_up),
            send(bufs[p].at[(*pre, away, hi)], one_down, to_down),
            send(bufs[p].at[(*pre, up, hi)], two_up.at[hi], to_up),
            send(bufs[p].at[(*pre, down, lo)], two_down.at[lo], to_down),
        ))
    yield
    late = []
    for p, (axis, pre) in enumerate(zip(axes, pres)):
        one_up, one_down, two_up, two_down = received[p]
        m = at[axis]
        up, down = (m + 1) % 4, (m + 3) % 4
        to_up, to_down = device_at(at, **{axis: up}), device_at(at, **{axis: down})
        lo, hi = halves(bufs[p].shape[len(pre) + 1])
        early[p][0].wait_recv()
        add_into(bufs[p], (*pre, up, lo), one_up[...])
        a = send(bufs[p].at[(*pre, up, lo)], two_up.at[lo], to_up)
        early[p][1].wait_recv()
        add_into(bufs[p], (*pre, down, hi), one_down[...])
        late.append((a, send(bufs[p].at[(*pre, down, hi)], two_down.at[hi], to_down)))
    yield
    sums = []
    for p, (axis, pre) in enumerate(zip(axes, pres)):
        for copy in early[p][2:]:
            copy.wait_recv()
        for copy in late[p]:
            copy.wait_recv()
        own = (*pre, at[axis])
        total = bufs[p][own].astype(F32)
        for ref in received[p][2:]:
            total = total + ref[...].astype(F32)
        if keep:
            bufs[p][own] = total.astype(BF)
        sums.append(total)
        if after:
            after(p)
    for p in range(len(axes)):
        for copy in (*early[p], *late[p]):
            copy.wait_send()
    yield sums


def reduce_torus(at, bufs, orders, line_received, plane_received, send):
    early, late, plane = {}, {}, {}
    lo, hi = pl.ds(0, 2), pl.ds(2, 2)

    def row(p, db):
        a, b, c = orders[p]
        m = at[c]
        return c, m, (m + 1) % 4, (m + 3) % 4, (at[b] + db) % 4

    def begin(db):
        for p in range(len(orders)):
            c, m, up, down, r = row(p, db)
            one_up, one_down, two_up, two_down = line_received[p]
            to_up, to_down = device_at(at, **{c: up}), device_at(at, **{c: down})
            away = (m + 2) % 4
            early[p, db] = (
                send(bufs[p].at[away, r, lo], one_up.at[db], to_up),
                send(bufs[p].at[away, r, hi], one_down.at[db], to_down),
                send(bufs[p].at[up, r, hi], two_up.at[db, hi], to_up),
                send(bufs[p].at[down, r, lo], two_down.at[db, lo], to_down),
            )

    def go_on(db):
        for p in range(len(orders)):
            c, m, up, down, r = row(p, db)
            one_up, one_down, two_up, two_down = line_received[p]
            to_up, to_down = device_at(at, **{c: up}), device_at(at, **{c: down})
            early[p, db][0].wait_recv()
            add_into(bufs[p], (up, r, lo), one_up[db])
            first = send(bufs[p].at[up, r, lo], two_up.at[db, lo], to_up)
            early[p, db][1].wait_recv()
            add_into(bufs[p], (down, r, hi), one_down[db])
            late[p, db] = (first, send(bufs[p].at[down, r, hi], two_down.at[db, hi], to_down))

    def end(db):
        for p, (a, b, c) in enumerate(orders):
            _, m, up, down, r = row(p, db)
            two_up, two_down = line_received[p][2:]
            for copy in (*early[p, db][2:], *late[p, db]):
                copy.wait_recv()
            total = bufs[p][m, r].astype(F32) + two_up[db].astype(F32) + two_down[db].astype(F32)
            bufs[p][m, r] = total.astype(BF)
            for da in range(4):
                if db or da:
                    n = 4 * db + da - 1
                    there = {a: (at[a] + da) % 4, b: r}
                    block = bufs[p].at[m, r, there[a]]
                    plane[p, n] = send(block, plane_received[p].at[n], device_at(at, **there))

    rows = ROWS[::-1]
    for db in rows:
        begin(db)
    for db in rows:
        go_on(db)
    for db in rows:
        end(db)
    sums = []
    for p, (a, b, c) in enumerate(orders):
        total = bufs[p][at[c], at[b], at[a]].astype(F32)
        for n in range(14, -1, -1):
            plane[p, n].wait_recv()
            total = total + plane_received[p][n].astype(F32)
        sums.append(total)
    for copies in (*early.values(), *late.values(), plane.values()):
        for copy in copies:
            copy.wait_send()
    return sums


def split(v):
    high = v.astype(BF)
    return high, (v - high.astype(F32)).astype(BF)


INPUTS = (
    "x", "lengths", "gain", "wq", "wf", "wi", "wo", "bound", "shrink", "lane_gain", "state",
    "result", "later_gain", "gate", "wide", "narrow",
)
SMALL = (
    ("lengths", (1, 128), jnp.int32),
    ("gain", (1, 256), F32),
    ("bound", (1, 256), F32),
    ("shrink", (2, 64), F32),
    ("lane_gain", (1, 128), F32),
    ("later_gain", (1, 32), F32),
)


def line_shapes(shape, count):
    shapes = []
    for _ in range(count):
        half = shape[0] // 2
        shapes += [(half, *shape[1:]), (shape[0] - half, *shape[1:]), shape, shape]
    return shapes


def scratch():
    counts = [count for _, count in PARTS]
    boxes = [(4, 4, 4, count, 16, 128) for count in counts]
    named = [
        *[("small_" + name, shape, kind) for name, shape, kind in SMALL],
        ("cols", (8, 32, 1024), BF),
        ("scaled", (1024, 256), BF),
        ("squares", (8, 8, 128), F32),
        ("squares_in", (15, 8, 128), F32),
        ("front_weights", (4, 256, 256), BF),
        ("pa", (2, 4, 4, 64, 256), BF),
        ("pb", (2, 4, 4, 64, 256), BF),
        ("z", (64, 1024), F32),
        ("query", (64, 256), F32),
        ("kept", (64, 256), F32),
        ("key", (64, 256), F32),
        ("output", (64, 256), F32),
        ("state_in", (8, 2, 128, 128), F32),
        ("state_out", (8, 2, 128, 128), F32),
        ("chosen", (512, 1024), BF),
        ("heads", (16, 2, 64, 128), BF),
        ("partial", (8, 64, 256), BF),
        ("arrived", (7, 64, 256), BF),
        ("own_gain", (8, 128), F32),
        ("gains", (8, 8, 128), F32),
        ("own_rows", (64, 256), F32),
        ("residual", (64, 256), F32),
        ("later_squares", (16, 8, 128), F32),
        ("squares_sum", (8, 128), F32),
        ("squares_line", (4, 8, 128), F32),
        ("weights", (2, 2, 128, 4096), BF),
        ("narrows", (2, 128, 4096), BF),
        ("staged", (3, 86, 4096), BF),
        ("result_in", (256, 256), BF),
        ("total", (2, 256, 256), F32),
        ("ypack", (8, 16, 128), BF),
        ("yarrive", (8, 16, 128), BF),
    ]
    groups = [
        ("gathered", boxes),
        ("terms", boxes),
        ("front_one", line_shapes((4, 64, 256), 4)),
        ("front_two", [(3, 64, 256)] * 4),
        (
            "mixer_line",
            [(4, n, count, 16, 128) for count in counts for n in (2, 2, 4, 4)],
        ),
        ("mixer_plane", [(15, count, 16, 128) for count in counts]),
    ]
    flat = [pltpu.VMEM(shape, kind) for _, shape, kind in named]
    for _, shapes in groups:
        flat += [pltpu.VMEM(shape, BF) for shape in shapes]
    return named, groups, flat


def layer_kernel(*refs):
    named, groups, flat = scratch()
    ref = dict(zip(INPUTS, refs))
    mixed_out, place_out, state_result = refs[len(INPUTS) : len(INPUTS) + 3]
    rest = refs[len(INPUTS) + 3 :]
    ref.update(zip(["_" + name for name, _, _ in named], rest))
    rest = rest[len(named) :]
    group = {}
    for name, shapes in groups:
        group[name], rest = rest[: len(shapes)], rest[len(shapes) :]
    sends, recvs, local, ready = rest
    send = Sender(sends, recvs)
    at = my_position()
    kv = 4 * at["z"] + at["y"]
    tp = 2 * at["x"] + at["c"]
    planes, lines = plane_offsets(), line_offsets()
    fours = lambda refs: [refs[i : i + 4] for i in range(0, len(refs), 4)]

    def fetch(n, src, dst):
        copy = pltpu.make_async_copy(src, dst, local.at[n])
        copy.start()
        return copy

    cols = ref["_cols"]
    small_copies = [
        fetch(11 + n, ref[name], ref["_small_" + name]) for n, (name, _, _) in enumerate(SMALL)
    ]
    for name, _, _ in SMALL:
        ref[name] = ref["_small_" + name]
    x_copy = fetch(0, ref["x"], cols.at[tp])
    front_copies = [
        fetch(1 + n, ref[name], ref["_front_weights"].at[n])
        for n, name in enumerate(("wq", "wf", "wi", "wo"))
    ]
    weight_copies = [
        fetch(5 + n, ref[name], ref["_staged"].at[n])
        for n, name in enumerate(("gate", "wide", "narrow"))
    ]
    state_copy = fetch(8, ref["state"], ref["_state_in"])
    result_copy = fetch(9, ref["result"], ref["_result_in"])
    weights, narrows, staged = ref["_weights"], ref["_narrows"], ref["_staged"]

    def pad_weights():
        for n, first in ((0, 80), (1, 96)):
            weights[n, :, first:128] = jnp.zeros((2, 128 - first, 4096), BF)
            narrows[n, first:128] = jnp.zeros((128 - first, 4096), BF)
        for copy in weight_copies:
            copy.wait()
        weights[0, :, 0:86] = staged[0:2]
        narrows[0, 0:86] = staged[2]

    turns = (1, 2, 3)
    meet(
        [line_peer(at, *d) for d in lines]
        + [plane_peer(at, dz, 0) for dz in turns]
        + [plane_peer(at, 0, dy) for dy in turns],
        lambda: None,
    )
    for dy in turns:
        pl.semaphore_signal(ready, inc=1, device_id=plane_peer(at, 0, dy), device_id_type=MESH)

    x_copy.wait()
    partner = line_peer(at, 0, 1)
    far_copies = [send(cols.at[tp], cols.at[tp], line_peer(at, dx, 0)) for dx in turns]
    near_copies = [send(cols.at[tp], cols.at[tp], partner)]
    for copy in small_copies:
        copy.wait()
    own_gain, gains = ref["_own_gain"], ref["_gains"]
    own_gain[...] = jnp.broadcast_to(
        jnp.concatenate([ref["later_gain"][...], jnp.zeros((1, 96), F32)], axis=1), (8, 128)
    )
    gain_copies = [send(own_gain, gains.at[tp], line_peer(at, *d)) for d in lines]
    gains[pl.ds(tp, 1)] = own_gain[...][None]

    lengths = jnp.broadcast_to(ref["lengths"][...], (8, 128)).astype(F32).astype(BF)
    s = lax.broadcasted_iota(jnp.int32, (128, 1024), 0)
    owner = lax.broadcasted_iota(jnp.int32, (128, 1024), 1) // 8
    start = times(lengths, jnp.where(s < owner, 1.0, 0.0).astype(BF), ((1,), (0,)))
    length = times(lengths, jnp.where(s == owner, 1.0, 0.0).astype(BF), ((1,), (0,)))
    slot = lax.broadcasted_iota(jnp.int32, (8, 1024), 1) % 8
    place = jnp.where(slot < length.astype(jnp.int32), start.astype(jnp.int32) + slot, -1)
    place_out[...] = place
    place = place[0:1]
    for part in range(4):
        ref["_chosen"][128 * part : 128 * part + 128] = picks(place, 128 * part, 128)
    gain = jnp.concatenate(
        [column_of(ref["gain"][:, 0:128], 128), column_of(ref["gain"][:, 128:256], 128)], axis=0
    )
    pad_weights()
    for dx, copy in zip(turns, far_copies):
        copy.wait()
        came = 2 * ((at["x"] + 4 - dx) % 4) + at["c"]
        near_copies.append(send(cols.at[came], cols.at[came], partner))
    for copy in near_copies:
        copy.wait()
    scaled, squares = ref["_scaled"], ref["_squares"]
    for k in range(8):
        lanes = slice(128 * k, 128 * k + 128)
        v = cols[:, :, lanes].reshape(256, 128).astype(F32)
        scaled[lanes, :] = (v * gain).astype(BF).T
        squares[k] = jnp.broadcast_to(jnp.sum(v * v, axis=0, keepdims=True), (8, 128))
    for copy in front_copies:
        copy.wait()
    pa, pb = ref["_pa"], ref["_pb"]

    chunks = ((0, pa.at[0], "yz"), (1, pb.at[0], "zy"), (2, pa.at[1], "yz"), (3, pb.at[1], "zy"))
    one, two = fours(group["front_one"]), group["front_two"]

    def project(n, terms, order):
        def body(a, carry):
            lhs = scaled[pl.ds(pl.multiple_of(256 * a, 256), 256), :]
            v = times(lhs, ref["_front_weights"][n], ((1,), (0,))).astype(BF).reshape(4, 64, 256)
            if order == "yz":
                terms[:, a] = v
            else:
                terms[a] = v
            return carry

        lax.fori_loop(0, 4, body, 0)

    lines_one = []
    for n, terms, order in chunks:
        project(n, terms, order)
        lines_one.append(reduce_line(at, (terms,), order[0], ((),), one[n : n + 1], send))
        next(lines_one[n])
    for step in lines_one:
        next(step)
    pl.semaphore_wait(ready, 3)
    square_copies = []
    for i, (dz, dy) in enumerate(planes):
        peer = plane_peer(at, dz, dy)
        block = squares.at[(4 * peer[0] + peer[1]) // 2]
        square_copies.append(send(block, ref["_squares_in"].at[i], peer))
    ref["_own_rows"][...] = times(picks(place, 64 * tp, 64), cols[...].reshape(256, 1024))
    second = []
    for n, terms, order in chunks:
        next(lines_one[n])
        here, axis = at[order[0]], order[1]
        second.append([])
        for turn in turns:
            there = (at[axis] + turn) % 4
            peer = device_at(at, **{axis: there})
            second[n].append(send(terms.at[here, there], two[n].at[turn - 1], peer))
    row = lax.broadcasted_iota(jnp.int32, (64, 128), 0)
    lane = lax.broadcasted_iota(jnp.int32, (64, 128), 1)
    length = jnp.sum(
        jnp.where(lane == 8 * kv + row // 8, ref["lengths"][...].astype(F32), 0.0),
        axis=1,
        keepdims=True,
    )
    live = (row[:, 0:1] % 8).astype(F32) < length
    for copy in square_copies:
        copy.wait()
    total = jnp.sum(ref["_squares_in"][...], axis=0) + squares[kv // 2]
    own = jnp.sum(
        jnp.where(lane == 64 * (kv % 2) + row, total[0:1, :], 0.0), axis=1, keepdims=True
    )
    scale = lax.rsqrt(own / 4096 + EPS)
    z = ref["_z"]
    for n, terms, order in chunks:
        total = terms[at[order[0]], at[order[1]]].astype(F32)
        for i, copy in enumerate(second[n]):
            copy.wait()
            total = total + two[n][i].astype(F32)
        z[:, 256 * n : 256 * n + 256] = total * scale

    weight_sends = [
        send(weights.at[0, :, 0:96], weights.at[1, :, 0:96], partner),
        send(narrows.at[0, 0:96], narrows.at[1, 0:96], partner),
    ]

    query, kept, keys, output = ref["_query"], ref["_kept"], ref["_key"], ref["_output"]
    slot = lax.broadcasted_iota(jnp.int32, (8, 8, 128), 1)
    state_in, state_out, heads = ref["_state_in"], ref["_state_out"], ref["_heads"]

    def read_state(h, n, carry):
        rows = pl.ds(pl.multiple_of(8 * n, 8), 8)
        lanes = slice(128 * h, 128 * h + 128)
        s_high, s_low = split(state_in[n, h])
        q_high, q_low = split(query[rows, lanes])
        lhs = jnp.concatenate(
            [
                jnp.concatenate([q_high, q_high], axis=1),
                jnp.concatenate([q_low, jnp.zeros_like(q_low)], axis=1),
            ],
            axis=0,
        )
        o = times(lhs, jnp.concatenate([s_high, s_low], axis=0), ((1,), (0,)))
        output[rows, lanes] += o[0:8] + o[8:16]
        return carry

    copies = []
    for h in range(2):
        lanes = slice(128 * h, 128 * h + 128)
        bound = ref["bound"][:, lanes]
        retain = bound + (1.0 - bound) * jax.nn.sigmoid(z[:, 256 + 128 * h : 384 + 128 * h])
        shrink = jnp.sum(
            jnp.where(lane[:, 0:64] == row[:, 0:64], ref["shrink"][h : h + 1, :], 0.0),
            axis=1,
            keepdims=True,
        )
        decay = jnp.where(live, jnp.exp(jnp.log(retain) + shrink), 1.0).reshape(8, 8, 128)
        key = jnp.where(live, 1.0 - retain, 0.0).reshape(8, 8, 128)
        zq = z[:, lanes]
        q = (zq * jax.nn.sigmoid(zq)).reshape(8, 8, 128)
        value = z[:, 512 + 128 * h : 640 + 128 * h].reshape(8, 8, 128)
        between = q
        out = jnp.sum(q * key, axis=2, keepdims=True) * value
        for back in range(1, 8):
            between = between * (decay if back == 1 else pltpu.roll(decay, back - 1, 1))
            weight = jnp.sum(between * pltpu.roll(key, back, 1), axis=2, keepdims=True)
            out = out + jnp.where(slot >= back, weight * pltpu.roll(value, back, 1), 0.0)
        output[:, lanes] = out.reshape(64, 128)
        before, after = decay, jnp.where(slot < 7, pltpu.roll(decay, 7, 1), 1.0)
        for step in (1, 2, 4):
            before = before * jnp.where(slot >= step, pltpu.roll(before, step, 1), 1.0)
            after = after * jnp.where(slot + step < 8, pltpu.roll(after, 8 - step, 1), 1.0)
        query[:, lanes] = (q * before).reshape(64, 128)
        kept[:, lanes] = before.reshape(64, 128)
        keys[:, lanes] = (key * after).reshape(64, 128)
        if h == 0:
            state_copy.wait()
        lax.fori_loop(0, 8, functools.partial(read_state, h), 0, unroll=2)
        o = output[:, lanes]
        zo = z[:, 768 + 128 * h : 896 + 128 * h]
        o = o * lax.rsqrt(jnp.mean(o * o, axis=1, keepdims=True) + EPS) * ref["lane_gain"][...]
        heads[kv, h] = jnp.where(live, o * (zo * jax.nn.sigmoid(zo)), 0.0).astype(BF)
        own = heads.at[kv, h]
        copies += [send(own, own, plane_peer(at, *d)) for d in planes]
    def write_state(n, carry):
        rows = pl.ds(pl.multiple_of(8 * n, 8), 8)
        for h in range(2):
            lanes = slice(128 * h, 128 * h + 128)
            k_high, k_low = split(keys[rows, lanes])
            v_high, v_low = split(z[rows, 512 + 128 * h : 640 + 128 * h])
            added = times(
                jnp.concatenate([k_high, k_high, k_low], axis=0),
                jnp.concatenate([v_high, v_low, v_high], axis=0),
                ((0,), (0,)),
            )
            state_out[n, h] = column_of(kept[rows, lanes][7:8, :], 128) * state_in[n, h] + added
        return carry

    lax.fori_loop(0, 8, write_state, 0)
    new_copy = fetch(10, state_out, state_result)
    result_copy.wait()
    for copy in gain_copies:
        copy.wait()
    gain = jnp.concatenate([gains[t, 0:1, 0:32] for t in range(8)], axis=1)
    for copy in copies:
        copy.wait()

    partial, arrived, result = ref["_partial"], ref["_arrived"], ref["_result_in"]
    all_heads = jnp.concatenate([heads[:, h].reshape(1024, 128) for h in range(2)], axis=1)
    for part in range(2):
        picked = ref["_chosen"][256 * part : 256 * part + 256]
        packed = times(picked, all_heads, ((1,), (0,))).astype(BF)
        partial[4 * part : 4 * part + 4] = (
            times(packed, result[...], ((1,), (0,))).astype(BF).reshape(4, 64, 256)
        )
    copies = []
    for i, (dx, dc) in enumerate(lines):
        peer = line_peer(at, dx, dc)
        copies.append(send(partial.at[2 * peer[2] + peer[3]], arrived.at[i], peer))
    attended = partial[tp].astype(F32)
    for i, copy in enumerate(copies):
        copy.wait()
        attended = attended + arrived[i].astype(F32)
    residual = (ref["_own_rows"][...] + attended).astype(BF).astype(F32)
    later = ref["_later_squares"]
    own_squares = jnp.sum(residual * residual, axis=1, keepdims=True)
    later[0] = jnp.broadcast_to(row_of(own_squares, 64), (8, 128))
    square_copies = [
        send(later.at[0], later.at[1 + i], plane_peer(at, *d)) for i, d in enumerate(planes)
    ]
    tile = (residual * gain).astype(BF)
    blocks = [
        tile[16 * i : 16 * i + 16, 128 * h : 128 * h + 128] for h in range(2) for i in range(4)
    ]
    gathered = group["gathered"]
    for p, ((first, count), order) in enumerate(zip(PARTS, ORDERS)):
        idx = tuple(at[a] for a in order[::-1])
        for b in range(count):
            gathered[p][(*idx, b)] = blocks[first + b]
    copies = gather_plane(at, gathered, ORDERS, send)
    ref["_residual"][...] = residual
    steps = gather_line(at, gathered, ORDERS, copies, send)
    next(steps)
    for copy in square_copies:
        copy.wait()
    squares_sum, squares_line = ref["_squares_sum"], ref["_squares_line"]
    own_sum = jnp.sum(later[...], axis=0)
    squares_sum[...] = own_sum
    squares_line[pl.ds(at["x"], 1)] = own_sum[None]
    line_copies = [
        send(squares_sum, squares_line.at[at["x"]], line_peer(at, dx, 0)) for dx in (1, 2, 3)
    ]
    next(steps)
    total = ref["_total"]
    total[...] = jnp.zeros_like(total)
    for copy in (*line_copies, *weight_sends):
        copy.wait()
    scale = lax.rsqrt(
        jnp.concatenate([column_of(squares_line[g, 0:1, :], 64) for g in range(4)], axis=0)
        / 4096
        + EPS
    )
    next(steps)

    ga, gb, gc = gathered

    def rows_at(zz, yy):
        v = jnp.concatenate([ga[zz, yy], gb[:, zz, yy], gc[yy, :, zz]], axis=1)
        return jnp.concatenate(
            [v[:, 0:4].reshape(256, 128), v[:, 4:8].reshape(256, 128)], axis=1
        )

    def widening(zz, carry):
        lhs = jnp.concatenate([rows_at(zz, yy) for yy in range(4)], axis=1)
        cols = pl.ds(pl.multiple_of(zz * 1024, 1024), 1024)
        for core in range(2):
            total[core] += times(lhs, weights[core, :, :, cols].reshape(256, 1024))
        return carry

    lax.fori_loop(0, 4, widening, 0)
    hidden = []
    for core in range(2):
        gated = total[core, :, 0:128] * scale
        upward = total[core, :, 128:256] * scale
        hidden.append((gated * jax.nn.sigmoid(gated) * upward).astype(BF))
    hidden = jnp.concatenate(hidden, axis=1)
    ta, tb, tc = group["terms"]

    def narrowing(zz, carry):
        cols = pl.ds(pl.multiple_of(zz * 1024, 1024), 1024)
        rhs = jnp.concatenate([narrows[0, :, cols], narrows[1, :, cols]], axis=0)
        term = times(hidden, rhs, ((1,), (0,))).astype(BF)
        for yy in range(4):
            v = jnp.concatenate(
                [
                    term[:, 256 * yy + 128 * h : 256 * yy + 128 * h + 128].reshape(4, 4, 16, 128)
                    for h in range(2)
                ],
                axis=1,
            )
            ta[zz, yy] = v[:, 0:3]
            tb[:, zz, yy] = v[:, 3:6]
            tc[yy, :, zz] = v[:, 6:8]
        return carry

    lax.fori_loop(0, 4, narrowing, 0)
    sums = jnp.concatenate(
        reduce_torus(
            at, group["terms"], ORDERS, fours(group["mixer_line"]), group["mixer_plane"], send
        ),
        axis=0,
    )

    mixed = []
    for h in range(2):
        for i in range(4):
            res = ref["_residual"][16 * i : 16 * i + 16, 128 * h : 128 * h + 128]
            mixed.append((res + sums[4 * h + i]).astype(BF))
    ypack, yarrive = ref["_ypack"], ref["_yarrive"]
    for t in range(8):
        h, first = t // 4, 32 * (t % 4)
        ypack[t] = jnp.concatenate(
            [mixed[4 * h + i][:, first : first + 32] for i in range(4)], axis=1
        )
    copies = []
    for dx, dc in lines:
        peer = line_peer(at, dx, dc)
        copies.append(send(ypack.at[2 * peer[2] + peer[3]], yarrive.at[tp], peer))
    yarrive[pl.ds(tp, 1)] = ypack[pl.ds(tp, 1)]
    for copy in copies:
        copy.wait()
    mixed_out[...] = yarrive[...]
    new_copy.wait()
    assert send.used <= sends.shape[0]


def layer(*arguments):
    vmem = pl.BlockSpec(memory_space=pltpu.VMEM)
    far = pl.BlockSpec(memory_space=pltpu.HBM)
    copies = 400
    return pl.pallas_call(
        layer_kernel,
        out_shape=(
            jax.ShapeDtypeStruct((8, 16, 128), BF),
            jax.ShapeDtypeStruct((8, 1024), jnp.int32),
            jax.ShapeDtypeStruct((8, 2, 128, 128), F32),
        ),
        in_specs=[far] * len(INPUTS),
        out_specs=(vmem, vmem, far),
        scratch_shapes=[
            *scratch()[2],
            pltpu.SemaphoreType.DMA((copies,)),
            pltpu.SemaphoreType.DMA((copies,)),
            pltpu.SemaphoreType.DMA((17,)),
            pltpu.SemaphoreType.REGULAR,
        ],
        compiler_params=pltpu.CompilerParams(
            collective_id=0, has_side_effects=True, vmem_limit_bytes=67043328
        ),
        name="layer",
    )(*arguments)


def finish_kernel(packed_ref, place_ref, state_ref, mixed_ref, new_ref, held, packed, place, out, sems):
    takes = []
    for n, (src, dst) in enumerate(((packed_ref, packed), (place_ref, place))):
        takes.append(pltpu.make_async_copy(src, dst, sems.at[n]))
        takes[n].start()
    for n in range(4):
        half = pl.ds(2 * n, 2)
        takes.append(pltpu.make_async_copy(state_ref.at[half], held.at[half], sems.at[2 + n]))
        takes[2 + n].start()
    takes[0].wait()
    takes[1].wait()
    j = lax.broadcasted_iota(jnp.int32, (128, 1024), 0)
    rows = 64 * (j // 16) + j % 16 - place[0:1, :]
    gives = []
    mixed = jnp.zeros((32, 1024), F32)
    for a in range(4):
        takes[2 + a].wait()
        half = pl.ds(2 * a, 2)
        gives.append(pltpu.make_async_copy(held.at[half], new_ref.at[half], sems.at[6 + a]))
        gives[a].start()
        chosen = jnp.where(rows == -16 * a, 1.0, 0.0).astype(BF)
        piece = packed[...].reshape(128, 128)[:, 32 * a : 32 * a + 32]
        mixed = mixed + times(piece, chosen, ((0,), (0,)))
    out[...] = mixed.astype(BF)
    give = pltpu.make_async_copy(out, mixed_ref, sems.at[10])
    give.start()
    for copy in gives:
        copy.wait()
    give.wait()


def finish(packed, place, state):
    far = pl.BlockSpec(memory_space=pltpu.HBM)
    return pl.pallas_call(
        finish_kernel,
        out_shape=(
            jax.ShapeDtypeStruct((32, 1024), BF),
            jax.ShapeDtypeStruct((8, 2, 128, 128), F32),
        ),
        in_specs=[far] * 3,
        out_specs=(far, far),
        scratch_shapes=[
            pltpu.VMEM((8, 2, 128, 128), F32),
            pltpu.VMEM((8, 16, 128), BF),
            pltpu.VMEM((8, 1024), jnp.int32),
            pltpu.VMEM((32, 1024), BF),
            pltpu.SemaphoreType.DMA((11,)),
        ],
        compiler_params=pltpu.CompilerParams(vmem_limit_bytes=67043328),
        name="finish",
    )(packed, place, state)


def local(
    residual_entries,
    fresh_extents,
    memory_matrix,
    initial_rescale_vector,
    probe_matrix,
    retain_matrix,
    content_matrix,
    result_switch_matrix,
    retain_lower_limit,
    extra_shrink_log,
    lane_result_rescale,
    result_matrix,
    later_rescale_vector,
    mixer_switch_matrix,
    widening_matrix,
    narrowing_matrix,
):
    packed, place, new_state = layer(
        residual_entries.T,
        fresh_extents.reshape(1, 128),
        initial_rescale_vector.reshape(1, 256),
        probe_matrix,
        retain_matrix,
        content_matrix,
        result_switch_matrix,
        retain_lower_limit.reshape(1, 256),
        extra_shrink_log.T,
        lane_result_rescale.reshape(1, 128),
        memory_matrix,
        result_matrix,
        later_rescale_vector.reshape(1, 32),
        mixer_switch_matrix.T,
        widening_matrix.T,
        narrowing_matrix,
    )
    mixed, carried = finish(packed, place, new_state)
    return (mixed.T, carried)


def solution(mesh):
    torus = Mesh(mesh.devices.reshape(4, 4, 4, 2), ("kv_0", "kv_1", "tp_0", "tp_1"))
    placed = (
        P(None, KV_TP),
        P(),
        P(KV, TP, None, None),
        P(KV),
        P(KV, TP),
        P(KV, TP),
        P(KV, TP),
        P(KV, TP),
        P(TP),
        P(KV, TP),
        P(),
        P(TP, KV),
        P(KV_TP),
        P(None, KV_TP),
        P(None, KV_TP),
        P(KV_TP, None),
    )
    return jax.shard_map(
        local,
        mesh=torus,
        in_specs=placed,
        out_specs=(P(None, KV_TP), P(KV, TP, None, None)),
        check_vma=False,
    )
```

```python
import functools

import jax
import jax.numpy as jnp
from jax import lax
from jax.experimental import pallas as pl
from jax.experimental.pallas import tpu as pltpu
from jax.sharding import Mesh
from jax.sharding import PartitionSpec as P

KV = ("kv_0", "kv_1")
TP = ("tp_0", "tp_1")
KV_TP = ("kv_0", "kv_1", "tp_0", "tp_1")
MESH = pl.DeviceIdType.MESH
EPS = 1e-06
F32 = jnp.float32
BF = jnp.bfloat16
PARTS = ((0, 3), (3, 3), (6, 2))
ORDERS = ("xyz", "yzx", "zxy")
ROWS = (0, 1, 3, 2)


def my_position():
    return dict(
        z=lax.axis_index("kv_0"),
        y=lax.axis_index("kv_1"),
        x=lax.axis_index("tp_0"),
        c=lax.axis_index("tp_1"),
    )


def device_at(at, **moved):
    there = dict(at, **moved)
    return (there["z"], there["y"], there["x"], there["c"])


def plane_offsets():
    return [(dz, dy) for dz in range(4) for dy in range(4) if dz or dy]


def line_offsets():
    return [(dx, dc) for dx in range(4) for dc in range(2) if dx or dc]


def plane_peer(at, dz, dy):
    return device_at(at, z=(at["z"] + dz) % 4, y=(at["y"] + dy) % 4)


def line_peer(at, dx, dc):
    return device_at(at, x=(at["x"] + dx) % 4, c=(at["c"] + dc) % 2)


def meet(peers, meanwhile):
    barrier = pltpu.get_barrier_semaphore()
    for peer in peers:
        pl.semaphore_signal(barrier, inc=1, device_id=peer, device_id_type=MESH)
    meanwhile()
    pl.semaphore_wait(barrier, len(peers))


class Sender:
    def __init__(self, sends, recvs):
        self.sends, self.recvs, self.used = sends, recvs, 0

    def __call__(self, src, dst, peer):
        i = self.used
        self.used = i + 1
        return start_copy(src, dst, self.sends.at[i], self.recvs.at[i], peer)


def start_copy(src, dst, send_sem, recv_sem, peer):
    copy = pltpu.make_async_remote_copy(
        src_ref=src,
        dst_ref=dst,
        send_sem=send_sem,
        recv_sem=recv_sem,
        device_id=peer,
        device_id_type=MESH,
    )
    copy.start()
    return copy


def times(a, b, dims=((1,), (1,))):
    return lax.dot_general(a, b, (dims, ((), ())), preferred_element_type=F32)


def row_of(column, rows):
    eye = lax.broadcasted_iota(jnp.int32, (rows, 128), 0) == lax.broadcasted_iota(
        jnp.int32, (rows, 128), 1
    )
    return jnp.sum(jnp.where(eye, column, 0.0), axis=0, keepdims=True)


def column_of(row, rows):
    eye = lax.broadcasted_iota(jnp.int32, (rows, 128), 0) == lax.broadcasted_iota(
        jnp.int32, (rows, 128), 1
    )
    return jnp.sum(jnp.where(eye, row, 0.0), axis=1, keepdims=True)


def picks(place, start, rows):
    want = lax.broadcasted_iota(jnp.int32, (rows, 1024), 0) + start
    return jnp.where(want == place, 1.0, 0.0).astype(BF)


def halves(length):
    return pl.ds(0, length // 2), pl.ds(length // 2, length - length // 2)


def gather_plane(at, bufs, orders, send):
    copies = [{} for _ in orders]
    for db in ROWS:
        for p, order in enumerate(orders):
            a, b, c = order
            own = bufs[p].at[at[c], at[b], at[a]]
            for da in range(4):
                if db or da:
                    there = {a: (at[a] + da) % 4, b: (at[b] + db) % 4}
                    copies[p][db, da] = send(own, own, device_at(at, **there))
    return copies


def gather_line(at, bufs, orders, plane, send):
    first = {}
    for db in ROWS:
        for p, (a, b, c) in enumerate(orders):
            for da in range(4):
                if db or da:
                    plane[p][db, da].wait_recv()
            own = bufs[p].at[at[c], (at[b] + 4 - db) % 4]
            first[p, db] = tuple(
                send(own, own, device_at(at, **{c: (at[c] + turn) % 4}))
                for turn in ((1, 3, 2) if db == 2 else (1, 3))
            )
    yield
    second = []
    for db, parts in ((0, ((1, 0, 4),)), (1, ((3, 0, 4),)), (3, ((1, 0, 2), (3, 2, 2)))):
        for p, (a, b, c) in enumerate(orders):
            for copy in first[p, db]:
                copy.wait_recv()
            for turn, start, size in parts:
                came = bufs[p].at[
                    (at[c] + 4 - turn) % 4, (at[b] + 4 - db) % 4, pl.ds(start, size)
                ]
                second.append(send(came, came, device_at(at, **{c: (at[c] + turn) % 4})))
    yield
    for p in range(len(orders)):
        for copy in first[p, 2]:
            copy.wait_recv()
    for part in (*[part.values() for part in plane], *first.values()):
        for copy in part:
            copy.wait_send()
    for copy in second:
        copy.wait()
    yield


def add_into(ref, idx, term):
    ref[idx] = (ref[idx].astype(F32) + term.astype(F32)).astype(BF)


def reduce_line(at, bufs, axes, pres, received, send, keep=True, after=None):
    early = []
    for p, (axis, pre) in enumerate(zip(axes, pres)):
        one_up, one_down, two_up, two_down = received[p]
        m = at[axis]
        up, down, away = (m + 1) % 4, (m + 3) % 4, (m + 2) % 4
        to_up, to_down = device_at(at, **{axis: up}), device_at(at, **{axis: down})
        lo, hi = halves(bufs[p].shape[len(pre) + 1])
        early.append((
            send(bufs[p].at[(*pre, away, lo)], one_up, to_up),
            send(bufs[p].at[(*pre, away, hi)], one_down, to_down),
            send(bufs[p].at[(*pre, up, hi)], two_up.at[hi], to_up),
            send(bufs[p].at[(*pre, down, lo)], two_down.at[lo], to_down),
        ))
    yield
    late = []
    for p, (axis, pre) in enumerate(zip(axes, pres)):
        one_up, one_down, two_up, two_down = received[p]
        m = at[axis]
        up, down = (m + 1) % 4, (m + 3) % 4
        to_up, to_down = device_at(at, **{axis: up}), device_at(at, **{axis: down})
        lo, hi = halves(bufs[p].shape[len(pre) + 1])
        early[p][0].wait_recv()
        add_into(bufs[p], (*pre, up, lo), one_up[...])
        a = send(bufs[p].at[(*pre, up, lo)], two_up.at[lo], to_up)
        early[p][1].wait_recv()
        add_into(bufs[p], (*pre, down, hi), one_down[...])
        late.append((a, send(bufs[p].at[(*pre, down, hi)], two_down.at[hi], to_down)))
    yield
    sums = []
    for p, (axis, pre) in enumerate(zip(axes, pres)):
        for copy in early[p][2:]:
            copy.wait_recv()
        for copy in late[p]:
            copy.wait_recv()
        own = (*pre, at[axis])
        total = bufs[p][own].astype(F32)
        for ref in received[p][2:]:
            total = total + ref[...].astype(F32)
        if keep:
            bufs[p][own] = total.astype(BF)
        sums.append(total)
        if after:
            after(p)
    for p in range(len(axes)):
        for copy in (*early[p], *late[p]):
            copy.wait_send()
    yield sums


def reduce_torus(at, bufs, orders, line_received, plane_received, send):
    early, late, plane = {}, {}, {}
    lo, hi = pl.ds(0, 2), pl.ds(2, 2)

    def row(p, db):
        a, b, c = orders[p]
        m = at[c]
        return c, m, (m + 1) % 4, (m + 3) % 4, (at[b] + db) % 4

    def begin(db):
        for p in range(len(orders)):
            c, m, up, down, r = row(p, db)
            one_up, one_down, two_up, two_down = line_received[p]
            to_up, to_down = device_at(at, **{c: up}), device_at(at, **{c: down})
            away = (m + 2) % 4
            early[p, db] = (
                send(bufs[p].at[away, r, lo], one_up.at[db], to_up),
                send(bufs[p].at[away, r, hi], one_down.at[db], to_down),
                send(bufs[p].at[up, r, hi], two_up.at[db, hi], to_up),
                send(bufs[p].at[down, r, lo], two_down.at[db, lo], to_down),
            )

    def go_on(db):
        for p in range(len(orders)):
            c, m, up, down, r = row(p, db)
            one_up, one_down, two_up, two_down = line_received[p]
            to_up, to_down = device_at(at, **{c: up}), device_at(at, **{c: down})
            early[p, db][0].wait_recv()
            add_into(bufs[p], (up, r, lo), one_up[db])
            first = send(bufs[p].at[up, r, lo], two_up.at[db, lo], to_up)
            early[p, db][1].wait_recv()
            add_into(bufs[p], (down, r, hi), one_down[db])
            late[p, db] = (first, send(bufs[p].at[down, r, hi], two_down.at[db, hi], to_down))

    def end(db):
        for p, (a, b, c) in enumerate(orders):
            _, m, up, down, r = row(p, db)
            two_up, two_down = line_received[p][2:]
            for copy in (*early[p, db][2:], *late[p, db]):
                copy.wait_recv()
            total = bufs[p][m, r].astype(F32) + two_up[db].astype(F32) + two_down[db].astype(F32)
            bufs[p][m, r] = total.astype(BF)
            for da in range(4):
                if db or da:
                    n = 4 * db + da - 1
                    there = {a: (at[a] + da) % 4, b: r}
                    block = bufs[p].at[m, r, there[a]]
                    plane[p, n] = send(block, plane_received[p].at[n], device_at(at, **there))

    rows = ROWS[::-1]
    for db in rows:
        begin(db)
    for db in rows:
        go_on(db)
    for db in rows:
        end(db)
    sums = []
    for p, (a, b, c) in enumerate(orders):
        total = bufs[p][at[c], at[b], at[a]].astype(F32)
        for n in range(14, -1, -1):
            plane[p, n].wait_recv()
            total = total + plane_received[p][n].astype(F32)
        sums.append(total)
    for copies in (*early.values(), *late.values(), plane.values()):
        for copy in copies:
            copy.wait_send()
    return sums


def split(v):
    high = v.astype(BF)
    return high, (v - high.astype(F32)).astype(BF)


INPUTS = (
    "x", "lengths", "gain", "wq", "wf", "wi", "wo", "bound", "shrink", "lane_gain", "state",
    "result", "later_gain", "gate", "wide", "narrow",
)
SMALL = (
    ("lengths", (1, 128), jnp.int32),
    ("gain", (1, 256), F32),
    ("bound", (1, 256), F32),
    ("shrink", (2, 64), F32),
    ("lane_gain", (1, 128), F32),
    ("later_gain", (1, 32), F32),
)


def line_shapes(shape, count):
    shapes = []
    for _ in range(count):
        half = shape[0] // 2
        shapes += [(half, *shape[1:]), (shape[0] - half, *shape[1:]), shape, shape]
    return shapes


def scratch():
    counts = [count for _, count in PARTS]
    boxes = [(4, 4, 4, count, 16, 128) for count in counts]
    named = [
        *[("small_" + name, shape, kind) for name, shape, kind in SMALL],
        ("cols", (8, 32, 1024), BF),
        ("scaled", (1024, 256), BF),
        ("squares", (8, 8, 128), F32),
        ("squares_in", (15, 8, 128), F32),
        ("front_weights", (4, 256, 256), BF),
        ("pa", (2, 4, 4, 64, 256), BF),
        ("pb", (2, 4, 4, 64, 256), BF),
        ("z", (64, 1024), F32),
        ("query", (64, 256), F32),
        ("kept", (64, 256), F32),
        ("key", (64, 256), F32),
        ("output", (64, 256), F32),
        ("state_in", (8, 2, 128, 128), F32),
        ("state_out", (8, 2, 128, 128), F32),
        ("chosen", (512, 1024), BF),
        ("heads", (16, 2, 64, 128), BF),
        ("partial", (8, 64, 256), BF),
        ("arrived", (7, 64, 256), BF),
        ("own_gain", (8, 128), F32),
        ("gains", (8, 8, 128), F32),
        ("own_rows", (64, 256), F32),
        ("residual", (64, 256), F32),
        ("later_squares", (16, 8, 128), F32),
        ("squares_sum", (8, 128), F32),
        ("squares_line", (4, 8, 128), F32),
        ("weights", (2, 2, 128, 4096), BF),
        ("narrows", (2, 128, 4096), BF),
        ("staged", (3, 86, 4096), BF),
        ("result_in", (256, 256), BF),
        ("total", (2, 256, 256), F32),
        ("ypack", (8, 16, 128), BF),
        ("yarrive", (8, 16, 128), BF),
    ]
    groups = [
        ("gathered", boxes),
        ("terms", boxes),
        ("front_one", line_shapes((4, 64, 256), 4)),
        ("front_two", [(3, 64, 256)] * 4),
        (
            "mixer_line",
            [(4, n, count, 16, 128) for count in counts for n in (2, 2, 4, 4)],
        ),
        ("mixer_plane", [(15, count, 16, 128) for count in counts]),
    ]
    flat = [pltpu.VMEM(shape, kind) for _, shape, kind in named]
    for _, shapes in groups:
        flat += [pltpu.VMEM(shape, BF) for shape in shapes]
    return named, groups, flat


def layer_kernel(*refs):
    named, groups, flat = scratch()
    ref = dict(zip(INPUTS, refs))
    mixed_out, place_out, state_result = refs[len(INPUTS) : len(INPUTS) + 3]
    rest = refs[len(INPUTS) + 3 :]
    ref.update(zip(["_" + name for name, _, _ in named], rest))
    rest = rest[len(named) :]
    group = {}
    for name, shapes in groups:
        group[name], rest = rest[: len(shapes)], rest[len(shapes) :]
    sends, recvs, local, ready = rest
    send = Sender(sends, recvs)
    at = my_position()
    kv = 4 * at["z"] + at["y"]
    tp = 2 * at["x"] + at["c"]
    planes, lines = plane_offsets(), line_offsets()
    fours = lambda refs: [refs[i : i + 4] for i in range(0, len(refs), 4)]

    def fetch(n, src, dst):
        copy = pltpu.make_async_copy(src, dst, local.at[n])
        copy.start()
        return copy

    cols = ref["_cols"]
    small_copies = [
        fetch(11 + n, ref[name], ref["_small_" + name]) for n, (name, _, _) in enumerate(SMALL)
    ]
    for name, _, _ in SMALL:
        ref[name] = ref["_small_" + name]
    x_copy = fetch(0, ref["x"], cols.at[tp])
    front_copies = [
        fetch(1 + n, ref[name], ref["_front_weights"].at[n])
        for n, name in enumerate(("wq", "wf", "wi", "wo"))
    ]
    weight_copies = [
        fetch(5 + n, ref[name], ref["_staged"].at[n])
        for n, name in enumerate(("gate", "wide", "narrow"))
    ]
    state_copy = fetch(8, ref["state"], ref["_state_in"])
    result_copy = fetch(9, ref["result"], ref["_result_in"])
    weights, narrows, staged = ref["_weights"], ref["_narrows"], ref["_staged"]

    def pad_weights():
        for n, first in ((0, 80), (1, 96)):
            weights[n, :, first:128] = jnp.zeros((2, 128 - first, 4096), BF)
            narrows[n, first:128] = jnp.zeros((128 - first, 4096), BF)
        for copy in weight_copies:
            copy.wait()
        weights[0, :, 0:86] = staged[0:2]
        narrows[0, 0:86] = staged[2]

    turns = (1, 2, 3)
    meet(
        [line_peer(at, *d) for d in lines]
        + [plane_peer(at, dz, 0) for dz in turns]
        + [plane_peer(at, 0, dy) for dy in turns],
        lambda: None,
    )
    for dy in turns:
        pl.semaphore_signal(ready, inc=1, device_id=plane_peer(at, 0, dy), device_id_type=MESH)

    x_copy.wait()
    partner = line_peer(at, 0, 1)
    far_copies = [send(cols.at[tp], cols.at[tp], line_peer(at, dx, 0)) for dx in turns]
    near_copies = [send(cols.at[tp], cols.at[tp], partner)]
    for copy in small_copies:
        copy.wait()
    own_gain, gains = ref["_own_gain"], ref["_gains"]
    own_gain[...] = jnp.broadcast_to(
        jnp.concatenate([ref["later_gain"][...], jnp.zeros((1, 96), F32)], axis=1), (8, 128)
    )
    gain_copies = [send(own_gain, gains.at[tp], line_peer(at, *d)) for d in lines]
    gains[pl.ds(tp, 1)] = own_gain[...][None]

    lengths = jnp.broadcast_to(ref["lengths"][...], (8, 128)).astype(F32).astype(BF)
    s = lax.broadcasted_iota(jnp.int32, (128, 1024), 0)
    owner = lax.broadcasted_iota(jnp.int32, (128, 1024), 1) // 8
    start = times(lengths, jnp.where(s < owner, 1.0, 0.0).astype(BF), ((1,), (0,)))
    length = times(lengths, jnp.where(s == owner, 1.0, 0.0).astype(BF), ((1,), (0,)))
    slot = lax.broadcasted_iota(jnp.int32, (8, 1024), 1) % 8
    place = jnp.where(slot < length.astype(jnp.int32), start.astype(jnp.int32) + slot, -1)
    place_out[...] = place
    place = place[0:1]
    for part in range(4):
        ref["_chosen"][128 * part : 128 * part + 128] = picks(place, 128 * part, 128)
    gain = jnp.concatenate(
        [column_of(ref["gain"][:, 0:128], 128), column_of(ref["gain"][:, 128:256], 128)], axis=0
    )
    pad_weights()
    for dx, copy in zip(turns, far_copies):
        copy.wait()
        came = 2 * ((at["x"] + 4 - dx) % 4) + at["c"]
        near_copies.append(send(cols.at[came], cols.at[came], partner))
    for copy in near_copies:
        copy.wait()
    scaled, squares = ref["_scaled"], ref["_squares"]
    for k in range(8):
        lanes = slice(128 * k, 128 * k + 128)
        v = cols[:, :, lanes].reshape(256, 128).astype(F32)
        scaled[lanes, :] = (v * gain).astype(BF).T
        squares[k] = jnp.broadcast_to(jnp.sum(v * v, axis=0, keepdims=True), (8, 128))
    for copy in front_copies:
        copy.wait()
    pa, pb = ref["_pa"], ref["_pb"]

    chunks = ((0, pa.at[0], "yz"), (1, pb.at[0], "zy"), (2, pa.at[1], "yz"), (3, pb.at[1], "zy"))
    one, two = fours(group["front_one"]), group["front_two"]

    def project(n, terms, order):
        def body(a, carry):
            lhs = scaled[pl.ds(pl.multiple_of(256 * a, 256), 256), :]
            v = times(lhs, ref["_front_weights"][n], ((1,), (0,))).astype(BF).reshape(4, 64, 256)
            if order == "yz":
                terms[:, a] = v
            else:
                terms[a] = v
            return carry

        lax.fori_loop(0, 4, body, 0, unroll=True)

    lines_one = []
    for n, terms, order in chunks:
        project(n, terms, order)
        lines_one.append(reduce_line(at, (terms,), order[0], ((),), one[n : n + 1], send))
        next(lines_one[n])
    for step in lines_one:
        next(step)
    pl.semaphore_wait(ready, 3)
    square_copies = []
    for i, (dz, dy) in enumerate(planes):
        peer = plane_peer(at, dz, dy)
        block = squares.at[(4 * peer[0] + peer[1]) // 2]
        square_copies.append(send(block, ref["_squares_in"].at[i], peer))
    ref["_own_rows"][...] = times(picks(place, 64 * tp, 64), cols[...].reshape(256, 1024))
    second = []
    for n, terms, order in chunks:
        next(lines_one[n])
        here, axis = at[order[0]], order[1]
        second.append([])
        for turn in turns:
            there = (at[axis] + turn) % 4
            peer = device_at(at, **{axis: there})
            second[n].append(send(terms.at[here, there], two[n].at[turn - 1], peer))
    row = lax.broadcasted_iota(jnp.int32, (64, 128), 0)
    lane = lax.broadcasted_iota(jnp.int32, (64, 128), 1)
    length = jnp.sum(
        jnp.where(lane == 8 * kv + row // 8, ref["lengths"][...].astype(F32), 0.0),
        axis=1,
        keepdims=True,
    )
    live = (row[:, 0:1] % 8).astype(F32) < length
    for copy in square_copies:
        copy.wait()
    total = jnp.sum(ref["_squares_in"][...], axis=0) + squares[kv // 2]
    own = jnp.sum(
        jnp.where(lane == 64 * (kv % 2) + row, total[0:1, :], 0.0), axis=1, keepdims=True
    )
    scale = lax.rsqrt(own / 4096 + EPS)
    z = ref["_z"]
    for n, terms, order in chunks:
        total = terms[at[order[0]], at[order[1]]].astype(F32)
        for i, copy in enumerate(second[n]):
            copy.wait()
            total = total + two[n][i].astype(F32)
        z[:, 256 * n : 256 * n + 256] = total * scale

    weight_sends = [
        send(weights.at[0, :, 0:96], weights.at[1, :, 0:96], partner),
        send(narrows.at[0, 0:96], narrows.at[1, 0:96], partner),
    ]

    query, kept, keys, output = ref["_query"], ref["_kept"], ref["_key"], ref["_output"]
    slot = lax.broadcasted_iota(jnp.int32, (8, 8, 128), 1)
    state_in, state_out, heads = ref["_state_in"], ref["_state_out"], ref["_heads"]

    def read_state(h, n, carry):
        rows = pl.ds(pl.multiple_of(8 * n, 8), 8)
        lanes = slice(128 * h, 128 * h + 128)
        s_high, s_low = split(state_in[n, h])
        q_high, q_low = split(query[rows, lanes])
        lhs = jnp.concatenate(
            [
                jnp.concatenate([q_high, q_high], axis=1),
                jnp.concatenate([q_low, jnp.zeros_like(q_low)], axis=1),
            ],
            axis=0,
        )
        o = times(lhs, jnp.concatenate([s_high, s_low], axis=0), ((1,), (0,)))
        output[rows, lanes] += o[0:8] + o[8:16]
        return carry

    copies = []
    for h in range(2):
        lanes = slice(128 * h, 128 * h + 128)
        bound = ref["bound"][:, lanes]
        retain = bound + (1.0 - bound) * jax.nn.sigmoid(z[:, 256 + 128 * h : 384 + 128 * h])
        shrink = jnp.sum(
            jnp.where(lane[:, 0:64] == row[:, 0:64], ref["shrink"][h : h + 1, :], 0.0),
            axis=1,
            keepdims=True,
        )
        decay = jnp.where(live, jnp.exp(jnp.log(retain) + shrink), 1.0).reshape(8, 8, 128)
        key = jnp.where(live, 1.0 - retain, 0.0).reshape(8, 8, 128)
        zq = z[:, lanes]
        q = (zq * jax.nn.sigmoid(zq)).reshape(8, 8, 128)
        value = z[:, 512 + 128 * h : 640 + 128 * h].reshape(8, 8, 128)
        between = q
        out = jnp.sum(q * key, axis=2, keepdims=True) * value
        for back in range(1, 8):
            between = between * (decay if back == 1 else pltpu.roll(decay, back - 1, 1))
            weight = jnp.sum(between * pltpu.roll(key, back, 1), axis=2, keepdims=True)
            out = out + jnp.where(slot >= back, weight * pltpu.roll(value, back, 1), 0.0)
        output[:, lanes] = out.reshape(64, 128)
        before, after = decay, jnp.where(slot < 7, pltpu.roll(decay, 7, 1), 1.0)
        for step in (1, 2, 4):
            before = before * jnp.where(slot >= step, pltpu.roll(before, step, 1), 1.0)
            after = after * jnp.where(slot + step < 8, pltpu.roll(after, 8 - step, 1), 1.0)
        query[:, lanes] = (q * before).reshape(64, 128)
        kept[:, lanes] = before.reshape(64, 128)
        keys[:, lanes] = (key * after).reshape(64, 128)
        if h == 0:
            state_copy.wait()
        lax.fori_loop(0, 8, functools.partial(read_state, h), 0, unroll=8)
        o = output[:, lanes]
        zo = z[:, 768 + 128 * h : 896 + 128 * h]
        o = o * lax.rsqrt(jnp.mean(o * o, axis=1, keepdims=True) + EPS) * ref["lane_gain"][...]
        heads[kv, h] = jnp.where(live, o * (zo * jax.nn.sigmoid(zo)), 0.0).astype(BF)
        own = heads.at[kv, h]
        copies += [send(own, own, plane_peer(at, *d)) for d in planes]
    def write_state(n, carry):
        rows = pl.ds(pl.multiple_of(8 * n, 8), 8)
        for h in range(2):
            lanes = slice(128 * h, 128 * h + 128)
            k_high, k_low = split(keys[rows, lanes])
            v_high, v_low = split(z[rows, 512 + 128 * h : 640 + 128 * h])
            added = times(
                jnp.concatenate([k_high, k_high, k_low], axis=0),
                jnp.concatenate([v_high, v_low, v_high], axis=0),
                ((0,), (0,)),
            )
            state_out[n, h] = column_of(kept[rows, lanes][7:8, :], 128) * state_in[n, h] + added
        return carry

    lax.fori_loop(0, 8, write_state, 0)
    new_copy = fetch(10, state_out, state_result)
    result_copy.wait()
    for copy in gain_copies:
        copy.wait()
    gain = jnp.concatenate([gains[t, 0:1, 0:32] for t in range(8)], axis=1)
    for copy in copies:
        copy.wait()

    partial, arrived, result = ref["_partial"], ref["_arrived"], ref["_result_in"]
    all_heads = jnp.concatenate([heads[:, h].reshape(1024, 128) for h in range(2)], axis=1)
    for part in range(2):
        picked = ref["_chosen"][256 * part : 256 * part + 256]
        packed = times(picked, all_heads, ((1,), (0,))).astype(BF)
        partial[4 * part : 4 * part + 4] = (
            times(packed, result[...], ((1,), (0,))).astype(BF).reshape(4, 64, 256)
        )
    other = 1 - at["c"]
    near = [send(partial.at[2 * ((at["x"] + dx) % 4) + other], arrived.at[dx], partner) for dx in (2, 1, 3, 0)]
    copies = []
    for dx, copy in zip((2, 1, 3, 0), near):
        copy.wait_recv()
        own = 2 * ((at["x"] + dx) % 4) + at["c"]
        both = partial[own].astype(F32) + arrived[dx].astype(F32)
        if dx:
            partial[own] = both.astype(BF)
            copies.append(send(partial.at[own], arrived.at[3 + dx], line_peer(at, dx, 0)))
    attended = both
    for dx, copy in zip((2, 1, 3), copies):
        copy.wait()
        attended = attended + arrived[3 + dx].astype(F32)
    for copy in near:
        copy.wait_send()
    residual = (ref["_own_rows"][...] + attended).astype(BF).astype(F32)
    later = ref["_later_squares"]
    own_squares = jnp.sum(residual * residual, axis=1, keepdims=True)
    later[0] = jnp.broadcast_to(row_of(own_squares, 64), (8, 128))
    square_copies = [
        send(later.at[0], later.at[1 + i], plane_peer(at, *d)) for i, d in enumerate(planes)
    ]
    tile = (residual * gain).astype(BF)
    blocks = [
        tile[16 * i : 16 * i + 16, 128 * h : 128 * h + 128] for h in range(2) for i in range(4)
    ]
    gathered = group["gathered"]
    for p, ((first, count), order) in enumerate(zip(PARTS, ORDERS)):
        idx = tuple(at[a] for a in order[::-1])
        for b in range(count):
            gathered[p][(*idx, b)] = blocks[first + b]
    copies = gather_plane(at, gathered, ORDERS, send)
    ref["_residual"][...] = residual
    steps = gather_line(at, gathered, ORDERS, copies, send)
    next(steps)
    for copy in square_copies:
        copy.wait()
    squares_sum, squares_line = ref["_squares_sum"], ref["_squares_line"]
    own_sum = jnp.sum(later[...], axis=0)
    squares_sum[...] = own_sum
    squares_line[pl.ds(at["x"], 1)] = own_sum[None]
    line_copies = [
        send(squares_sum, squares_line.at[at["x"]], line_peer(at, dx, 0)) for dx in (1, 2, 3)
    ]
    next(steps)
    total = ref["_total"]
    total[...] = jnp.zeros_like(total)
    for copy in (*line_copies, *weight_sends):
        copy.wait()
    scale = lax.rsqrt(
        jnp.concatenate([column_of(squares_line[g, 0:1, :], 64) for g in range(4)], axis=0)
        / 4096
        + EPS
    )
    next(steps)

    ga, gb, gc = gathered

    def rows_at(zz, yy):
        v = jnp.concatenate([ga[zz, yy], gb[:, zz, yy], gc[yy, :, zz]], axis=1)
        return jnp.concatenate(
            [v[:, 0:4].reshape(256, 128), v[:, 4:8].reshape(256, 128)], axis=1
        )

    def widening(zz, carry):
        lhs = jnp.concatenate([rows_at(zz, yy) for yy in range(4)], axis=1)
        cols = pl.ds(pl.multiple_of(zz * 1024, 1024), 1024)
        for core in range(2):
            total[core] += times(lhs, weights[core, :, :, cols].reshape(256, 1024))
        return carry

    lax.fori_loop(0, 4, widening, 0, unroll=2)
    hidden = []
    for core in range(2):
        gated = total[core, :, 0:128] * scale
        upward = total[core, :, 128:256] * scale
        hidden.append((gated * jax.nn.sigmoid(gated) * upward).astype(BF))
    hidden = jnp.concatenate(hidden, axis=1)
    ta, tb, tc = group["terms"]

    def narrowing(zz, carry):
        cols = pl.ds(pl.multiple_of(zz * 1024, 1024), 1024)
        rhs = jnp.concatenate([narrows[0, :, cols], narrows[1, :, cols]], axis=0)
        term = times(hidden, rhs, ((1,), (0,))).astype(BF)
        for yy in range(4):
            v = jnp.concatenate(
                [
                    term[:, 256 * yy + 128 * h : 256 * yy + 128 * h + 128].reshape(4, 4, 16, 128)
                    for h in range(2)
                ],
                axis=1,
            )
            ta[zz, yy] = v[:, 0:3]
            tb[:, zz, yy] = v[:, 3:6]
            tc[yy, :, zz] = v[:, 6:8]
        return carry

    lax.fori_loop(0, 4, narrowing, 0, unroll=2)
    sums = jnp.concatenate(
        reduce_torus(
            at, group["terms"], ORDERS, fours(group["mixer_line"]), group["mixer_plane"], send
        ),
        axis=0,
    )

    mixed = []
    for h in range(2):
        for i in range(4):
            res = ref["_residual"][16 * i : 16 * i + 16, 128 * h : 128 * h + 128]
            mixed.append((res + sums[4 * h + i]).astype(BF))
    ypack, yarrive = ref["_ypack"], ref["_yarrive"]
    for t in range(8):
        h, first = t // 4, 32 * (t % 4)
        ypack[t] = jnp.concatenate(
            [mixed[4 * h + i][:, first : first + 32] for i in range(4)], axis=1
        )
    copies = []
    for dx, dc in lines:
        peer = line_peer(at, dx, dc)
        copies.append(send(ypack.at[2 * peer[2] + peer[3]], yarrive.at[tp], peer))
    yarrive[pl.ds(tp, 1)] = ypack[pl.ds(tp, 1)]
    for copy in copies:
        copy.wait()
    mixed_out[...] = yarrive[...]
    new_copy.wait()
    assert send.used <= sends.shape[0]


def layer(*arguments):
    vmem = pl.BlockSpec(memory_space=pltpu.VMEM)
    far = pl.BlockSpec(memory_space=pltpu.HBM)
    copies = 400
    return pl.pallas_call(
        layer_kernel,
        out_shape=(
            jax.ShapeDtypeStruct((8, 16, 128), BF),
            jax.ShapeDtypeStruct((8, 1024), jnp.int32),
            jax.ShapeDtypeStruct((8, 2, 128, 128), F32),
        ),
        in_specs=[far] * len(INPUTS),
        out_specs=(vmem, vmem, far),
        scratch_shapes=[
            *scratch()[2],
            pltpu.SemaphoreType.DMA((copies,)),
            pltpu.SemaphoreType.DMA((copies,)),
            pltpu.SemaphoreType.DMA((17,)),
            pltpu.SemaphoreType.REGULAR,
        ],
        compiler_params=pltpu.CompilerParams(
            collective_id=0, has_side_effects=True, vmem_limit_bytes=67043328
        ),
        name="layer",
    )(*arguments)


def finish_kernel(packed_ref, place_ref, state_ref, mixed_ref, new_ref, held, packed, place, out, sems):
    takes = []
    for n, (src, dst) in enumerate(((packed_ref, packed), (place_ref, place))):
        takes.append(pltpu.make_async_copy(src, dst, sems.at[n]))
        takes[n].start()
    for n in range(4):
        half = pl.ds(2 * n, 2)
        takes.append(pltpu.make_async_copy(state_ref.at[half], held.at[half], sems.at[2 + n]))
        takes[2 + n].start()
    takes[0].wait()
    takes[1].wait()
    j = lax.broadcasted_iota(jnp.int32, (128, 1024), 0)
    rows = 64 * (j // 16) + j % 16 - place[0:1, :]
    gives = []
    mixed = jnp.zeros((32, 1024), F32)
    for a in range(4):
        takes[2 + a].wait()
        half = pl.ds(2 * a, 2)
        gives.append(pltpu.make_async_copy(held.at[half], new_ref.at[half], sems.at[6 + a]))
        gives[a].start()
        chosen = jnp.where(rows == -16 * a, 1.0, 0.0).astype(BF)
        piece = packed[...].reshape(128, 128)[:, 32 * a : 32 * a + 32]
        mixed = mixed + times(piece, chosen, ((0,), (0,)))
    out[...] = mixed.astype(BF)
    give = pltpu.make_async_copy(out, mixed_ref, sems.at[10])
    give.start()
    for copy in gives:
        copy.wait()
    give.wait()


def finish(packed, place, state):
    far = pl.BlockSpec(memory_space=pltpu.HBM)
    return pl.pallas_call(
        finish_kernel,
        out_shape=(
            jax.ShapeDtypeStruct((32, 1024), BF),
            jax.ShapeDtypeStruct((8, 2, 128, 128), F32),
        ),
        in_specs=[far] * 3,
        out_specs=(far, far),
        scratch_shapes=[
            pltpu.VMEM((8, 2, 128, 128), F32),
            pltpu.VMEM((8, 16, 128), BF),
            pltpu.VMEM((8, 1024), jnp.int32),
            pltpu.VMEM((32, 1024), BF),
            pltpu.SemaphoreType.DMA((11,)),
        ],
        compiler_params=pltpu.CompilerParams(vmem_limit_bytes=67043328),
        name="finish",
    )(packed, place, state)


def local(
    residual_entries,
    fresh_extents,
    memory_matrix,
    initial_rescale_vector,
    probe_matrix,
    retain_matrix,
    content_matrix,
    result_switch_matrix,
    retain_lower_limit,
    extra_shrink_log,
    lane_result_rescale,
    result_matrix,
    later_rescale_vector,
    mixer_switch_matrix,
    widening_matrix,
    narrowing_matrix,
):
    packed, place, new_state = layer(
        residual_entries.T,
        fresh_extents.reshape(1, 128),
        initial_rescale_vector.reshape(1, 256),
        probe_matrix,
        retain_matrix,
        content_matrix,
        result_switch_matrix,
        retain_lower_limit.reshape(1, 256),
        extra_shrink_log.T,
        lane_result_rescale.reshape(1, 128),
        memory_matrix,
        result_matrix,
        later_rescale_vector.reshape(1, 32),
        mixer_switch_matrix.T,
        widening_matrix.T,
        narrowing_matrix,
    )
    mixed, carried = finish(packed, place, new_state)
    return (mixed.T, carried)


def solution(mesh):
    torus = Mesh(mesh.devices.reshape(4, 4, 4, 2), ("kv_0", "kv_1", "tp_0", "tp_1"))
    placed = (
        P(None, KV_TP),
        P(),
        P(KV, TP, None, None),
        P(KV),
        P(KV, TP),
        P(KV, TP),
        P(KV, TP),
        P(KV, TP),
        P(TP),
        P(KV, TP),
        P(),
        P(TP, KV),
        P(KV_TP),
        P(None, KV_TP),
        P(None, KV_TP),
        P(KV_TP, None),
    )
    return jax.shard_map(
        local,
        mesh=torus,
        in_specs=placed,
        out_specs=(P(None, KV_TP), P(KV, TP, None, None)),
        check_vma=False,
    )
```
